32 devices in a mesh: grp: 2 (over y), sp: 4 (over z), tp: 4 (over x, core).
Axes of the slice: x: 2, y: 2, z: 4, core: 2. Of those that a mesh axis runs over, the one named last changes fastest.
Arguments:
- latent: bfloat16 [4096, 2048], P(('grp', 'sp', 'tp')), parts along dimension 0, may hold values from -3 to 3
- context: bfloat16 [1024, 2048], P(('grp', 'sp')), parts along dimension 0, may hold values from -6 to 6
- condition: float32 [4096], P(('grp', 'sp')), parts along dimension 0, may hold values from -6 to 6
- context_condition: float32 [2048], P('sp'), may hold values from -6 to 6
- mod_weight: bfloat16 [2048, 6144], P('sp', 'tp'), may hold values from -0.1875 to 0.1875
- mod_bias: float32 [6144], replicated, may hold values from -1.5 to 1.5
- query_weight: bfloat16 [2048, 1024], P('sp'), may hold values from -0.125 to 0.125
- key_weight: bfloat16 [2048, 1024], P('sp'), may hold values from -0.125 to 0.125
- value_weight: bfloat16 [2048, 2048], P(None, 'tp'), may hold values from -3 to 3
- out_gate_weight: bfloat16 [2048, 2048], P(None, 'tp'), may hold values from -0.125 to 0.125
- decay_in_weight: bfloat16 [2048, 32], replicated, may hold values from -0.125 to 0.125
- decay_weight: bfloat16 [2, 16, 1024], replicated, may hold values from -1.5 to 1.5
- decay_bias: float32 [2, 1024], replicated, may hold values from 0.5 to 11
- extra_decay: float32 [2, 4, 2048], P(None, None, 'sp'), may hold values from -2.1 to 0
- norm_gain: float32 [512], replicated, may hold values from 0.1 to 1.9
- out_weight: bfloat16 [2048, 2048], P('tp'), may hold values from -0.25 to 0.25
- final_gain: float32 [2048], replicated, may hold values from 0.1 to 1.9
- final_bias: float32 [2048], replicated, may hold values from -1.5 to 1.5
Outputs:
- output: bfloat16 [4096, 2048], P(('grp', 'sp', 'tp')), parts along dimension 0
The draws below stay inside these ranges and needn't reach their ends.
There are 2 independent parts, one for each index of `grp`. The reference program is written for one: setup_inputs(seed, part) draws one part's arguments, and reference() takes and returns one part's arrays. A program takes and returns all parts, laid end to end along the dimension named above; an argument that names none is the same for every part. Nothing has to cross between parts.
All inputs are finite; a program needn't handle non-finite values.
Results may differ from the reference program's by a relative error of at most 0.012.
The reference program's roundings to bfloat16 on the way count: a program that leaves them out, or rounds other values in their place, can miss the bound.
Values may be sent and summed in bfloat16 or wider, within the bound.
A program may use at most 64 MiB of HBM per device.

```python
import math
import jax
import jax.numpy as jnp
from jax import lax

D = 2048
ATTENTION_HEADS = 4
DK = 256
DV = 512
RANK = 16
BLOCK = 64
GRID_W = 64
CTX = 512
TOK_SP = 512
LATENT_TOKENS = 2048
QK = 1024
VD = 2048


def draw_value_weight(key, part):
    noise = jax.random.truncated_normal(key, -4.0, 4.0, (D, ATTENTION_HEADS * DV), jnp.float32)
    column = (jnp.arange(ATTENTION_HEADS * DV) % DV).astype(jnp.float32)
    rising = 4.0 ** (column / DV)
    return (noise * rising * (0.6 / math.sqrt(D))).astype(jnp.bfloat16)


def draw_decay_bias(key, part):
    choose_key, slow_key, fast_key = jax.random.split(key, 3)
    fast_share = 0.5
    picked = jax.random.uniform(choose_key, (2, ATTENTION_HEADS * DK), jnp.float32) < fast_share
    slow_values = jax.random.uniform(slow_key, (2, ATTENTION_HEADS * DK), jnp.float32, 9.0, 11.0)
    fast_values = jax.random.uniform(fast_key, (2, ATTENTION_HEADS * DK), jnp.float32, 0.5, 2.0)
    return jnp.where(picked, fast_values, slow_values)


def draw_extra_decay(key, part):
    rate_key, location_key, keep_key = jax.random.split(key, 3)
    blocks = LATENT_TOKENS // TOK_SP
    rate_values = jnp.exp(jax.random.uniform(rate_key, (2, ATTENTION_HEADS, blocks), jnp.float32, math.log(0.15), math.log(0.9)))
    stable_part = -jnp.repeat(rate_values, TOK_SP, axis=2) / LATENT_TOKENS
    spike_locations = jax.random.randint(location_key, (2, ATTENTION_HEADS, 3), 0, LATENT_TOKENS)
    retain_fraction = jax.random.uniform(keep_key, (2, ATTENTION_HEADS, 3), jnp.float32, 0.5, 0.8)
    token_places = jnp.arange(LATENT_TOKENS)
    match_lookup = token_places[None, None, None, :] == spike_locations[:, :, :, None]
    spike_events = jnp.sum(jnp.where(match_lookup, jnp.log(retain_fraction)[:, :, :, None], 0.0), axis=2)
    return stable_part + spike_events


def steps_of(key, extent, cuts, least, high):
    def one(position, shards_of):
        heights = jax.random.uniform(jax.random.fold_in(jax.random.fold_in(key, 6), position), (shards_of,), jnp.float32, least / len(cuts), high / len(cuts))
        return jnp.repeat(jnp.exp(heights), extent[position] // shards_of).reshape((-1,) + (1,) * (len(extent) - position - 1))

    loudness = one(*cuts[0])
    for cut in cuts[1:]:
        loudness = loudness * one(*cut)
    return loudness


def gaussian(key, dims, scale, limit, pieces=(), kind=jnp.bfloat16):
    values = scale * jax.random.normal(key, dims, jnp.float32)
    if pieces:
        values = values * steps_of(key, dims, pieces, -0.22, 0.18)
    return jnp.clip(values, -limit, limit).astype(kind)


def setup_inputs(seed: int = 0, part: int = 0) -> dict:
    seeds = jax.random.split(jax.random.key(seed), 19)
    own_keys = jax.random.split(jax.random.fold_in(seeds[18], part), 19)
    return {
        "latent": gaussian(own_keys[0], (LATENT_TOKENS, D), 0.5, 3.0, ((0, 16),)),
        "context": gaussian(own_keys[1], (CTX, D), 1.0, 6.0, ((0, 4),)),
        "condition": gaussian(own_keys[2], (D,), 1.0, 6.0, ((0, 4),), jnp.float32),
        "context_condition": gaussian(seeds[3], (D,), 1.0, 6.0, ((0, 4),), jnp.float32),
        "mod_weight": gaussian(seeds[4], (D, 3 * D), (D // 2) ** -0.5, 0.1875, ((0, 4), (1, 4))),
        "mod_bias": gaussian(seeds[5], (3 * D,), 0.3, 1.5, (), jnp.float32),
        "query_weight": gaussian(seeds[6], (D, QK), D ** -0.5, 0.125, ((0, 4),)),
        "key_weight": gaussian(seeds[7], (D, QK), D ** -0.5, 0.125, ((0, 4),)),
        "value_weight": draw_value_weight(jax.random.fold_in(seeds[18], 71), part),
        "out_gate_weight": gaussian(seeds[9], (D, VD), D ** -0.5, 0.125, ((1, 4),)),
        "decay_in_weight": gaussian(seeds[10], (D, 2 * RANK), D ** -0.5, 0.125),
        "decay_weight": gaussian(seeds[11], (2, RANK, QK), RANK ** -0.5, 1.5),
        "decay_bias": draw_decay_bias(jax.random.fold_in(seeds[18], 71), part),
        "extra_decay": draw_extra_decay(jax.random.fold_in(seeds[18], 71), part),
        "norm_gain": jnp.clip(1.0 + 0.18 * jax.random.normal(seeds[14], (DV,), jnp.float32), 0.1, 1.9),
        "out_weight": gaussian(seeds[15], (VD, D), (VD // 4) ** -0.5, 0.25, ((0, 4),)),
        "final_gain": jnp.clip(1.0 + 0.18 * jax.random.normal(seeds[16], (D,), jnp.float32), 0.1, 1.9),
        "final_bias": gaussian(seeds[17], (D,), 0.3, 1.5, (), jnp.float32),
    }


norm_eps = 1e-05
gate_scale = 16.0
rope_base = 10000.0
residual_scale = 2.0 ** 0.5
highest = lax.Precision.HIGHEST

def rotate_half(values, angle):
    half_width = values.shape[-1] // 2
    first_half = values[..., :half_width]
    second_half = values[..., half_width:]
    cosine = jnp.cos(angle)
    sine_part = jnp.sin(angle)
    return jnp.concatenate([first_half * cosine - second_half * sine_part, first_half * sine_part + second_half * cosine], axis=-1)

def rotary(values, token_places):
    quarter = values.shape[-1] // 4
    frequency = rope_base ** (-jnp.arange(quarter, dtype=jnp.float32) / quarter)
    row_index = (token_places // GRID_W).astype(jnp.float32)
    col_index = (token_places % GRID_W).astype(jnp.float32)
    half_width = 2 * quarter
    by_row = rotate_half(values[..., :half_width], row_index[:, None] * frequency)
    by_col = rotate_half(values[..., half_width:], col_index[:, None] * frequency)
    return jnp.concatenate([by_row, by_col], axis=-1)

def log_decays(low_rank, decay_weight, decay_bias):
    rank_width = decay_weight.shape[1]
    decay_parts = []
    for direction in range(2):
        logits = jnp.dot(low_rank[:, direction * rank_width:(direction + 1) * rank_width], decay_weight[direction], preferred_element_type=jnp.float32) + decay_bias[direction]
        decay_parts.append(jax.nn.log_sigmoid(logits) / gate_scale)
    return decay_parts

def by_head(rows, size):
    return rows.astype(jnp.float32).reshape(rows.shape[0], -1, size).transpose(1, 0, 2)

def flip_rows(values):
    return jnp.flip(values, axis=1)

def end_state(key_heads, value_heads, logdec):
    cumulative = jnp.cumsum(logdec, axis=1)
    weights = jnp.exp(cumulative[:, -1:] - cumulative)
    return jnp.einsum('hnd,hnv->hdv', key_heads * weights, value_heads, precision=highest)

def blocked_scan(queries, key_heads, value_heads, logdec, start):
    heads, length, unused_width = queries.shape
    block_count = length // BLOCK
    lower_mask = jnp.tril(jnp.ones((BLOCK, BLOCK), dtype=bool))

    def blocks(values):
        return jnp.moveaxis(values.reshape(heads, block_count, BLOCK, values.shape[-1]), 1, 0)

    def advance(carry_state, block_data):
        query_block, key_block, value_block, decay_block = block_data
        cumulative = jnp.cumsum(decay_block, axis=1)
        total_decay = cumulative[:, -1:]
        query_decayed = query_block * jnp.exp(cumulative)
        key_inverse = key_block * jnp.exp(-cumulative)
        key_closing = key_block * jnp.exp(total_decay - cumulative)
        scores = jnp.einsum('hcd,hsd->hcs', query_decayed, key_inverse, precision=highest)
        scores = jnp.where(lower_mask[None], scores, 0.0)
        outputs = jnp.einsum('hcs,hsv->hcv', scores, value_block, precision=highest) + jnp.einsum('hcd,hdv->hcv', query_decayed, carry_state, precision=highest)
        carry_state = jnp.exp(total_decay)[:, 0, :, None] * carry_state + jnp.einsum('hcd,hcv->hdv', key_closing, value_block, precision=highest)
        return (carry_state, outputs)
    unused_state, outputs = lax.scan(advance, start, (blocks(queries), blocks(key_heads), blocks(value_heads), blocks(logdec)))
    return jnp.moveaxis(outputs, 0, 1).reshape(heads, length, value_heads.shape[-1])

def reference(latent, context, condition, context_condition, mod_weight, mod_bias, query_weight, key_weight, value_weight, out_gate_weight, decay_in_weight, decay_weight, decay_bias, extra_decay, norm_gain, out_weight, final_gain, final_bias):
    model_width = latent.shape[1]
    activated = jax.nn.silu(jnp.stack([condition, context_condition])).astype(jnp.bfloat16)
    modulation = jnp.dot(activated, mod_weight, preferred_element_type=jnp.float32) + mod_bias
    shifts = modulation[:, :model_width]
    scales = modulation[:, model_width:2 * model_width]
    branch_gate = modulation[0, 2 * model_width:]
    mod_latent = (latent.astype(jnp.float32) * (1.0 + scales[0]) + shifts[0]).astype(jnp.bfloat16)
    mod_context = (context.astype(jnp.float32) * (1.0 + scales[1]) + shifts[1]).astype(jnp.bfloat16)

    def project(rows, weight):
        return jnp.dot(rows, weight, preferred_element_type=jnp.float32).astype(jnp.bfloat16)
    queries = project(mod_latent, query_weight)
    out_gate = project(mod_latent, out_gate_weight)
    key_rows = project(mod_latent, key_weight)
    value_rows = project(mod_latent, value_weight)
    low_rank = project(mod_latent, decay_in_weight)
    context_keys = project(mod_context, key_weight)
    context_values = project(mod_context, value_weight)
    context_low = project(mod_context, decay_in_weight)
    token_places = jnp.arange(LATENT_TOKENS, dtype=jnp.int32)
    query_heads = rotary(by_head(queries, DK) * DK ** (-0.5), token_places)
    key_heads = rotary(by_head(key_rows, DK), token_places)
    value_heads = by_head(value_rows, DV)
    latent_decay = log_decays(low_rank, decay_weight, decay_bias)
    forward_decay = by_head(latent_decay[0], DK) + extra_decay[0][:, :, None]
    backward_decay = by_head(latent_decay[1], DK) + extra_decay[1][:, :, None]
    context_decay = log_decays(context_low, decay_weight, decay_bias)
    ctx_key_heads = by_head(context_keys, DK)
    ctx_value_heads = by_head(context_values, DV)
    start_forward = end_state(ctx_key_heads, ctx_value_heads, by_head(context_decay[0], DK))
    start_backward = end_state(flip_rows(ctx_key_heads), flip_rows(ctx_value_heads), flip_rows(by_head(context_decay[1], DK)))
    out_forward = blocked_scan(query_heads, key_heads, value_heads, forward_decay, start_forward)
    out_backward = flip_rows(blocked_scan(flip_rows(query_heads), flip_rows(key_heads), flip_rows(value_heads), flip_rows(backward_decay), start_backward))
    mixture = out_forward + out_backward
    normed = mixture * lax.rsqrt(lax.optimization_barrier(jnp.mean(mixture * mixture, axis=-1, keepdims=True)) + norm_eps) * norm_gain
    normed = normed.transpose(1, 0, 2).reshape(LATENT_TOKENS, ATTENTION_HEADS * DV)
    gated_rows = (normed * jax.nn.silu(out_gate.astype(jnp.float32))).astype(jnp.bfloat16)
    branch = jnp.dot(gated_rows, out_weight, preferred_element_type=jnp.float32)
    summed = residual_scale * latent.astype(jnp.float32) + branch_gate * branch
    row_mean = lax.optimization_barrier(jnp.mean(summed, axis=1, keepdims=True))
    centered = summed - row_mean
    variance = lax.optimization_barrier(jnp.mean(centered * centered, axis=1, keepdims=True))
    return (centered * lax.rsqrt(variance + norm_eps) * final_gain + final_bias).astype(jnp.bfloat16)
```

```python
import functools
from typing import Any, NamedTuple

import jax
import jax.numpy as jnp
from jax import lax
from jax.experimental import pallas as pl
from jax.experimental.pallas import tpu as pltpu
from jax.sharding import PartitionSpec as P

ATTENTION_HEADS = 4
DV = 512
BLOCK = 64
GRID_W = 64


norm_eps = 1e-05
gate_scale = 16.0
rope_base = 10000.0
residual_scale = 2.0**0.5
highest = lax.Precision.HIGHEST
f32 = jnp.float32
bf16 = jnp.bfloat16


def rope_tables(token_places, width):
    quarter = width // 4
    frequency = rope_base ** (-jnp.arange(quarter, dtype=f32) / quarter)
    row_angle = (token_places // GRID_W).astype(f32)[:, None] * frequency
    col_angle = (token_places % GRID_W).astype(f32)[:, None] * frequency
    cosine = jnp.concatenate([jnp.cos(row_angle)] * 2 + [jnp.cos(col_angle)] * 2, axis=1)
    row_sine, col_sine = jnp.sin(row_angle), jnp.sin(col_angle)
    sine = jnp.concatenate([-row_sine, row_sine, -col_sine, col_sine], axis=1)
    return cosine, sine


def dot(a, b, contract=((1,), (0,)), precision=None):
    return lax.dot_general(a, b, (contract, ((), ())), precision=precision,
                           preferred_element_type=f32)


def log_sigmoid(x):
    return jnp.minimum(x, 0.0) - jnp.log1p(jnp.exp(-jnp.abs(x)))


def rotate(x, cosine, sine):
    half = x.shape[1] // 2
    parts = [pltpu.roll(x[:, i * half:(i + 1) * half], half // 2, 1) for i in range(2)]
    return x * cosine + jnp.concatenate(parts, axis=1) * sine


def triangle(size, reverse):
    row = lax.broadcasted_iota(jnp.int32, (size, size), 0)
    col = lax.broadcasted_iota(jnp.int32, (size, size), 1)
    return row <= col if reverse else row >= col


def decay_block(low, decay_weight, decay_bias, direction):
    rank = decay_weight.shape[1]
    logits = dot(low[:, direction * rank:(direction + 1) * rank], decay_weight[direction])
    return log_sigmoid(logits + decay_bias[direction:direction + 1, :]) / gate_scale


def context_kernel(k_ref, v_ref, low_ref, dw_ref, db_ref, state_ref):
    length, width = k_ref.shape
    size = min(2 * BLOCK, length)
    count = length // size
    for direction in range(2):
        mask = triangle(size, direction == 1).astype(f32)
        edge = 0 if direction == 1 else size - 1
        state = None
        for step in range(count):
            b = count - 1 - step if direction == 1 else step
            rows = slice(b * size, (b + 1) * size)
            logdec = decay_block(low_ref[rows, :], dw_ref[...], db_ref[...], direction)
            cum = dot(mask, logdec, precision=highest)
            total = cum[edge:edge + 1, :]
            closing = (k_ref[rows, :].astype(f32) * jnp.exp(total - cum)).astype(bf16)
            term = dot(closing, v_ref[rows, :], ((0,), (0,)))
            state = term if state is None else jnp.exp(total).T * state + term
        state_ref[direction] = state


def local_kernel(q_ref, k_ref, v_ref, low_ref, extra_ref, dw_ref, db_ref, cos_ref, sin_ref,
                 out_ref, qc_ref, state_ref, total_ref):
    length, width = q_ref.shape
    size = 2 * BLOCK
    count = length // size
    rq, rk, within, scores = [], [], [], []
    for b in range(count):
        rows = slice(b * size, (b + 1) * size)
        cosine, sine = cos_ref[rows, :], sin_ref[rows, :]
        rq.append(rotate(q_ref[rows, :].astype(f32) * width ** -0.5, cosine, sine))
        rk.append(rotate(k_ref[rows, :].astype(f32), cosine, sine))
        scores.append(None)
    for direction in range(2):
        keep = triangle(size, direction == 1)
        mask = keep.astype(f32)
        edge = 0 if direction == 1 else size - 1
        middle = size // 2 if direction == 1 else size // 2 - 1
        state = None
        before = None
        for step in range(count):
            b = count - 1 - step if direction == 1 else step
            rows = slice(b * size, (b + 1) * size)
            logdec = decay_block(low_ref[rows, :], dw_ref[...], db_ref[...], direction)
            logdec = logdec + extra_ref[rows, direction:direction + 1]
            cum = dot(mask, logdec, precision=highest)
            total = cum[edge:edge + 1, :]
            center = cum[middle:middle + 1, :]
            q_mid = (rq[b] * jnp.exp(cum - center)).astype(bf16)
            k_mid = (rk[b] * jnp.exp(center - cum)).astype(bf16)
            score = jnp.where(keep, dot(q_mid, k_mid, ((1,), (1,))), 0.0)
            q_dec = rq[b] * jnp.exp(cum)
            if direction == 0:
                scores[b] = score
                out = None
            else:
                out = dot((scores[b] + score).astype(bf16), v_ref[rows, :])
            if state is not None:
                carried = dot(q_dec.astype(bf16), state.astype(bf16))
                out = carried if out is None else out + carried
            if direction == 0:
                out_ref[rows, :] = jnp.zeros((size, v_ref.shape[1]), f32) if out is None else out
            else:
                out_ref[rows, :] += out
            q_all = q_dec if before is None else q_dec * jnp.exp(before)
            qc_ref[rows, direction * width:(direction + 1) * width] = q_all.astype(bf16)
            closing = (rk[b] * jnp.exp(total - cum)).astype(bf16)
            term = dot(closing, v_ref[rows, :], ((0,), (0,)))
            state = term if state is None else jnp.exp(total).T * state + term
            before = total if before is None else before + total
        state_ref[direction * width:(direction + 1) * width, :] = state.astype(bf16)
        total_ref[direction:direction + 1, :] = before


def join_kernel(final, out_ref, qc_ref, states_ref, totals_ref, start_ref, gate_ref, gain_ref,
                place_ref, result_ref):
    count = states_ref.shape[0]
    width = qc_ref.shape[1] // 2
    place = place_ref[...]
    mixture = out_ref[...]
    for direction in range(2):
        state = start_ref[direction]
        for lap in range(count):
            j = count - 1 - lap if direction == 1 else lap
            decay = jnp.exp(totals_ref[j, direction:direction + 1, :]).T
            joined = decay * state + states_ref[
                j, direction * width:(direction + 1) * width, :].astype(f32)
            ahead = place < j if direction == 1 else place > j
            state = jnp.where(ahead, joined, state)
        mixture = mixture + dot(qc_ref[:, direction * width:(direction + 1) * width],
                                state.astype(bf16))
    if final:
        squares = jnp.mean(mixture * mixture, axis=1, keepdims=True)
        gate = gate_ref[...].astype(f32)
        normed = mixture * lax.rsqrt(squares + norm_eps) * gain_ref[...]
        result_ref[...] = (normed * (gate / (1.0 + jnp.exp(-gate)))).astype(bf16)
    else:
        result_ref[...] = mixture


def call(kernel, out_shape, *args):
    return pl.pallas_call(
        kernel,
        out_shape=out_shape,
        in_specs=[pl.BlockSpec(memory_space=pltpu.VMEM)] * len(args),
        out_specs=jax.tree.map(lambda _: pl.BlockSpec(memory_space=pltpu.VMEM), out_shape),
        compiler_params=pltpu.CompilerParams(vmem_limit_bytes=48 * 1024 * 1024),
        cost_estimate=pl.CostEstimate(flops=4_000_000_000, bytes_accessed=4_000_000,
                                      transcendentals=1_000_000),
    )(*args)


MESH = pl.DeviceIdType.MESH


def remote(src, dst, send_sem, recv_sem, axis, target):
    return pltpu.make_async_remote_copy(
        src_ref=src, dst_ref=dst, send_sem=send_sem, recv_sem=recv_sem,
        device_id={axis: target}, device_id_type=MESH)


class Line:
    def __init__(self, place, count, axis, target_of, view, chunks, send_sem, recv_sem):
        self.place, self.count, self.axis, self.target_of = place, count, axis, target_of
        self.view, self.chunks, self.send_sem, self.recv_sem = view, chunks, send_sem, recv_sem

    def copy(self, way, hop, chunk, block, target):
        ref = self.view(block, chunk)
        return remote(ref, ref, self.send_sem.at[way, hop, chunk],
                      self.recv_sem.at[way, hop, chunk], self.axis, self.target_of(target))

    def outgoing(self, way, hop):
        place, count = self.place, self.count
        if way == 0:
            return place - hop, place + 1, jnp.logical_and(place >= hop, place < count - 1)
        return place + hop, place - 1, jnp.logical_and(place + hop < count, place > 0)

    def each_send(self, way, hop, chunk, act):
        block, target, valid = self.outgoing(way, hop)

        @pl.when(valid)
        def _():
            act(self.copy(way, hop, chunk, block, target))

    def send(self, way, hop, chunk):
        self.each_send(way, hop, chunk, lambda c: c.start())

    def drain(self):
        for way in range(2):
            for hop in range(self.count - 1):
                for chunk in range(self.chunks):
                    self.each_send(way, hop, chunk, lambda c: c.wait_send())

    def arrive(self, way, hop, chunk, then=None):
        if way == 0:
            block, source, valid = self.place - 1 - hop, self.place - 1, self.place > hop
        else:
            block, source = self.place + 1 + hop, self.place + 1
            valid = self.place + 1 + hop < self.count

        @pl.when(valid)
        def _():
            self.copy(way, hop, chunk, block, source).wait_recv()
            if then is not None:
                then(block)

    def forward(self, hop, then=None):
        for chunk in range(self.chunks):
            for way in range(2):
                self.arrive(way, hop, chunk, None if then is None else functools.partial(then, way))
                if hop + 1 < self.count - 1:
                    self.send(way, hop + 1, chunk)


def open_kernel(partners):
    barrier = pltpu.get_barrier_semaphore()
    for axis, target in partners:
        pl.semaphore_signal(barrier, inc=1, device_id={axis: target}, device_id_type=MESH)
    return lambda: pl.semaphore_wait(barrier, len(partners))


def others(axis):
    count, place = lax.axis_size(axis), lax.axis_index(axis)
    return [lax.rem(place + k, count) for k in range(1, count)]


def sources(axis):
    count, place = lax.axis_size(axis), lax.axis_index(axis)
    return [lax.rem(place + count - k, count) for k in range(1, count)]


def spread(buffer, axis, send_sem, recv_sem):
    place = lax.axis_index(axis)
    for k, target in enumerate(others(axis)):
        remote(buffer.at[place], buffer.at[place], send_sem.at[k], recv_sem.at[k],
               axis, target).start()


def spread_arrive(buffer, axis, send_sem, recv_sem):
    for k, source in enumerate(sources(axis)):
        remote(buffer.at[source], buffer.at[source], send_sem.at[k], recv_sem.at[k],
               axis, source).wait_recv()


def spread_drain(buffer, axis, send_sem, recv_sem):
    place = lax.axis_index(axis)
    for k, target in enumerate(others(axis)):
        remote(buffer.at[place], buffer.at[place], send_sem.at[k], recv_sem.at[k],
               axis, target).wait_send()


def enter_kernel(chunks, latent_ref, context_ref, cond_ref, mw_ref, mb_ref, qw_ref, kw_ref,
                 ml_ref, mc_ref, gate_ref, qk_ref,
                 rows_ref, part_ref, sums_ref, zs, zr, xs, xr, cs, cr, ps, pr, ss, sr):
    sp, sp_count = lax.axis_index("sp"), lax.axis_size("sp")
    tp, tp_count = lax.axis_index("tp"), lax.axis_size("tp")
    own, model_width = latent_ref.shape
    depth = qw_ref.shape[0]
    head_keys = qk_ref.shape[1] // 2
    ready = open_kernel([("sp", t) for t in others("sp")] + [("tp", t) for t in others("tp")])
    v = cond_ref[...]
    activated = (v / (1.0 + jnp.exp(-v))).astype(bf16)
    part_ref[sp] = dot(activated, mw_ref[...])
    columns = pl.ds(pl.multiple_of((tp // (tp_count // ATTENTION_HEADS)) * head_keys, head_keys),
                    head_keys)
    qk_rows = pl.ds(pl.multiple_of(sp * depth, depth), depth)
    qk_ref[qk_rows, :head_keys] = qw_ref[:, columns]
    qk_ref[qk_rows, head_keys:] = kw_ref[:, columns]
    rows_ref[pl.ds(pl.multiple_of(tp * own, own), own), :] = latent_ref[...]

    step = depth // chunks
    z_line = Line(
        sp, sp_count, "sp", lambda p: p,
        lambda block, chunk: qk_ref.at[
            pl.ds(pl.multiple_of(block * depth + chunk * step, step), step), :],
        chunks, zs, zr)
    x_count = tp_count // 2
    x, core = tp // 2, tp % 2

    def rows_of(block, chunk):
        return rows_ref.at[pl.ds(pl.multiple_of((2 * block + core) * own, own), own), :]

    x_line = Line(x, x_count, "tp", lambda p: 2 * p + core, rows_of, 1, xs, xr)
    sibling = tp + 1 - 2 * core

    def cross(block, slot, other=False):
        side = 1 - core if other else core
        ref = rows_ref.at[pl.ds(pl.multiple_of((2 * block + side) * own, own), own), :]
        return remote(ref, ref, cs.at[slot], cr.at[slot], "tp", sibling)

    def slot_of(way, hop):
        return 1 + way * (x_count - 1) + hop

    ready()
    spread(part_ref, "sp", ps, pr)
    for way in range(2):
        x_line.send(way, 0, 0)
    cross(x, 0).start()
    for chunk in range(chunks):
        for way in range(2):
            z_line.send(way, 0, chunk)
    spread_arrive(part_ref, "sp", ps, pr)
    total = part_ref[0]
    for j in range(1, sp_count):
        total = total + part_ref[j]
    sums_ref[tp] = total
    spread(sums_ref, "tp", ss, sr)
    z_line.forward(0)
    for hop in range(x_count - 1):
        x_line.forward(hop, lambda way, block, hop=hop: cross(block, slot_of(way, hop)).start())
    if sp_count > 2:
        z_line.forward(1)
    spread_arrive(sums_ref, "tp", ss, sr)
    modulation = jnp.concatenate([sums_ref[j] for j in range(tp_count)], axis=1) + mb_ref[...]
    shifts = modulation[:, :model_width]
    scales = modulation[:, model_width:2 * model_width]
    gate_ref[...] = modulation[0:1, 2 * model_width:]
    mc_ref[...] = (context_ref[...].astype(f32) * (1.0 + scales[1:2]) + shifts[1:2]).astype(bf16)

    def each_cross(act_own, act_line):
        act_own()
        for way in range(2):
            for hop in range(x_count - 1):
                block = x - 1 - hop if way == 0 else x + 1 + hop
                valid = x > hop if way == 0 else x + 1 + hop < x_count

                @pl.when(valid)
                def _():
                    act_line(block, slot_of(way, hop))

    each_cross(lambda: cross(x, 0, True).wait_recv(),
               lambda block, slot: cross(block, slot, True).wait_recv())
    for j in range(tp_count):
        rows = slice(j * own, (j + 1) * own)
        ml_ref[rows, :] = (rows_ref[rows, :].astype(f32) * (1.0 + scales[0:1])
                           + shifts[0:1]).astype(bf16)
    for hop in range(2, sp_count - 1):
        z_line.forward(hop)
    each_cross(lambda: cross(x, 0).wait_send(),
               lambda block, slot: cross(block, slot).wait_send())
    spread_drain(part_ref, "sp", ps, pr)
    spread_drain(sums_ref, "tp", ss, sr)
    x_line.drain()
    z_line.drain()


def comm_call(kernel, out_shape, scratch, collective_id, *args):
    return pl.pallas_call(
        kernel,
        out_shape=out_shape,
        in_specs=[pl.BlockSpec(memory_space=pltpu.VMEM)] * len(args),
        out_specs=jax.tree.map(lambda _: pl.BlockSpec(memory_space=pltpu.VMEM), out_shape),
        scratch_shapes=scratch,
        compiler_params=pltpu.CompilerParams(
            vmem_limit_bytes=48 * 1024 * 1024, collective_id=collective_id,
            has_side_effects=True),
        cost_estimate=pl.CostEstimate(flops=20_000_000_000, bytes_accessed=60_000_000,
                                      transcendentals=1_000_000),
    )(*args)


def enter(latent, context, cond, mod_weight, mod_bias, query_weight, key_weight):
    sp_count, tp_count = lax.axis_size("sp"), lax.axis_size("tp")
    own, model_width = latent.shape
    depth = query_weight.shape[0]
    head_keys = query_weight.shape[1] // ATTENTION_HEADS
    chunks = 4
    sds = jax.ShapeDtypeStruct
    dma = pltpu.SemaphoreType.DMA
    x_hops = tp_count // 2 - 1
    return comm_call(
        functools.partial(enter_kernel, chunks),
        (
            sds((own * tp_count, model_width), bf16),
            sds(context.shape, bf16),
            sds((1, model_width), f32),
            sds((depth * sp_count, 2 * head_keys), bf16),
        ),
        [
            pltpu.VMEM((own * tp_count, model_width), bf16),
            pltpu.VMEM((sp_count, 2, mod_weight.shape[1]), f32),
            pltpu.VMEM((tp_count, 2, mod_weight.shape[1]), f32),
            dma((2, sp_count - 1, chunks)), dma((2, sp_count - 1, chunks)),
            dma((2, x_hops, 1)), dma((2, x_hops, 1)),
            dma((1 + 2 * x_hops,)), dma((1 + 2 * x_hops,)),
            dma((sp_count - 1,)), dma((sp_count - 1,)),
            dma((tp_count - 1,)), dma((tp_count - 1,)),
        ],
        1, latent, context, cond, mod_weight, mod_bias[None, :], query_weight, key_weight,
    )


def project(rows, weight):
    return jnp.dot(rows, weight, preferred_element_type=f32).astype(bf16)


def body(
    latent,
    context,
    condition,
    context_condition,
    mod_weight,
    mod_bias,
    query_weight,
    key_weight,
    value_weight,
    out_gate_weight,
    decay_in_weight,
    decay_weight,
    decay_bias,
    extra_decay,
    norm_gain,
    out_weight,
    final_gain,
    final_bias,
):
    head_keys = query_weight.shape[1] // ATTENTION_HEADS
    value_cols = value_weight.shape[1]
    tp_index = lax.axis_index("tp")
    sp_index = lax.axis_index("sp")
    head_share = lax.axis_size("tp") // ATTENTION_HEADS
    head_index = tp_index // head_share
    part_index = tp_index % head_share
    key_start = head_index * head_keys

    full_out = lax.all_gather(out_weight, "tp", axis=0, tiled=True)
    mod_latent, mod_context, branch_gate, qk_head = enter(
        latent, context, jnp.stack([condition, context_condition]), mod_weight, mod_bias,
        query_weight, key_weight,
    )
    context_local = jnp.concatenate(
        [
            project(mod_context, qk_head[:, head_keys:]),
            project(mod_context, value_weight),
            project(mod_context, decay_in_weight),
        ],
        axis=1,
    )
    gathered_context = lax.all_gather(context_local, "sp", axis=0, tiled=True)
    qk = project(mod_latent, qk_head)
    value_rows = project(mod_latent, value_weight)
    out_gate = project(mod_latent, out_gate_weight)
    low_rank = project(mod_latent, decay_in_weight)
    count = mod_latent.shape[0]
    token_places = sp_index * count + jnp.arange(count, dtype=jnp.int32)
    cosine, sine = rope_tables(token_places, head_keys)
    head_bias = lax.dynamic_slice_in_dim(decay_bias, key_start, head_keys, 1)
    head_gate = lax.dynamic_slice_in_dim(decay_weight, key_start, head_keys, 2)
    head_extra = lax.dynamic_index_in_dim(extra_decay, head_index, 1, keepdims=False).T

    sds = jax.ShapeDtypeStruct
    out_local, qc, states, totals = call(
        local_kernel,
        (
            sds((count, value_cols), f32),
            sds((count, 2 * head_keys), bf16),
            sds((2 * head_keys, value_cols), bf16),
            sds((2, head_keys), f32),
        ),
        qk[:, :head_keys], qk[:, head_keys:], value_rows, low_rank, head_extra, head_gate,
        head_bias, cosine, sine,
    )
    start = call(
        context_kernel,
        sds((2, head_keys, value_cols), f32),
        gathered_context[:, :head_keys],
        gathered_context[:, head_keys : head_keys + value_cols],
        gathered_context[:, head_keys + value_cols :],
        head_gate, head_bias,
    )
    states, totals, full_out = lax.optimization_barrier((states, totals, full_out))
    all_states = lax.all_gather(states, "sp")
    all_totals = lax.all_gather(totals, "sp")
    place = jnp.full((1, value_cols), sp_index, jnp.int32)
    gain_slice = lax.dynamic_slice_in_dim(norm_gain, part_index * value_cols, value_cols, 0)
    final = head_share == 1
    joined = call(
        functools.partial(join_kernel, final),
        sds((count, value_cols), bf16 if final else f32),
        out_local, qc, all_states, all_totals, start, out_gate, gain_slice[None, :], place,
    )
    if final:
        gated_rows = joined
    else:
        squares = jnp.sum(joined * joined, axis=1)
        onehot = (jnp.arange(ATTENTION_HEADS) == head_index).astype(f32)
        sums = lax.psum(onehot[:, None] * squares[None, :], "tp")
        head_sum = jnp.sum(sums * onehot[:, None], axis=0)
        normed = joined * lax.rsqrt(head_sum / DV + norm_eps)[:, None] * gain_slice
        gated_rows = (normed * jax.nn.silu(out_gate.astype(f32))).astype(bf16)
    regrouped = lax.all_to_all(gated_rows, "tp", split_axis=0, concat_axis=1, tiled=True)
    branch = jnp.dot(regrouped, full_out, preferred_element_type=f32)
    summed = residual_scale * latent.astype(f32) + branch_gate * branch
    row_mean = jnp.mean(summed, axis=1, keepdims=True)
    centered = summed - row_mean
    variance = jnp.mean(centered * centered, axis=1, keepdims=True)
    return (centered * lax.rsqrt(variance + norm_eps) * final_gain + final_bias).astype(bf16)


class Scratch(NamedTuple):
    cond: Any
    ctx_cond: Any
    mod_w: Any
    mod_b: Any
    wqk: Any
    rows: Any
    mod_latent: Any
    context: Any
    mod_context: Any
    low_w: Any
    value_w: Any
    gate_w: Any
    out_w: Any
    decay_w: Any
    decay_b: Any
    extra: Any
    norm_gain: Any
    final_gain: Any
    final_bias: Any
    part: Any
    sums: Any
    totals: Any
    shifts: Any
    scales: Any
    branch_gate: Any
    cosine: Any
    sine: Any
    ctx_close: Any
    ctx_value: Any
    low: Any
    value: Any
    gate: Any
    key: Any
    cum: Any
    ahead: Any
    total: Any
    start: Any
    state: Any
    carry: Any
    own_decay: Any
    ahead_decay: Any
    chain_in: Any
    chain_out: Any
    q_all: Any
    mixture: Any
    joined: Any
    gated: Any
    pair_out: Any
    pair_in: Any
    far_out: Any
    far_in: Any
    branch: Any
    load_sem: Any
    zs: Any
    zr: Any
    ys: Any
    yr: Any
    xs: Any
    xr: Any
    cs: Any
    cr: Any
    ps: Any
    pr: Any
    ts: Any
    tr: Any
    ss: Any
    sr: Any
    hs: Any
    hr: Any
    ds: Any
    dr: Any
    fs: Any
    fr: Any


def spread_of(ref, axis, send_sem, recv_sem):
    return (lambda: spread(ref, axis, send_sem, recv_sem),
            lambda: spread_arrive(ref, axis, send_sem, recv_sem),
            lambda: spread_drain(ref, axis, send_sem, recv_sem))


PARTS = 2


def fused_kernel(latent, context, cond, ctx_cond, mod_w, mod_b, query_w, key_w, value_w, gate_w,
                 low_w, decay_w, decay_b, extra, norm_gain, out_w, final_gain, final_bias,
                 out_ref, s):
    grp = lax.axis_index("grp")
    sp, sp_count = lax.axis_index("sp"), lax.axis_size("sp")
    tp, tp_count = lax.axis_index("tp"), lax.axis_size("tp")
    own, width = latent.shape
    depth = query_w.shape[0]
    keys = query_w.shape[1] // ATTENTION_HEADS
    vals = value_w.shape[1]
    count = own * tp_count
    size = 2 * BLOCK
    blocks = count // size
    ctx = context.shape[0]
    x, core = tp // 2, tp % 2
    sibling, across = tp + 1 - 2 * core, 2 * (1 - x) + core
    far_sibling = 2 * (1 - x) + 1 - core

    def block_rows(j):
        return pl.ds(pl.multiple_of(j * own, own), own)

    ready = open_kernel([("sp", t) for t in others("sp")] + [("tp", t) for t in others("tp")]
                        + [("grp", 1 - grp)])
    head_cols = pl.ds(pl.multiple_of(tp * keys, keys), keys)
    own_depth = pl.ds(pl.multiple_of(sp * depth, depth), depth)
    loads = []
    for i, (source, target) in enumerate((
        (cond, s.cond), (ctx_cond, s.ctx_cond),
        (mod_w, s.mod_w),
        (key_w.at[:, head_cols], s.wqk.at[0, own_depth, :]),
        (query_w.at[:, head_cols], s.wqk.at[1, own_depth, :]),
        (latent, s.rows.at[block_rows(tp), :]),
        (mod_b, s.mod_b), (context, s.context),
        (low_w, s.low_w), (value_w, s.value_w),
        (decay_w.at[:, :, head_cols], s.decay_w),
        (decay_b.at[:, head_cols], s.decay_b), (extra, s.extra),
        (gate_w, s.gate_w), (norm_gain, s.norm_gain),
        (out_w, s.out_w), (final_gain, s.final_gain),
        (final_bias, s.final_bias),
    )):
        loads.append(pltpu.make_async_copy(source, target, s.load_sem.at[i]))
        loads[i].start()
    (load_cond, load_ctx_cond, load_mod_w, load_key_w, load_query_w, load_latent,
     load_mod_b, load_context, load_low_w, load_value_w, load_decay_w, load_decay_b,
     load_extra, load_gate_w, load_norm_gain, load_out_w, load_final_gain, load_final_bias) = loads

    half = depth // 2
    step = half // PARTS

    def weight_view(side):
        def view(block, chunk):
            start = block * depth + side * half + (chunk % PARTS) * step
            return s.wqk.at[chunk // PARTS, pl.ds(pl.multiple_of(start, step), step), :]
        return view

    line = Line(sp, sp_count, "sp", lambda p: p, weight_view(grp), 2 * PARTS, s.zs, s.zr)
    other_view = weight_view(1 - grp)

    def y_copy(ref, way, hop, chunk):
        return remote(ref, ref, s.ys.at[way, hop, chunk], s.yr.at[way, hop, chunk],
                      "grp", 1 - grp)

    def z_arrive(hop, chunk):
        for way in range(2):
            line.arrive(way, hop, chunk, lambda block: y_copy(
                weight_view(grp)(block, chunk), way, hop, chunk).start())
            if hop + 1 < sp_count - 1:
                line.send(way, hop + 1, chunk)

    def y_each(hop, chunk, view, act):
        for way in range(2):
            block = sp - 1 - hop if way == 0 else sp + 1 + hop
            valid = sp > hop if way == 0 else sp + 1 + hop < sp_count

            @pl.when(valid)
            def _():
                act(y_copy(view(block, chunk), way, hop, chunk))

    key_chunks, query_chunks = range(PARTS), range(PARTS, 2 * PARTS)

    def send_own(chunks):
        for chunk in chunks:
            for way in range(2):
                line.send(way, 0, chunk)

    pieces = s.xs.shape[0]
    piece = own // pieces

    def rows_piece(j, p):
        return s.rows.at[pl.ds(pl.multiple_of(j * own + p * piece, piece), piece), :]

    def x_copy(j, p):
        return remote(rows_piece(j, p), rows_piece(j, p), s.xs.at[p], s.xr.at[p],
                      "tp", across)

    def cross(j, p, slot):
        k = slot * pieces + p
        return remote(rows_piece(j, p), rows_piece(j, p), s.cs.at[k], s.cr.at[k],
                      "tp", sibling)

    part_go, part_arrive, part_drain = spread_of(s.part, "sp", s.ps, s.pr)
    sums_go, sums_arrive, sums_drain = spread_of(s.sums, "tp", s.ss, s.sr)
    tot_go, tot_arrive, tot_drain = spread_of(s.totals, "sp", s.ts, s.tr)

    for load in (load_cond, load_ctx_cond, load_mod_w):
        load.wait()
    v = jnp.concatenate([s.cond[...], s.ctx_cond[...]], axis=0)
    activated = (v / (1.0 + jnp.exp(-v))).astype(bf16)
    s.part[sp] = dot(activated, s.mod_w[...])
    for load in (load_key_w, load_query_w, load_latent):
        load.wait()

    ready()
    part_go()
    send_own(key_chunks)
    send_own(query_chunks[:1])
    for p in range(pieces):
        if p < pieces // 2:
            x_copy(tp, p).start()
        cross(tp, p, 0).start()

    quarter = keys // 4

    def rope(b, carry):
        rows = pl.ds(pl.multiple_of(b * size, size), size)
        lane = lax.broadcasted_iota(jnp.int32, (1, keys), 1)
        index = jnp.bitwise_and(lane, quarter - 1).astype(f32)
        frequency = jnp.exp(index * (-jnp.log(rope_base) / quarter))
        by_row = lane < keys // 2
        first = jnp.bitwise_and(lane, 2 * quarter - 1) < quarter
        place = lax.broadcasted_iota(jnp.int32, (size, 1), 0) + (sp * count + b * size)
        place = place.astype(f32)
        row = jnp.floor((place + 0.5) * (1.0 / GRID_W))
        col = place - row * GRID_W
        angle = jnp.where(by_row, row, col) * frequency
        s.cosine[rows, :] = jnp.cos(angle)
        sine = jnp.sin(angle)
        s.sine[rows, :] = jnp.where(first, -sine, sine)
        return carry

    lax.fori_loop(0, blocks, rope, 0)

    @pl.when(sp == 0)
    def _():
        s.chain_in[0] = jnp.zeros(s.chain_in.shape[1:], bf16)

    @pl.when(sp == sp_count - 1)
    def _():
        s.chain_in[1] = jnp.zeros(s.chain_in.shape[1:], bf16)

    part_arrive()
    total = s.part[0]
    for j in range(1, sp_count):
        total = total + s.part[j]
    s.sums[tp] = total
    sums_go()
    for p in range(pieces // 2, pieces):
        x_copy(tp, p).start()
    for chunk in key_chunks:
        z_arrive(0, chunk)
    send_own(query_chunks[1:])
    sums_arrive()
    for load in (load_mod_b, load_context, load_low_w, load_value_w, load_decay_w, load_decay_b, load_extra):
        load.wait()
    modulation = (jnp.concatenate([s.sums[j] for j in range(tp_count)], axis=1)
                  + s.mod_b[...])
    s.shifts[...] = modulation[:, :width]
    s.scales[...] = 1.0 + modulation[:, width:2 * width]
    s.branch_gate[...] = modulation[0:1, 2 * width:]
    s.mod_context[...] = (s.context[...].astype(f32) * s.scales[1:2, :]
                             + s.shifts[1:2, :]).astype(bf16)

    def decay_of(low, direction):
        rank = s.decay_w.shape[1]
        logits = dot(low[:, direction * rank:(direction + 1) * rank], s.decay_w[direction])
        return log_sigmoid(logits + s.decay_b[direction:direction + 1, :]) / gate_scale

    ctx_low = dot(s.mod_context[...], s.low_w[...], ((1,), (1,))).astype(bf16)
    ctx_totals = []
    for direction in range(2):
        mask = triangle(ctx, direction == 1).astype(f32)
        edge = 0 if direction == 1 else ctx - 1
        cum = dot(mask, decay_of(ctx_low, direction), precision=highest)
        ctx_totals.append(cum[edge:edge + 1, :])
        s.ctx_close[direction] = jnp.exp(ctx_totals[direction] - cum)
    s.ctx_value[...] = dot(s.mod_context[...], s.value_w[...]).astype(bf16)
    load_gate_w.wait()

    def project_chip(chip):
        rows = pl.ds(pl.multiple_of(chip * 2 * own, 2 * own), 2 * own)
        mod = (s.rows[rows, :].astype(f32) * s.scales[0:1, :]
               + s.shifts[0:1, :]).astype(bf16)
        s.mod_latent[rows, :] = mod
        s.low[rows, :] = dot(mod, s.low_w[...], ((1,), (1,))).astype(bf16)
        s.value[rows, :] = dot(mod, s.value_w[...]).astype(bf16)
        s.gate[rows, :] = dot(mod, s.gate_w[...]).astype(bf16)

    for chunk in key_chunks:
        if sp_count > 2:
            z_arrive(1, chunk)
    for p in range(pieces):
        cross(tp, p, 0).wait_send()
        remote(rows_piece(sibling, p), rows_piece(sibling, p), s.cs.at[p], s.cr.at[p],
               "tp", sibling).wait_recv()
    project_chip(x)
    for chunk in query_chunks:
        z_arrive(0, chunk)
    for p in range(pieces):
        x_copy(across, p).wait_recv()
        cross(across, p, 1).start()
    for hop in range(2, sp_count - 1):
        for chunk in key_chunks:
            z_arrive(hop, chunk)
    for p in range(pieces):
        cross(far_sibling, p, 1).wait_recv()
    project_chip(1 - x)

    own_head = lax.broadcasted_iota(jnp.int32, (ATTENTION_HEADS, size), 0) == tp
    for direction in range(2):
        mask = triangle(size, direction == 1).astype(f32)
        edge = 0 if direction == 1 else size - 1
        before = None
        for turn in range(blocks):
            b = blocks - 1 - turn if direction == 1 else turn
            rows = slice(b * size, (b + 1) * size)
            head_extra = jnp.sum(jnp.where(own_head, s.extra[direction, :, rows], 0.0), axis=0,
                                 keepdims=True)
            added = jnp.sum(mask * head_extra, axis=1, keepdims=True)
            cum = dot(mask, decay_of(s.low[rows, :], direction), precision=highest) + added
            s.cum[direction, rows, :] = cum
            block_total = cum[edge:edge + 1, :]
            if before is not None:
                s.ahead[direction, b:b + 1, :] = before
            before = block_total if before is None else before + block_total
        s.total[direction:direction + 1, :] = before
    s.totals[sp] = jnp.concatenate([s.total[...]] + ctx_totals, axis=0)
    tot_go()

    for hop in range(sp_count - 1):
        for chunk in key_chunks:
            y_each(hop, chunk, other_view, lambda c: c.wait_recv())
    ctx_key = dot(s.mod_context[...], s.wqk[0]).astype(bf16).astype(f32)
    for direction in range(2):
        closing = (ctx_key * s.ctx_close[direction]).astype(bf16)
        s.carry[direction] = dot(closing, s.ctx_value[...], ((0,), (0,)))
    for b in range(blocks):
        rows = slice(b * size, (b + 1) * size)
        key = dot(s.mod_latent[rows, :], s.wqk[0]).astype(bf16)
        s.key[rows, :] = rotate(key.astype(f32), s.cosine[rows, :], s.sine[rows, :])
    if sp_count > 2:
        for chunk in query_chunks:
            z_arrive(1, chunk)
    for direction in range(2):
        edge = 0 if direction == 1 else size - 1
        state = None
        for turn in range(blocks):
            b = blocks - 1 - turn if direction == 1 else turn
            rows = slice(b * size, (b + 1) * size)
            cum = s.cum[direction, rows, :]
            block_total = cum[edge:edge + 1, :]
            closing = (s.key[rows, :] * jnp.exp(block_total - cum)).astype(bf16)
            term = dot(closing, s.value[rows, :], ((0,), (0,)))
            if state is None:
                state = term
            else:
                s.start[direction, b] = state.astype(bf16)
                state = jnp.exp(block_total).T * state + term
        s.state[direction] = state
    tot_arrive()
    chunk_width = s.chain_in.shape[3]
    chunk_count = s.chain_in.shape[1]

    def column(row):
        return jnp.broadcast_to(jnp.exp(row).T, (keys, chunk_width))

    for direction in range(2):
        ahead = jnp.zeros((1, keys), f32)
        after = jnp.zeros((1, keys), f32)
        for j in range(sp_count):
            upstream = (j > sp) if direction == 1 else (j < sp)
            downstream = (j < sp) if direction == 1 else (j > sp)
            ahead = ahead + jnp.where(upstream, s.totals[j, direction:direction + 1, :], 0.0)
            after = after + jnp.where(
                downstream, s.totals[j, 2 + direction:3 + direction, :], 0.0)
        s.own_decay[direction] = column(s.total[direction:direction + 1, :])
        s.ahead_decay[direction] = column(ahead)
        after_decay = column(after)
        for c in range(chunk_count):
            cols = slice(c * chunk_width, (c + 1) * chunk_width)
            carried = after_decay * s.carry[direction, :, cols]
            s.carry[direction, :, cols] = carried
            s.state[direction, :, cols] += (
                s.own_decay[direction] * s.ahead_decay[direction] * carried)

    first_way = jnp.where(sp < sp_count // 2, 0, 1)

    def chain_copy(way, c, target):
        return remote(s.chain_out.at[way, c], s.chain_in.at[way, c], s.hs.at[way, c],
                      s.hr.at[way, c], "sp", target)

    def chain(way, c, sources):
        cols = slice(c * chunk_width, (c + 1) * chunk_width)
        onward = 1 - 2 * way
        has_before = jnp.where(way == 0, sp > 0, sp < sp_count - 1)
        has_next = jnp.where(way == 0, sp < sp_count - 1, sp > 0)

        @pl.when(jnp.logical_and(has_next, jnp.logical_not(has_before)) if sources else has_before)
        def _():
            if not sources:
                chain_copy(way, c, sp - onward).wait_recv()

            @pl.when(has_next)
            def _():
                s.chain_out[way, c, :keys, :] = (
                    s.own_decay[way] * s.chain_in[way, c, :keys, :].astype(f32)
                    + s.state[way, :, cols]).astype(bf16)
                s.chain_out[way, c, keys:, :] = (
                    s.chain_in[way, c, keys:, :].astype(f32)
                    + s.carry[1 - way, :, cols]).astype(bf16)
                chain_copy(way, c, sp + onward).start()

    def attend(b):
        rows = slice(b * size, (b + 1) * size)
        query = dot(s.mod_latent[rows, :], s.wqk[1]).astype(bf16)
        rq = rotate(query.astype(f32) * keys ** -0.5, s.cosine[rows, :], s.sine[rows, :])
        rk = s.key[rows, :]
        scores, out = None, None
        for direction in range(2):
            keep = triangle(size, direction == 1)
            middle = size // 2 if direction == 1 else size // 2 - 1
            cum = s.cum[direction, rows, :]
            center = cum[middle:middle + 1, :]
            q_mid = (rq * jnp.exp(cum - center)).astype(bf16)
            k_mid = (rk * jnp.exp(center - cum)).astype(bf16)
            score = jnp.where(keep, dot(q_mid, k_mid, ((1,), (1,))), 0.0)
            scores = score if scores is None else scores + score
            q_dec = rq * jnp.exp(cum)
            q_all = q_dec
            if b != (blocks - 1 if direction == 1 else 0):
                carried = dot(q_dec.astype(bf16), s.start[direction, b])
                out = carried if out is None else out + carried
                q_all = q_dec * jnp.exp(s.ahead[direction, b:b + 1, :])
            s.q_all[rows, direction * keys:(direction + 1) * keys] = q_all.astype(bf16)
        inner = dot(scores.astype(bf16), s.value[rows, :])
        s.mixture[rows, :] = inner if out is None else out + inner

    for c in range(chunk_count):
        chain(first_way, c, True)
    for hop in range(2, sp_count - 1):
        for chunk in query_chunks:
            z_arrive(hop, chunk)
    for hop in range(sp_count - 1):
        for chunk in query_chunks:
            y_each(hop, chunk, other_view, lambda c: c.wait_recv())
    for turn in range(max(blocks, chunk_count)):
        if turn < blocks:
            attend(turn)
        if turn < chunk_count:
            chain(first_way, turn, False)
    for c in range(chunk_count):
        chain(1 - first_way, c, False)
    for c in range(chunk_count):
        cols = slice(c * chunk_width, (c + 1) * chunk_width)
        for direction in range(2):
            joined = (s.chain_in[direction, c, :keys, :].astype(f32)
                      + s.ahead_decay[direction]
                      * (s.carry[direction, :, cols]
                         + s.chain_in[1 - direction, c, keys:, :].astype(f32)))
            s.joined[direction * keys:(direction + 1) * keys, cols] = joined.astype(bf16)
    for load in (load_norm_gain, load_out_w, load_final_gain, load_final_bias):
        load.wait()

    def gate_rows(chip):
        rows = pl.ds(pl.multiple_of(chip * 2 * own, 2 * own), 2 * own)
        mixture = s.mixture[rows, :] + dot(s.q_all[rows, :], s.joined[...])
        squares = jnp.mean(mixture * mixture, axis=1, keepdims=True)
        gate = s.gate[rows, :].astype(f32)
        normed = mixture * lax.rsqrt(squares + norm_eps) * s.norm_gain[...]
        s.gated[rows, :] = (normed * (gate / (1.0 + jnp.exp(-gate)))).astype(bf16)

    out_chunks = s.far_out.shape[0]
    out_width = width // out_chunks

    def product(j, n):
        cols = slice(n * out_width, (n + 1) * out_width)
        return dot(s.gated[block_rows(j), :], s.out_w[:, cols])

    def pair_copy(slot, n):
        return remote(s.pair_out.at[slot, n], s.pair_in.at[slot, n], s.ds.at[slot, n],
                      s.dr.at[slot, n], "tp", sibling)

    def far_copy(n):
        return remote(s.far_out.at[n], s.far_in.at[n], s.fs.at[n], s.fr.at[n],
                      "tp", across)

    gate_rows(1 - x)
    for n in range(out_chunks):
        s.pair_out[0, n] = product(far_sibling, n).astype(bf16)
        pair_copy(0, n).start()
    for n in range(out_chunks):
        mine = product(across, n)
        pair_copy(0, n).wait_recv()
        s.far_out[n] = (mine + s.pair_in[0, n].astype(f32)).astype(bf16)
        far_copy(n).start()
    gate_rows(x)
    for n in range(out_chunks):
        s.pair_out[1, n] = product(sibling, n).astype(bf16)
        pair_copy(1, n).start()
    for n in range(out_chunks):
        cols = slice(n * out_width, (n + 1) * out_width)
        mine = product(tp, n)
        pair_copy(1, n).wait_recv()
        s.branch[:, cols] = mine + s.pair_in[1, n].astype(f32)
    for n in range(out_chunks):
        cols = slice(n * out_width, (n + 1) * out_width)
        far_copy(n).wait_recv()
        branch = s.branch[:, cols] + s.far_in[n].astype(f32)
        s.branch[:, cols] = (residual_scale * s.rows[block_rows(tp), cols].astype(f32)
                                + s.branch_gate[:, cols] * branch)
    summed = s.branch[...]
    centered = summed - jnp.mean(summed, axis=1, keepdims=True)
    variance = jnp.mean(centered * centered, axis=1, keepdims=True)
    out_ref[...] = (centered * lax.rsqrt(variance + norm_eps) * s.final_gain[...]
                    + s.final_bias[...]).astype(bf16)

    part_drain()
    sums_drain()
    tot_drain()
    line.drain()
    for hop in range(sp_count - 1):
        for chunk in range(2 * PARTS):
            y_each(hop, chunk, weight_view(grp), lambda c: c.wait_send())
    for p in range(pieces):
        x_copy(tp, p).wait_send()
        cross(across, p, 1).wait_send()
    for way in range(2):
        has_next = sp < sp_count - 1 if way == 0 else sp > 0

        @pl.when(has_next)
        def _():
            for c in range(chunk_count):
                chain_copy(way, c, sp + 1 if way == 0 else sp - 1).wait_send()
    for n in range(out_chunks):
        pair_copy(0, n).wait_send()
        pair_copy(1, n).wait_send()
        far_copy(n).wait_send()


def fused(latent, context, condition, context_condition, mod_weight, mod_bias, query_weight,
          key_weight, value_weight, out_gate_weight, decay_in_weight, decay_weight, decay_bias,
          extra_decay, norm_gain, out_weight, final_gain, final_bias):
    sp_count, tp_count = lax.axis_size("sp"), lax.axis_size("tp")
    own, width = latent.shape
    depth = query_weight.shape[0]
    keys = query_weight.shape[1] // ATTENTION_HEADS
    vals = value_weight.shape[1]
    ctx = context.shape[0]
    count = own * tp_count
    blocks = count // (2 * BLOCK)
    mod_cols = mod_weight.shape[1]
    chains, outs, pieces = 4, 4, 4
    args = (latent, context, condition[None, :], context_condition[None, :], mod_weight,
            mod_bias[None, :], query_weight, key_weight, value_weight, out_gate_weight,
            decay_in_weight.T, decay_weight, decay_bias, extra_decay, norm_gain[None, :],
            out_weight, final_gain[None, :], final_bias[None, :])
    dma, vmem = pltpu.SemaphoreType.DMA, pltpu.VMEM
    hops = sp_count - 1
    scratch = Scratch(
        cond=vmem((1, condition.shape[0]), f32),
        ctx_cond=vmem((1, condition.shape[0]), f32),
        mod_w=vmem(mod_weight.shape, bf16),
        mod_b=vmem((1, mod_bias.shape[0]), f32),
        wqk=vmem((2, depth * sp_count, keys), bf16),
        rows=vmem((count, width), bf16),
        mod_latent=vmem((count, width), bf16),
        context=vmem(context.shape, bf16),
        mod_context=vmem(context.shape, bf16),
        low_w=vmem(decay_in_weight.shape[::-1], bf16),
        value_w=vmem(value_weight.shape, bf16),
        gate_w=vmem(out_gate_weight.shape, bf16),
        out_w=vmem(out_weight.shape, bf16),
        decay_w=vmem(decay_weight.shape[:2] + (keys,), bf16),
        decay_b=vmem((2, keys), f32),
        extra=vmem(extra_decay.shape, f32),
        norm_gain=vmem((1, vals), f32),
        final_gain=vmem((1, width), f32),
        final_bias=vmem((1, width), f32),
        part=vmem((sp_count, 2, mod_cols), f32),
        sums=vmem((tp_count, 2, mod_cols), f32),
        totals=vmem((sp_count, 4, keys), f32),
        shifts=vmem((2, width), f32),
        scales=vmem((2, width), f32),
        branch_gate=vmem((1, width), f32),
        cosine=vmem((count, keys), f32),
        sine=vmem((count, keys), f32),
        ctx_close=vmem((2, ctx, keys), f32),
        ctx_value=vmem((ctx, vals), bf16),
        low=vmem((count, decay_in_weight.shape[1]), bf16),
        value=vmem((count, vals), bf16),
        gate=vmem((count, vals), bf16),
        key=vmem((count, keys), f32),
        cum=vmem((2, count, keys), f32),
        ahead=vmem((2, blocks, keys), f32),
        total=vmem((2, keys), f32),
        start=vmem((2, blocks, keys, vals), bf16),
        state=vmem((2, keys, vals), f32),
        carry=vmem((2, keys, vals), f32),
        own_decay=vmem((2, keys, vals // chains), f32),
        ahead_decay=vmem((2, keys, vals // chains), f32),
        chain_in=vmem((2, chains, 2 * keys, vals // chains), bf16),
        chain_out=vmem((2, chains, 2 * keys, vals // chains), bf16),
        q_all=vmem((count, 2 * keys), bf16),
        mixture=vmem((count, vals), f32),
        joined=vmem((2 * keys, vals), bf16),
        gated=vmem((count, vals), bf16),
        pair_out=vmem((2, outs, own, width // outs), bf16),
        pair_in=vmem((2, outs, own, width // outs), bf16),
        far_out=vmem((outs, own, width // outs), bf16),
        far_in=vmem((outs, own, width // outs), bf16),
        branch=vmem((own, width), f32),
        load_sem=dma((len(args),)),
        zs=dma((2, hops, 2 * PARTS)), zr=dma((2, hops, 2 * PARTS)),
        ys=dma((2, hops, 2 * PARTS)), yr=dma((2, hops, 2 * PARTS)),
        xs=dma((pieces,)), xr=dma((pieces,)),
        cs=dma((2 * pieces,)), cr=dma((2 * pieces,)),
        ps=dma((hops,)), pr=dma((hops,)), ts=dma((hops,)), tr=dma((hops,)),
        ss=dma((tp_count - 1,)), sr=dma((tp_count - 1,)),
        hs=dma((2, chains)), hr=dma((2, chains)),
        ds=dma((2, outs)), dr=dma((2, outs)), fs=dma((outs,)), fr=dma((outs,)),
    )
    return pl.pallas_call(
        fused_kernel,
        out_shape=jax.ShapeDtypeStruct((own, width), bf16),
        in_specs=[pl.BlockSpec(memory_space=pltpu.HBM)] * len(args),
        out_specs=pl.BlockSpec(memory_space=pltpu.VMEM),
        scratch_shapes=[scratch],
        compiler_params=pltpu.CompilerParams(
            vmem_limit_bytes=60 * 1024 * 1024, collective_id=2, has_side_effects=True),
        cost_estimate=pl.CostEstimate(flops=6_000_000_000, bytes_accessed=12_000_000,
                                      transcendentals=2_000_000),
    )(*args)


def whole_heads(mesh):
    return mesh.shape["tp"] == ATTENTION_HEADS and mesh.shape["grp"] == 2


def solution(mesh):
    placed = (
        P(("grp", "sp", "tp"), None),
        P(("grp", "sp"), None),
        P(("grp", "sp")),
        P("sp"),
        P("sp", "tp"),
        P(),
        P("sp", None),
        P("sp", None),
        P(None, "tp"),
        P(None, "tp"),
        P(),
        P(),
        P(),
        P(None, None, "sp"),
        P(),
        P("tp", None),
        P(),
        P(),
    )
    return jax.shard_map(
        fused if whole_heads(mesh) else body, mesh=mesh, in_specs=placed, out_specs=P(("grp", "sp", "tp"), None), check_vma=False
    )
```

```python
import functools
from typing import Any, NamedTuple

import jax
import jax.numpy as jnp
from jax import lax
from jax.experimental import pallas as pl
from jax.experimental.pallas import tpu as pltpu
from jax.sharding import PartitionSpec as P

ATTENTION_HEADS = 4
DV = 512
BLOCK = 64
GRID_W = 64


norm_eps = 1e-05
gate_scale = 16.0
rope_base = 10000.0
residual_scale = 2.0**0.5
highest = lax.Precision.HIGHEST
f32 = jnp.float32
bf16 = jnp.bfloat16


def rope_tables(token_places, width):
    quarter = width // 4
    frequency = rope_base ** (-jnp.arange(quarter, dtype=f32) / quarter)
    row_angle = (token_places // GRID_W).astype(f32)[:, None] * frequency
    col_angle = (token_places % GRID_W).astype(f32)[:, None] * frequency
    cosine = jnp.concatenate([jnp.cos(row_angle)] * 2 + [jnp.cos(col_angle)] * 2, axis=1)
    row_sine, col_sine = jnp.sin(row_angle), jnp.sin(col_angle)
    sine = jnp.concatenate([-row_sine, row_sine, -col_sine, col_sine], axis=1)
    return cosine, sine


def dot(a, b, contract=((1,), (0,)), precision=None):
    return lax.dot_general(a, b, (contract, ((), ())), precision=precision,
                           preferred_element_type=f32)


def log_sigmoid(x):
    return jnp.minimum(x, 0.0) - jnp.log1p(jnp.exp(-jnp.abs(x)))


def rotate(x, cosine, sine):
    half = x.shape[1] // 2
    parts = [pltpu.roll(x[:, i * half:(i + 1) * half], half // 2, 1) for i in range(2)]
    return x * cosine + jnp.concatenate(parts, axis=1) * sine


def triangle(size, reverse):
    row = lax.broadcasted_iota(jnp.int32, (size, size), 0)
    col = lax.broadcasted_iota(jnp.int32, (size, size), 1)
    return row <= col if reverse else row >= col


def decay_block(low, decay_weight, decay_bias, direction):
    rank = decay_weight.shape[1]
    logits = dot(low[:, direction * rank:(direction + 1) * rank], decay_weight[direction])
    return log_sigmoid(logits + decay_bias[direction:direction + 1, :]) / gate_scale


def context_kernel(k_ref, v_ref, low_ref, dw_ref, db_ref, state_ref):
    length, width = k_ref.shape
    size = min(2 * BLOCK, length)
    count = length // size
    for direction in range(2):
        mask = triangle(size, direction == 1).astype(f32)
        edge = 0 if direction == 1 else size - 1
        state = None
        for step in range(count):
            b = count - 1 - step if direction == 1 else step
            rows = slice(b * size, (b + 1) * size)
            logdec = decay_block(low_ref[rows, :], dw_ref[...], db_ref[...], direction)
            cum = dot(mask, logdec, precision=highest)
            total = cum[edge:edge + 1, :]
            closing = (k_ref[rows, :].astype(f32) * jnp.exp(total - cum)).astype(bf16)
            term = dot(closing, v_ref[rows, :], ((0,), (0,)))
            state = term if state is None else jnp.exp(total).T * state + term
        state_ref[direction] = state


def local_kernel(q_ref, k_ref, v_ref, low_ref, extra_ref, dw_ref, db_ref, cos_ref, sin_ref,
                 out_ref, qc_ref, state_ref, total_ref):
    length, width = q_ref.shape
    size = 2 * BLOCK
    count = length // size
    rq, rk, within, scores = [], [], [], []
    for b in range(count):
        rows = slice(b * size, (b + 1) * size)
        cosine, sine = cos_ref[rows, :], sin_ref[rows, :]
        rq.append(rotate(q_ref[rows, :].astype(f32) * width ** -0.5, cosine, sine))
        rk.append(rotate(k_ref[rows, :].astype(f32), cosine, sine))
        scores.append(None)
    for direction in range(2):
        keep = triangle(size, direction == 1)
        mask = keep.astype(f32)
        edge = 0 if direction == 1 else size - 1
        middle = size // 2 if direction == 1 else size // 2 - 1
        state = None
        before = None
        for step in range(count):
            b = count - 1 - step if direction == 1 else step
            rows = slice(b * size, (b + 1) * size)
            logdec = decay_block(low_ref[rows, :], dw_ref[...], db_ref[...], direction)
            logdec = logdec + extra_ref[rows, direction:direction + 1]
            cum = dot(mask, logdec, precision=highest)
            total = cum[edge:edge + 1, :]
            center = cum[middle:middle + 1, :]
            q_mid = (rq[b] * jnp.exp(cum - center)).astype(bf16)
            k_mid = (rk[b] * jnp.exp(center - cum)).astype(bf16)
            score = jnp.where(keep, dot(q_mid, k_mid, ((1,), (1,))), 0.0)
            q_dec = rq[b] * jnp.exp(cum)
            if direction == 0:
                scores[b] = score
                out = None
            else:
                out = dot((scores[b] + score).astype(bf16), v_ref[rows, :])
            if state is not None:
                carried = dot(q_dec.astype(bf16), state.astype(bf16))
                out = carried if out is None else out + carried
            if direction == 0:
                out_ref[rows, :] = jnp.zeros((size, v_ref.shape[1]), f32) if out is None else out
            else:
                out_ref[rows, :] += out
            q_all = q_dec if before is None else q_dec * jnp.exp(before)
            qc_ref[rows, direction * width:(direction + 1) * width] = q_all.astype(bf16)
            closing = (rk[b] * jnp.exp(total - cum)).astype(bf16)
            term = dot(closing, v_ref[rows, :], ((0,), (0,)))
            state = term if state is None else jnp.exp(total).T * state + term
            before = total if before is None else before + total
        state_ref[direction * width:(direction + 1) * width, :] = state.astype(bf16)
        total_ref[direction:direction + 1, :] = before


def join_kernel(final, out_ref, qc_ref, states_ref, totals_ref, start_ref, gate_ref, gain_ref,
                place_ref, result_ref):
    count = states_ref.shape[0]
    width = qc_ref.shape[1] // 2
    place = place_ref[...]
    mixture = out_ref[...]
    for direction in range(2):
        state = start_ref[direction]
        for lap in range(count):
            j = count - 1 - lap if direction == 1 else lap
            decay = jnp.exp(totals_ref[j, direction:direction + 1, :]).T
            joined = decay * state + states_ref[
                j, direction * width:(direction + 1) * width, :].astype(f32)
            ahead = place < j if direction == 1 else place > j
            state = jnp.where(ahead, joined, state)
        mixture = mixture + dot(qc_ref[:, direction * width:(direction + 1) * width],
                                state.astype(bf16))
    if final:
        squares = jnp.mean(mixture * mixture, axis=1, keepdims=True)
        gate = gate_ref[...].astype(f32)
        normed = mixture * lax.rsqrt(squares + norm_eps) * gain_ref[...]
        result_ref[...] = (normed * (gate / (1.0 + jnp.exp(-gate)))).astype(bf16)
    else:
        result_ref[...] = mixture


def call(kernel, out_shape, *args):
    return pl.pallas_call(
        kernel,
        out_shape=out_shape,
        in_specs=[pl.BlockSpec(memory_space=pltpu.VMEM)] * len(args),
        out_specs=jax.tree.map(lambda _: pl.BlockSpec(memory_space=pltpu.VMEM), out_shape),
        compiler_params=pltpu.CompilerParams(vmem_limit_bytes=48 * 1024 * 1024),
        cost_estimate=pl.CostEstimate(flops=4_000_000_000, bytes_accessed=4_000_000,
                                      transcendentals=1_000_000),
    )(*args)


MESH = pl.DeviceIdType.MESH


def remote(src, dst, send_sem, recv_sem, axis, target):
    return pltpu.make_async_remote_copy(
        src_ref=src, dst_ref=dst, send_sem=send_sem, recv_sem=recv_sem,
        device_id={axis: target}, device_id_type=MESH)


class Line:
    def __init__(self, place, count, axis, target_of, view, chunks, send_sem, recv_sem):
        self.place, self.count, self.axis, self.target_of = place, count, axis, target_of
        self.view, self.chunks, self.send_sem, self.recv_sem = view, chunks, send_sem, recv_sem

    def copy(self, way, hop, chunk, block, target):
        ref = self.view(block, chunk)
        return remote(ref, ref, self.send_sem.at[way, hop, chunk],
                      self.recv_sem.at[way, hop, chunk], self.axis, self.target_of(target))

    def outgoing(self, way, hop):
        place, count = self.place, self.count
        if way == 0:
            return place - hop, place + 1, jnp.logical_and(place >= hop, place < count - 1)
        return place + hop, place - 1, jnp.logical_and(place + hop < count, place > 0)

    def each_send(self, way, hop, chunk, act):
        block, target, valid = self.outgoing(way, hop)

        @pl.when(valid)
        def _():
            act(self.copy(way, hop, chunk, block, target))

    def send(self, way, hop, chunk):
        self.each_send(way, hop, chunk, lambda c: c.start())

    def drain(self):
        for way in range(2):
            for hop in range(self.count - 1):
                for chunk in range(self.chunks):
                    self.each_send(way, hop, chunk, lambda c: c.wait_send())

    def arrive(self, way, hop, chunk, then=None):
        if way == 0:
            block, source, valid = self.place - 1 - hop, self.place - 1, self.place > hop
        else:
            block, source = self.place + 1 + hop, self.place + 1
            valid = self.place + 1 + hop < self.count

        @pl.when(valid)
        def _():
            self.copy(way, hop, chunk, block, source).wait_recv()
            if then is not None:
                then(block)

    def forward(self, hop, then=None):
        for chunk in range(self.chunks):
            for way in range(2):
                self.arrive(way, hop, chunk, None if then is None else functools.partial(then, way))
                if hop + 1 < self.count - 1:
                    self.send(way, hop + 1, chunk)


def open_kernel(partners):
    barrier = pltpu.get_barrier_semaphore()
    for axis, target in partners:
        pl.semaphore_signal(barrier, inc=1, device_id={axis: target}, device_id_type=MESH)
    return lambda: pl.semaphore_wait(barrier, len(partners))


def others(axis):
    count, place = lax.axis_size(axis), lax.axis_index(axis)
    return [lax.rem(place + k, count) for k in range(1, count)]


def sources(axis):
    count, place = lax.axis_size(axis), lax.axis_index(axis)
    return [lax.rem(place + count - k, count) for k in range(1, count)]


def spread(buffer, axis, send_sem, recv_sem):
    place = lax.axis_index(axis)
    for k, target in enumerate(others(axis)):
        remote(buffer.at[place], buffer.at[place], send_sem.at[k], recv_sem.at[k],
               axis, target).start()


def spread_arrive(buffer, axis, send_sem, recv_sem):
    for k, source in enumerate(sources(axis)):
        remote(buffer.at[source], buffer.at[source], send_sem.at[k], recv_sem.at[k],
               axis, source).wait_recv()


def spread_drain(buffer, axis, send_sem, recv_sem):
    place = lax.axis_index(axis)
    for k, target in enumerate(others(axis)):
        remote(buffer.at[place], buffer.at[place], send_sem.at[k], recv_sem.at[k],
               axis, target).wait_send()


def enter_kernel(chunks, latent_ref, context_ref, cond_ref, mw_ref, mb_ref, qw_ref, kw_ref,
                 ml_ref, mc_ref, gate_ref, qk_ref,
                 rows_ref, part_ref, sums_ref, zs, zr, xs, xr, cs, cr, ps, pr, ss, sr):
    sp, sp_count = lax.axis_index("sp"), lax.axis_size("sp")
    tp, tp_count = lax.axis_index("tp"), lax.axis_size("tp")
    own, model_width = latent_ref.shape
    depth = qw_ref.shape[0]
    head_keys = qk_ref.shape[1] // 2
    ready = open_kernel([("sp", t) for t in others("sp")] + [("tp", t) for t in others("tp")])
    v = cond_ref[...]
    activated = (v / (1.0 + jnp.exp(-v))).astype(bf16)
    part_ref[sp] = dot(activated, mw_ref[...])
    columns = pl.ds(pl.multiple_of((tp // (tp_count // ATTENTION_HEADS)) * head_keys, head_keys),
                    head_keys)
    qk_rows = pl.ds(pl.multiple_of(sp * depth, depth), depth)
    qk_ref[qk_rows, :head_keys] = qw_ref[:, columns]
    qk_ref[qk_rows, head_keys:] = kw_ref[:, columns]
    rows_ref[pl.ds(pl.multiple_of(tp * own, own), own), :] = latent_ref[...]

    step = depth // chunks
    z_line = Line(
        sp, sp_count, "sp", lambda p: p,
        lambda block, chunk: qk_ref.at[
            pl.ds(pl.multiple_of(block * depth + chunk * step, step), step), :],
        chunks, zs, zr)
    x_count = tp_count // 2
    x, core = tp // 2, tp % 2

    def rows_of(block, chunk):
        return rows_ref.at[pl.ds(pl.multiple_of((2 * block + core) * own, own), own), :]

    x_line = Line(x, x_count, "tp", lambda p: 2 * p + core, rows_of, 1, xs, xr)
    sibling = tp + 1 - 2 * core

    def cross(block, slot, other=False):
        side = 1 - core if other else core
        ref = rows_ref.at[pl.ds(pl.multiple_of((2 * block + side) * own, own), own), :]
        return remote(ref, ref, cs.at[slot], cr.at[slot], "tp", sibling)

    def slot_of(way, hop):
        return 1 + way * (x_count - 1) + hop

    ready()
    spread(part_ref, "sp", ps, pr)
    for way in range(2):
        x_line.send(way, 0, 0)
    cross(x, 0).start()
    for chunk in range(chunks):
        for way in range(2):
            z_line.send(way, 0, chunk)
    spread_arrive(part_ref, "sp", ps, pr)
    total = part_ref[0]
    for j in range(1, sp_count):
        total = total + part_ref[j]
    sums_ref[tp] = total
    spread(sums_ref, "tp", ss, sr)
    z_line.forward(0)
    for hop in range(x_count - 1):
        x_line.forward(hop, lambda way, block, hop=hop: cross(block, slot_of(way, hop)).start())
    if sp_count > 2:
        z_line.forward(1)
    spread_arrive(sums_ref, "tp", ss, sr)
    modulation = jnp.concatenate([sums_ref[j] for j in range(tp_count)], axis=1) + mb_ref[...]
    shifts = modulation[:, :model_width]
    scales = modulation[:, model_width:2 * model_width]
    gate_ref[...] = modulation[0:1, 2 * model_width:]
    mc_ref[...] = (context_ref[...].astype(f32) * (1.0 + scales[1:2]) + shifts[1:2]).astype(bf16)

    def each_cross(act_own, act_line):
        act_own()
        for way in range(2):
            for hop in range(x_count - 1):
                block = x - 1 - hop if way == 0 else x + 1 + hop
                valid = x > hop if way == 0 else x + 1 + hop < x_count

                @pl.when(valid)
                def _():
                    act_line(block, slot_of(way, hop))

    each_cross(lambda: cross(x, 0, True).wait_recv(),
               lambda block, slot: cross(block, slot, True).wait_recv())
    for j in range(tp_count):
        rows = slice(j * own, (j + 1) * own)
        ml_ref[rows, :] = (rows_ref[rows, :].astype(f32) * (1.0 + scales[0:1])
                           + shifts[0:1]).astype(bf16)
    for hop in range(2, sp_count - 1):
        z_line.forward(hop)
    each_cross(lambda: cross(x, 0).wait_send(),
               lambda block, slot: cross(block, slot).wait_send())
    spread_drain(part_ref, "sp", ps, pr)
    spread_drain(sums_ref, "tp", ss, sr)
    x_line.drain()
    z_line.drain()


def comm_call(kernel, out_shape, scratch, collective_id, *args):
    return pl.pallas_call(
        kernel,
        out_shape=out_shape,
        in_specs=[pl.BlockSpec(memory_space=pltpu.VMEM)] * len(args),
        out_specs=jax.tree.map(lambda _: pl.BlockSpec(memory_space=pltpu.VMEM), out_shape),
        scratch_shapes=scratch,
        compiler_params=pltpu.CompilerParams(
            vmem_limit_bytes=48 * 1024 * 1024, collective_id=collective_id,
            has_side_effects=True),
        cost_estimate=pl.CostEstimate(flops=20_000_000_000, bytes_accessed=60_000_000,
                                      transcendentals=1_000_000),
    )(*args)


def enter(latent, context, cond, mod_weight, mod_bias, query_weight, key_weight):
    sp_count, tp_count = lax.axis_size("sp"), lax.axis_size("tp")
    own, model_width = latent.shape
    depth = query_weight.shape[0]
    head_keys = query_weight.shape[1] // ATTENTION_HEADS
    chunks = 4
    sds = jax.ShapeDtypeStruct
    dma = pltpu.SemaphoreType.DMA
    x_hops = tp_count // 2 - 1
    return comm_call(
        functools.partial(enter_kernel, chunks),
        (
            sds((own * tp_count, model_width), bf16),
            sds(context.shape, bf16),
            sds((1, model_width), f32),
            sds((depth * sp_count, 2 * head_keys), bf16),
        ),
        [
            pltpu.VMEM((own * tp_count, model_width), bf16),
            pltpu.VMEM((sp_count, 2, mod_weight.shape[1]), f32),
            pltpu.VMEM((tp_count, 2, mod_weight.shape[1]), f32),
            dma((2, sp_count - 1, chunks)), dma((2, sp_count - 1, chunks)),
            dma((2, x_hops, 1)), dma((2, x_hops, 1)),
            dma((1 + 2 * x_hops,)), dma((1 + 2 * x_hops,)),
            dma((sp_count - 1,)), dma((sp_count - 1,)),
            dma((tp_count - 1,)), dma((tp_count - 1,)),
        ],
        1, latent, context, cond, mod_weight, mod_bias[None, :], query_weight, key_weight,
    )


def project(rows, weight):
    return jnp.dot(rows, weight, preferred_element_type=f32).astype(bf16)


def body(
    latent,
    context,
    condition,
    context_condition,
    mod_weight,
    mod_bias,
    query_weight,
    key_weight,
    value_weight,
    out_gate_weight,
    decay_in_weight,
    decay_weight,
    decay_bias,
    extra_decay,
    norm_gain,
    out_weight,
    final_gain,
    final_bias,
):
    head_keys = query_weight.shape[1] // ATTENTION_HEADS
    value_cols = value_weight.shape[1]
    tp_index = lax.axis_index("tp")
    sp_index = lax.axis_index("sp")
    head_share = lax.axis_size("tp") // ATTENTION_HEADS
    head_index = tp_index // head_share
    part_index = tp_index % head_share
    key_start = head_index * head_keys

    full_out = lax.all_gather(out_weight, "tp", axis=0, tiled=True)
    mod_latent, mod_context, branch_gate, qk_head = enter(
        latent, context, jnp.stack([condition, context_condition]), mod_weight, mod_bias,
        query_weight, key_weight,
    )
    context_local = jnp.concatenate(
        [
            project(mod_context, qk_head[:, head_keys:]),
            project(mod_context, value_weight),
            project(mod_context, decay_in_weight),
        ],
        axis=1,
    )
    gathered_context = lax.all_gather(context_local, "sp", axis=0, tiled=True)
    qk = project(mod_latent, qk_head)
    value_rows = project(mod_latent, value_weight)
    out_gate = project(mod_latent, out_gate_weight)
    low_rank = project(mod_latent, decay_in_weight)
    count = mod_latent.shape[0]
    token_places = sp_index * count + jnp.arange(count, dtype=jnp.int32)
    cosine, sine = rope_tables(token_places, head_keys)
    head_bias = lax.dynamic_slice_in_dim(decay_bias, key_start, head_keys, 1)
    head_gate = lax.dynamic_slice_in_dim(decay_weight, key_start, head_keys, 2)
    head_extra = lax.dynamic_index_in_dim(extra_decay, head_index, 1, keepdims=False).T

    sds = jax.ShapeDtypeStruct
    out_local, qc, states, totals = call(
        local_kernel,
        (
            sds((count, value_cols), f32),
            sds((count, 2 * head_keys), bf16),
            sds((2 * head_keys, value_cols), bf16),
            sds((2, head_keys), f32),
        ),
        qk[:, :head_keys], qk[:, head_keys:], value_rows, low_rank, head_extra, head_gate,
        head_bias, cosine, sine,
    )
    start = call(
        context_kernel,
        sds((2, head_keys, value_cols), f32),
        gathered_context[:, :head_keys],
        gathered_context[:, head_keys : head_keys + value_cols],
        gathered_context[:, head_keys + value_cols :],
        head_gate, head_bias,
    )
    states, totals, full_out = lax.optimization_barrier((states, totals, full_out))
    all_states = lax.all_gather(states, "sp")
    all_totals = lax.all_gather(totals, "sp")
    place = jnp.full((1, value_cols), sp_index, jnp.int32)
    gain_slice = lax.dynamic_slice_in_dim(norm_gain, part_index * value_cols, value_cols, 0)
    final = head_share == 1
    joined = call(
        functools.partial(join_kernel, final),
        sds((count, value_cols), bf16 if final else f32),
        out_local, qc, all_states, all_totals, start, out_gate, gain_slice[None, :], place,
    )
    if final:
        gated_rows = joined
    else:
        squares = jnp.sum(joined * joined, axis=1)
        onehot = (jnp.arange(ATTENTION_HEADS) == head_index).astype(f32)
        sums = lax.psum(onehot[:, None] * squares[None, :], "tp")
        head_sum = jnp.sum(sums * onehot[:, None], axis=0)
        normed = joined * lax.rsqrt(head_sum / DV + norm_eps)[:, None] * gain_slice
        gated_rows = (normed * jax.nn.silu(out_gate.astype(f32))).astype(bf16)
    regrouped = lax.all_to_all(gated_rows, "tp", split_axis=0, concat_axis=1, tiled=True)
    branch = jnp.dot(regrouped, full_out, preferred_element_type=f32)
    summed = residual_scale * latent.astype(f32) + branch_gate * branch
    row_mean = jnp.mean(summed, axis=1, keepdims=True)
    centered = summed - row_mean
    variance = jnp.mean(centered * centered, axis=1, keepdims=True)
    return (centered * lax.rsqrt(variance + norm_eps) * final_gain + final_bias).astype(bf16)


class Scratch(NamedTuple):
    cond: Any
    ctx_cond: Any
    mod_w: Any
    mod_b: Any
    wqk: Any
    rows: Any
    mod_latent: Any
    context: Any
    mod_context: Any
    low_w: Any
    value_w: Any
    gate_w: Any
    out_w: Any
    decay_w: Any
    decay_b: Any
    extra: Any
    norm_gain: Any
    final_gain: Any
    final_bias: Any
    part: Any
    sums: Any
    totals: Any
    shifts: Any
    scales: Any
    branch_gate: Any
    cosine: Any
    sine: Any
    ctx_close: Any
    ctx_value: Any
    low: Any
    value: Any
    gate: Any
    key: Any
    cum: Any
    ahead: Any
    block_total: Any
    total: Any
    start: Any
    state: Any
    carry: Any
    own_decay: Any
    ahead_decay: Any
    chain_in: Any
    chain_out: Any
    q_all: Any
    mixture: Any
    joined: Any
    gated: Any
    pair_out: Any
    pair_in: Any
    far_out: Any
    far_in: Any
    branch: Any
    load_sem: Any
    zs: Any
    zr: Any
    ys: Any
    yr: Any
    xs: Any
    xr: Any
    cs: Any
    cr: Any
    ps: Any
    pr: Any
    ts: Any
    tr: Any
    ss: Any
    sr: Any
    hs: Any
    hr: Any
    ds: Any
    dr: Any
    fs: Any
    fr: Any


def spread_of(ref, axis, send_sem, recv_sem):
    return (lambda: spread(ref, axis, send_sem, recv_sem),
            lambda: spread_arrive(ref, axis, send_sem, recv_sem),
            lambda: spread_drain(ref, axis, send_sem, recv_sem))


PARTS = 2


def fused_kernel(latent, context, cond, ctx_cond, mod_w, mod_b, query_w, key_w, value_w, gate_w,
                 low_w, decay_w, decay_b, extra, norm_gain, out_w, final_gain, final_bias,
                 out_ref, s):
    grp = lax.axis_index("grp")
    sp, sp_count = lax.axis_index("sp"), lax.axis_size("sp")
    tp, tp_count = lax.axis_index("tp"), lax.axis_size("tp")
    own, width = latent.shape
    depth = query_w.shape[0]
    keys = query_w.shape[1] // ATTENTION_HEADS
    vals = value_w.shape[1]
    count = own * tp_count
    size = 2 * BLOCK
    blocks = count // size
    ctx = context.shape[0]
    x, core = tp // 2, tp % 2
    sibling, across = tp + 1 - 2 * core, 2 * (1 - x) + core
    far_sibling = 2 * (1 - x) + 1 - core

    def block_rows(j):
        return pl.ds(pl.multiple_of(j * own, own), own)

    ready = open_kernel([("sp", t) for t in others("sp")] + [("tp", t) for t in others("tp")]
                        + [("grp", 1 - grp)])
    head_cols = pl.ds(pl.multiple_of(tp * keys, keys), keys)
    own_depth = pl.ds(pl.multiple_of(sp * depth, depth), depth)
    loads = []
    for i, (source, target) in enumerate((
        (cond, s.cond), (ctx_cond, s.ctx_cond),
        (mod_w, s.mod_w),
        (key_w.at[:, head_cols], s.wqk.at[0, own_depth, :]),
        (query_w.at[:, head_cols], s.wqk.at[1, own_depth, :]),
        (latent, s.rows.at[block_rows(tp), :]),
        (mod_b, s.mod_b), (context, s.context),
        (low_w, s.low_w), (value_w, s.value_w),
        (decay_w.at[:, :, head_cols], s.decay_w),
        (decay_b.at[:, head_cols], s.decay_b), (extra, s.extra),
        (gate_w, s.gate_w), (norm_gain, s.norm_gain),
        (out_w, s.out_w), (final_gain, s.final_gain),
        (final_bias, s.final_bias),
    )):
        loads.append(pltpu.make_async_copy(source, target, s.load_sem.at[i]))
        loads[i].start()
    (load_cond, load_ctx_cond, load_mod_w, load_key_w, load_query_w, load_latent,
     load_mod_b, load_context, load_low_w, load_value_w, load_decay_w, load_decay_b,
     load_extra, load_gate_w, load_norm_gain, load_out_w, load_final_gain, load_final_bias) = loads

    half = depth // 2
    step = half // PARTS

    def weight_view(side):
        def view(block, chunk):
            start = block * depth + side * half + (chunk % PARTS) * step
            return s.wqk.at[chunk // PARTS, pl.ds(pl.multiple_of(start, step), step), :]
        return view

    line = Line(sp, sp_count, "sp", lambda p: p, weight_view(grp), 2 * PARTS, s.zs, s.zr)
    other_view = weight_view(1 - grp)

    def y_copy(ref, way, hop, chunk):
        return remote(ref, ref, s.ys.at[way, hop, chunk], s.yr.at[way, hop, chunk],
                      "grp", 1 - grp)

    def z_arrive(hop, chunk, pass_on=True):
        for way in range(2):
            line.arrive(way, hop, chunk, (lambda block: y_copy(
                weight_view(grp)(block, chunk), way, hop, chunk).start()) if pass_on else None)
            if hop + 1 < sp_count - 1:
                line.send(way, hop + 1, chunk)

    def y_each(hop, chunk, view, act):
        for way in range(2):
            block = sp - 1 - hop if way == 0 else sp + 1 + hop
            valid = sp > hop if way == 0 else sp + 1 + hop < sp_count

            @pl.when(valid)
            def _():
                act(y_copy(view(block, chunk), way, hop, chunk))

    key_chunks, query_chunks = range(PARTS), range(PARTS, 2 * PARTS)

    def send_own(chunks):
        for chunk in chunks:
            for way in range(2):
                line.send(way, 0, chunk)

    pieces, early = s.xs.shape[0], 1
    piece = own // pieces

    def rows_piece(j, p):
        return s.rows.at[pl.ds(pl.multiple_of(j * own + p * piece, piece), piece), :]

    def x_copy(j, p):
        return remote(rows_piece(j, p), rows_piece(j, p), s.xs.at[p], s.xr.at[p],
                      "tp", across)

    def cross(j, p, slot):
        k = slot * pieces + p
        return remote(rows_piece(j, p), rows_piece(j, p), s.cs.at[k], s.cr.at[k],
                      "tp", sibling)

    part_go, part_arrive, part_drain = spread_of(s.part, "sp", s.ps, s.pr)
    sums_go, sums_arrive, sums_drain = spread_of(s.sums, "tp", s.ss, s.sr)
    tot_go, tot_arrive, tot_drain = spread_of(s.totals, "sp", s.ts, s.tr)

    for load in (load_cond, load_ctx_cond, load_mod_w):
        load.wait()
    v = jnp.concatenate([s.cond[...], s.ctx_cond[...]], axis=0)
    activated = (v / (1.0 + jnp.exp(-v))).astype(bf16)
    s.part[sp] = dot(activated, s.mod_w[...])
    for load in (load_key_w, load_query_w, load_latent):
        load.wait()

    ready()
    part_go()
    send_own(key_chunks)
    send_own(query_chunks[:1])
    for p in range(pieces):
        if p < early:
            x_copy(tp, p).start()
        cross(tp, p, 0).start()

    quarter = keys // 4

    def rope(b, carry):
        rows = pl.ds(pl.multiple_of(b * size, size), size)
        lane = lax.broadcasted_iota(jnp.int32, (1, keys), 1)
        index = jnp.bitwise_and(lane, quarter - 1).astype(f32)
        frequency = jnp.exp(index * (-jnp.log(rope_base) / quarter))
        by_row = lane < keys // 2
        first = jnp.bitwise_and(lane, 2 * quarter - 1) < quarter
        place = lax.broadcasted_iota(jnp.int32, (size, 1), 0) + (sp * count + b * size)
        place = place.astype(f32)
        row = jnp.floor((place + 0.5) * (1.0 / GRID_W))
        col = place - row * GRID_W
        angle = jnp.where(by_row, row, col) * frequency
        s.cosine[rows, :] = jnp.cos(angle)
        sine = jnp.sin(angle)
        s.sine[rows, :] = jnp.where(first, -sine, sine)
        return carry

    lax.fori_loop(0, blocks, rope, 0)

    @pl.when(sp == 0)
    def _():
        s.chain_in[0] = jnp.zeros(s.chain_in.shape[1:], bf16)

    @pl.when(sp == sp_count - 1)
    def _():
        s.chain_in[1] = jnp.zeros(s.chain_in.shape[1:], bf16)

    part_arrive()
    total = s.part[0]
    for j in range(1, sp_count):
        total = total + s.part[j]
    s.sums[tp] = total
    sums_go()
    for p in range(early, pieces):
        x_copy(tp, p).start()
    for chunk in key_chunks:
        z_arrive(0, chunk)
    send_own(query_chunks[1:])
    sums_arrive()
    for load in (load_mod_b, load_context, load_low_w, load_value_w, load_decay_w, load_decay_b, load_extra):
        load.wait()
    modulation = (jnp.concatenate([s.sums[j] for j in range(tp_count)], axis=1)
                  + s.mod_b[...])
    s.shifts[...] = modulation[:, :width]
    s.scales[...] = 1.0 + modulation[:, width:2 * width]
    s.branch_gate[...] = modulation[0:1, 2 * width:]
    s.mod_context[...] = (s.context[...].astype(f32) * s.scales[1:2, :]
                             + s.shifts[1:2, :]).astype(bf16)

    def decay_of(low, direction):
        rank = s.decay_w.shape[1]
        logits = dot(low[:, direction * rank:(direction + 1) * rank], s.decay_w[direction])
        return log_sigmoid(logits + s.decay_b[direction:direction + 1, :]) / gate_scale

    own_head = lax.broadcasted_iota(jnp.int32, (ATTENTION_HEADS, size), 0) == tp

    def project_chip(chip):
        rows = pl.ds(pl.multiple_of(chip * 2 * own, 2 * own), 2 * own)
        mod = (s.rows[rows, :].astype(f32) * s.scales[0:1, :]
               + s.shifts[0:1, :]).astype(bf16)
        s.mod_latent[rows, :] = mod
        s.low[rows, :] = dot(mod, s.low_w[...], ((1,), (1,))).astype(bf16)
        s.value[rows, :] = dot(mod, s.value_w[...]).astype(bf16)

    def gate_chip(chip):
        rows = pl.ds(pl.multiple_of(chip * 2 * own, 2 * own), 2 * own)
        s.gate[rows, :] = dot(s.mod_latent[rows, :], s.gate_w[...]).astype(bf16)

    def decay_chip(chip):
        for i in range(2 * own // size):
            b = chip * (2 * own // size) + i
            rows = pl.ds(pl.multiple_of(b * size, size), size)
            low = s.low[rows, :]
            for direction in range(2):
                mask = triangle(size, direction == 1).astype(f32)
                edge = 0 if direction == 1 else size - 1
                head_extra = jnp.sum(jnp.where(own_head, s.extra[direction, :, rows], 0.0),
                                     axis=0, keepdims=True)
                added = jnp.sum(mask * head_extra, axis=1, keepdims=True)
                cum = dot(mask, decay_of(low, direction), precision=highest) + added
                s.cum[direction, rows, :] = cum
                s.block_total[direction, b] = cum[edge:edge + 1, :]

    for p in range(pieces):
        cross(tp, p, 0).wait_send()
        remote(rows_piece(sibling, p), rows_piece(sibling, p), s.cs.at[p], s.cr.at[p],
               "tp", sibling).wait_recv()
    project_chip(x)
    for chunk in key_chunks:
        if sp_count > 2:
            z_arrive(1, chunk)
    decay_chip(x)
    for chunk in query_chunks:
        z_arrive(0, chunk, False)
    ctx_low = dot(s.mod_context[...], s.low_w[...], ((1,), (1,))).astype(bf16)
    ctx_totals = []
    for direction in range(2):
        mask = triangle(ctx, direction == 1).astype(f32)
        edge = 0 if direction == 1 else ctx - 1
        cum = dot(mask, decay_of(ctx_low, direction), precision=highest)
        ctx_totals.append(cum[edge:edge + 1, :])
        s.ctx_close[direction] = jnp.exp(ctx_totals[direction] - cum)
    s.ctx_value[...] = dot(s.mod_context[...], s.value_w[...]).astype(bf16)
    for hop in range(2, sp_count - 1):
        for chunk in key_chunks:
            z_arrive(hop, chunk)
    for chunk in query_chunks:
        y_each(0, chunk, weight_view(grp), lambda c: c.start())
    for p in range(pieces):
        x_copy(across, p).wait_recv()
        cross(across, p, 1).start()
    if sp_count > 2:
        for chunk in query_chunks:
            z_arrive(1, chunk)
    for p in range(pieces):
        cross(far_sibling, p, 1).wait_recv()
    project_chip(1 - x)
    decay_chip(1 - x)
    for direction in range(2):
        before = None
        for turn in range(blocks):
            b = blocks - 1 - turn if direction == 1 else turn
            if before is not None:
                s.ahead[direction, b:b + 1, :] = before
            block_total = s.block_total[direction, b]
            before = block_total if before is None else before + block_total
        s.total[direction:direction + 1, :] = before
    s.totals[sp] = jnp.concatenate([s.total[...]] + ctx_totals, axis=0)
    tot_go()
    for hop in range(sp_count - 1):
        for chunk in key_chunks:
            y_each(hop, chunk, other_view, lambda c: c.wait_recv())
    ctx_key = dot(s.mod_context[...], s.wqk[0]).astype(bf16).astype(f32)
    for direction in range(2):
        closing = (ctx_key * s.ctx_close[direction]).astype(bf16)
        s.carry[direction] = dot(closing, s.ctx_value[...], ((0,), (0,)))
    for b in range(blocks):
        rows = slice(b * size, (b + 1) * size)
        key = dot(s.mod_latent[rows, :], s.wqk[0]).astype(bf16)
        s.key[rows, :] = rotate(key.astype(f32), s.cosine[rows, :], s.sine[rows, :])
    for direction in range(2):
        edge = 0 if direction == 1 else size - 1
        state = None
        for turn in range(blocks):
            b = blocks - 1 - turn if direction == 1 else turn
            rows = slice(b * size, (b + 1) * size)
            cum = s.cum[direction, rows, :]
            block_total = cum[edge:edge + 1, :]
            closing = (s.key[rows, :] * jnp.exp(block_total - cum)).astype(bf16)
            term = dot(closing, s.value[rows, :], ((0,), (0,)))
            if state is None:
                state = term
            else:
                s.start[direction, b] = state.astype(bf16)
                state = jnp.exp(block_total).T * state + term
        s.state[direction] = state
    tot_arrive()
    chunk_width = s.chain_in.shape[3]
    chunk_count = vals // chunk_width
    steps = s.chain_in.shape[1]

    def column(row):
        return jnp.broadcast_to(jnp.exp(row).T, (keys, chunk_width))

    for direction in range(2):
        ahead = jnp.zeros((1, keys), f32)
        after = jnp.zeros((1, keys), f32)
        for j in range(sp_count):
            upstream = (j > sp) if direction == 1 else (j < sp)
            downstream = (j < sp) if direction == 1 else (j > sp)
            ahead = ahead + jnp.where(upstream, s.totals[j, direction:direction + 1, :], 0.0)
            after = after + jnp.where(
                downstream, s.totals[j, 2 + direction:3 + direction, :], 0.0)
        s.own_decay[direction] = column(s.total[direction:direction + 1, :])
        s.ahead_decay[direction] = column(ahead)
        after_decay = column(after)
        for c in range(chunk_count):
            cols = slice(c * chunk_width, (c + 1) * chunk_width)
            carried = after_decay * s.carry[direction, :, cols]
            s.carry[direction, :, cols] = carried
            s.state[direction, :, cols] += (
                s.own_decay[direction] * s.ahead_decay[direction] * carried)

    first_way = jnp.where(sp < sp_count // 2, 0, 1)
    halves = keys // s.chain_in.shape[2] * 2
    part_keys = keys // halves

    def chain_copy(way, i, target):
        return remote(s.chain_out.at[way, i], s.chain_in.at[way, i], s.hs.at[way, i],
                      s.hr.at[way, i], "sp", target)

    def chain(way, i, sources):
        c, part = i // halves, i % halves
        cols = slice(c * chunk_width, (c + 1) * chunk_width)
        rows = slice(part * part_keys, (part + 1) * part_keys)
        onward = 1 - 2 * way
        has_before = jnp.where(way == 0, sp > 0, sp < sp_count - 1)
        has_next = jnp.where(way == 0, sp < sp_count - 1, sp > 0)

        @pl.when(jnp.logical_and(has_next, jnp.logical_not(has_before)) if sources else has_before)
        def _():
            if not sources:
                chain_copy(way, i, sp - onward).wait_recv()

            @pl.when(has_next)
            def _():
                s.chain_out[way, i, :part_keys, :] = (
                    s.own_decay[way, rows, :] * s.chain_in[way, i, :part_keys, :].astype(f32)
                    + s.state[way, rows, cols]).astype(bf16)
                s.chain_out[way, i, part_keys:, :] = (
                    s.chain_in[way, i, part_keys:, :].astype(f32)
                    + s.carry[1 - way, rows, cols]).astype(bf16)
                chain_copy(way, i, sp + onward).start()

    def attend(b):
        rows = slice(b * size, (b + 1) * size)
        query = dot(s.mod_latent[rows, :], s.wqk[1]).astype(bf16)
        rq = rotate(query.astype(f32) * keys ** -0.5, s.cosine[rows, :], s.sine[rows, :])
        rk = s.key[rows, :]
        scores, out = None, None
        for direction in range(2):
            keep = triangle(size, direction == 1)
            middle = size // 2 if direction == 1 else size // 2 - 1
            cum = s.cum[direction, rows, :]
            center = cum[middle:middle + 1, :]
            q_mid = (rq * jnp.exp(cum - center)).astype(bf16)
            k_mid = (rk * jnp.exp(center - cum)).astype(bf16)
            score = jnp.where(keep, dot(q_mid, k_mid, ((1,), (1,))), 0.0)
            scores = score if scores is None else scores + score
            q_dec = rq * jnp.exp(cum)
            q_all = q_dec
            if b != (blocks - 1 if direction == 1 else 0):
                carried = dot(q_dec.astype(bf16), s.start[direction, b])
                out = carried if out is None else out + carried
                q_all = q_dec * jnp.exp(s.ahead[direction, b:b + 1, :])
            s.q_all[rows, direction * keys:(direction + 1) * keys] = q_all.astype(bf16)
        inner = dot(scores.astype(bf16), s.value[rows, :])
        s.mixture[rows, :] = inner if out is None else out + inner

    for i in range(steps):
        chain(first_way, i, True)
    for hop in range(2, sp_count - 1):
        for chunk in query_chunks:
            z_arrive(hop, chunk)
    load_gate_w.wait()
    gate_chip(x)
    gate_chip(1 - x)
    for hop in range(sp_count - 1):
        for chunk in query_chunks:
            y_each(hop, chunk, other_view, lambda c: c.wait_recv())
    lag = 2
    for turn in range(max(blocks, steps + lag)):
        if turn < blocks:
            attend(turn)
        if turn < steps:
            chain(first_way, turn, False)
        if turn >= lag:
            chain(1 - first_way, turn - lag, False)
    for c in range(chunk_count):
        cols = slice(c * chunk_width, (c + 1) * chunk_width)
        for part in range(halves):
            i = c * halves + part
            rows = slice(part * part_keys, (part + 1) * part_keys)
            for direction in range(2):
                joined = (s.chain_in[direction, i, :part_keys, :].astype(f32)
                          + s.ahead_decay[direction, rows, :]
                          * (s.carry[direction, rows, cols]
                             + s.chain_in[1 - direction, i, part_keys:, :].astype(f32)))
                start = direction * keys + part * part_keys
                s.joined[start:start + part_keys, cols] = joined.astype(bf16)
    for load in (load_norm_gain, load_out_w, load_final_gain, load_final_bias):
        load.wait()

    def gate_rows(chip):
        rows = pl.ds(pl.multiple_of(chip * 2 * own, 2 * own), 2 * own)
        mixture = s.mixture[rows, :] + dot(s.q_all[rows, :], s.joined[...])
        squares = jnp.mean(mixture * mixture, axis=1, keepdims=True)
        gate = s.gate[rows, :].astype(f32)
        normed = mixture * lax.rsqrt(squares + norm_eps) * s.norm_gain[...]
        s.gated[rows, :] = (normed * (gate / (1.0 + jnp.exp(-gate)))).astype(bf16)

    out_chunks = s.far_out.shape[0]
    out_width = width // out_chunks

    def product(j, n):
        cols = slice(n * out_width, (n + 1) * out_width)
        return dot(s.gated[block_rows(j), :], s.out_w[:, cols])

    def pair_copy(slot, n):
        return remote(s.pair_out.at[slot, n], s.pair_in.at[slot, n], s.ds.at[slot, n],
                      s.dr.at[slot, n], "tp", sibling)

    def far_copy(n):
        return remote(s.far_out.at[n], s.far_in.at[n], s.fs.at[n], s.fr.at[n],
                      "tp", across)

    gate_rows(1 - x)
    for n in range(out_chunks):
        s.pair_out[0, n] = product(far_sibling, n).astype(bf16)
        pair_copy(0, n).start()
    for n in range(out_chunks):
        mine = product(across, n)
        pair_copy(0, n).wait_recv()
        s.far_out[n] = (mine + s.pair_in[0, n].astype(f32)).astype(bf16)
        far_copy(n).start()
    gate_rows(x)
    for n in range(out_chunks):
        s.pair_out[1, n] = product(sibling, n).astype(bf16)
        pair_copy(1, n).start()
    for n in range(out_chunks):
        cols = slice(n * out_width, (n + 1) * out_width)
        mine = product(tp, n)
        pair_copy(1, n).wait_recv()
        s.branch[:, cols] = mine + s.pair_in[1, n].astype(f32)
    for n in range(out_chunks):
        cols = slice(n * out_width, (n + 1) * out_width)
        far_copy(n).wait_recv()
        branch = s.branch[:, cols] + s.far_in[n].astype(f32)
        s.branch[:, cols] = (residual_scale * s.rows[block_rows(tp), cols].astype(f32)
                                + s.branch_gate[:, cols] * branch)
    summed = s.branch[...]
    centered = summed - jnp.mean(summed, axis=1, keepdims=True)
    variance = jnp.mean(centered * centered, axis=1, keepdims=True)
    out_ref[...] = (centered * lax.rsqrt(variance + norm_eps) * s.final_gain[...]
                    + s.final_bias[...]).astype(bf16)

    part_drain()
    sums_drain()
    tot_drain()
    line.drain()
    for hop in range(sp_count - 1):
        for chunk in range(2 * PARTS):
            y_each(hop, chunk, weight_view(grp), lambda c: c.wait_send())
    for p in range(pieces):
        x_copy(tp, p).wait_send()
        cross(across, p, 1).wait_send()
    for way in range(2):
        has_next = sp < sp_count - 1 if way == 0 else sp > 0

        @pl.when(has_next)
        def _():
            for i in range(steps):
                chain_copy(way, i, sp + 1 if way == 0 else sp - 1).wait_send()
    for n in range(out_chunks):
        pair_copy(0, n).wait_send()
        pair_copy(1, n).wait_send()
        far_copy(n).wait_send()


def fused(latent, context, condition, context_condition, mod_weight, mod_bias, query_weight,
          key_weight, value_weight, out_gate_weight, decay_in_weight, decay_weight, decay_bias,
          extra_decay, norm_gain, out_weight, final_gain, final_bias):
    sp_count, tp_count = lax.axis_size("sp"), lax.axis_size("tp")
    own, width = latent.shape
    depth = query_weight.shape[0]
    keys = query_weight.shape[1] // ATTENTION_HEADS
    vals = value_weight.shape[1]
    ctx = context.shape[0]
    count = own * tp_count
    blocks = count // (2 * BLOCK)
    mod_cols = mod_weight.shape[1]
    chains, outs, pieces = 4, 4, 4
    args = (latent, context, condition[None, :], context_condition[None, :], mod_weight,
            mod_bias[None, :], query_weight, key_weight, value_weight, out_gate_weight,
            decay_in_weight.T, decay_weight, decay_bias, extra_decay, norm_gain[None, :],
            out_weight, final_gain[None, :], final_bias[None, :])
    dma, vmem = pltpu.SemaphoreType.DMA, pltpu.VMEM
    hops = sp_count - 1
    scratch = Scratch(
        cond=vmem((1, condition.shape[0]), f32),
        ctx_cond=vmem((1, condition.shape[0]), f32),
        mod_w=vmem(mod_weight.shape, bf16),
        mod_b=vmem((1, mod_bias.shape[0]), f32),
        wqk=vmem((2, depth * sp_count, keys), bf16),
        rows=vmem((count, width), bf16),
        mod_latent=vmem((count, width), bf16),
        context=vmem(context.shape, bf16),
        mod_context=vmem(context.shape, bf16),
        low_w=vmem(decay_in_weight.shape[::-1], bf16),
        value_w=vmem(value_weight.shape, bf16),
        gate_w=vmem(out_gate_weight.shape, bf16),
        out_w=vmem(out_weight.shape, bf16),
        decay_w=vmem(decay_weight.shape[:2] + (keys,), bf16),
        decay_b=vmem((2, keys), f32),
        extra=vmem(extra_decay.shape, f32),
        norm_gain=vmem((1, vals), f32),
        final_gain=vmem((1, width), f32),
        final_bias=vmem((1, width), f32),
        part=vmem((sp_count, 2, mod_cols), f32),
        sums=vmem((tp_count, 2, mod_cols), f32),
        totals=vmem((sp_count, 4, keys), f32),
        shifts=vmem((2, width), f32),
        scales=vmem((2, width), f32),
        branch_gate=vmem((1, width), f32),
        cosine=vmem((count, keys), f32),
        sine=vmem((count, keys), f32),
        ctx_close=vmem((2, ctx, keys), f32),
        ctx_value=vmem((ctx, vals), bf16),
        low=vmem((count, decay_in_weight.shape[1]), bf16),
        value=vmem((count, vals), bf16),
        gate=vmem((count, vals), bf16),
        key=vmem((count, keys), f32),
        cum=vmem((2, count, keys), f32),
        ahead=vmem((2, blocks, keys), f32),
        block_total=vmem((2, blocks, 1, keys), f32),
        total=vmem((2, keys), f32),
        start=vmem((2, blocks, keys, vals), bf16),
        state=vmem((2, keys, vals), f32),
        carry=vmem((2, keys, vals), f32),
        own_decay=vmem((2, keys, vals // chains), f32),
        ahead_decay=vmem((2, keys, vals // chains), f32),
        chain_in=vmem((2, 2 * chains, keys, vals // chains), bf16),
        chain_out=vmem((2, 2 * chains, keys, vals // chains), bf16),
        q_all=vmem((count, 2 * keys), bf16),
        mixture=vmem((count, vals), f32),
        joined=vmem((2 * keys, vals), bf16),
        gated=vmem((count, vals), bf16),
        pair_out=vmem((2, outs, own, width // outs), bf16),
        pair_in=vmem((2, outs, own, width // outs), bf16),
        far_out=vmem((outs, own, width // outs), bf16),
        far_in=vmem((outs, own, width // outs), bf16),
        branch=vmem((own, width), f32),
        load_sem=dma((len(args),)),
        zs=dma((2, hops, 2 * PARTS)), zr=dma((2, hops, 2 * PARTS)),
        ys=dma((2, hops, 2 * PARTS)), yr=dma((2, hops, 2 * PARTS)),
        xs=dma((pieces,)), xr=dma((pieces,)),
        cs=dma((2 * pieces,)), cr=dma((2 * pieces,)),
        ps=dma((hops,)), pr=dma((hops,)), ts=dma((hops,)), tr=dma((hops,)),
        ss=dma((tp_count - 1,)), sr=dma((tp_count - 1,)),
        hs=dma((2, 2 * chains)), hr=dma((2, 2 * chains)),
        ds=dma((2, outs)), dr=dma((2, outs)), fs=dma((outs,)), fr=dma((outs,)),
    )
    return pl.pallas_call(
        fused_kernel,
        out_shape=jax.ShapeDtypeStruct((own, width), bf16),
        in_specs=[pl.BlockSpec(memory_space=pltpu.HBM)] * len(args),
        out_specs=pl.BlockSpec(memory_space=pltpu.VMEM),
        scratch_shapes=[scratch],
        compiler_params=pltpu.CompilerParams(
            vmem_limit_bytes=60 * 1024 * 1024, collective_id=2, has_side_effects=True),
        cost_estimate=pl.CostEstimate(flops=6_000_000_000, bytes_accessed=12_000_000,
                                      transcendentals=2_000_000),
    )(*args)


def whole_heads(mesh):
    return mesh.shape["tp"] == ATTENTION_HEADS and mesh.shape["grp"] == 2


def solution(mesh):
    placed = (
        P(("grp", "sp", "tp"), None),
        P(("grp", "sp"), None),
        P(("grp", "sp")),
        P("sp"),
        P("sp", "tp"),
        P(),
        P("sp", None),
        P("sp", None),
        P(None, "tp"),
        P(None, "tp"),
        P(),
        P(),
        P(),
        P(None, None, "sp"),
        P(),
        P("tp", None),
        P(),
        P(),
    )
    return jax.shard_map(
        fused if whole_heads(mesh) else body, mesh=mesh, in_specs=placed, out_specs=P(("grp", "sp", "tp"), None), check_vma=False
    )
```

```python
import functools
from typing import Any, NamedTuple

import jax
import jax.numpy as jnp
from jax import lax
from jax.experimental import pallas as pl
from jax.experimental.pallas import tpu as pltpu
from jax.sharding import PartitionSpec as P

ATTENTION_HEADS = 4
DV = 512
BLOCK = 64
GRID_W = 64


norm_eps = 1e-05
gate_scale = 16.0
rope_base = 10000.0
residual_scale = 2.0**0.5
highest = lax.Precision.HIGHEST
f32 = jnp.float32
bf16 = jnp.bfloat16


def rope_tables(token_places, width):
    quarter = width // 4
    frequency = rope_base ** (-jnp.arange(quarter, dtype=f32) / quarter)
    row_angle = (token_places // GRID_W).astype(f32)[:, None] * frequency
    col_angle = (token_places % GRID_W).astype(f32)[:, None] * frequency
    cosine = jnp.concatenate([jnp.cos(row_angle)] * 2 + [jnp.cos(col_angle)] * 2, axis=1)
    row_sine, col_sine = jnp.sin(row_angle), jnp.sin(col_angle)
    sine = jnp.concatenate([-row_sine, row_sine, -col_sine, col_sine], axis=1)
    return cosine, sine


def dot(a, b, contract=((1,), (0,)), precision=None):
    return lax.dot_general(a, b, (contract, ((), ())), precision=precision,
                           preferred_element_type=f32)


def log_sigmoid(x):
    return jnp.minimum(x, 0.0) - jnp.log1p(jnp.exp(-jnp.abs(x)))


def rotate(x, cosine, sine):
    half = x.shape[1] // 2
    parts = [pltpu.roll(x[:, i * half:(i + 1) * half], half // 2, 1) for i in range(2)]
    return x * cosine + jnp.concatenate(parts, axis=1) * sine


def triangle(size, reverse):
    row = lax.broadcasted_iota(jnp.int32, (size, size), 0)
    col = lax.broadcasted_iota(jnp.int32, (size, size), 1)
    return row <= col if reverse else row >= col


def decay_block(low, decay_weight, decay_bias, direction):
    rank = decay_weight.shape[1]
    logits = dot(low[:, direction * rank:(direction + 1) * rank], decay_weight[direction])
    return log_sigmoid(logits + decay_bias[direction:direction + 1, :]) / gate_scale


def context_kernel(k_ref, v_ref, low_ref, dw_ref, db_ref, state_ref):
    length, width = k_ref.shape
    size = min(2 * BLOCK, length)
    count = length // size
    for direction in range(2):
        mask = triangle(size, direction == 1).astype(f32)
        edge = 0 if direction == 1 else size - 1
        state = None
        for step in range(count):
            b = count - 1 - step if direction == 1 else step
            rows = slice(b * size, (b + 1) * size)
            logdec = decay_block(low_ref[rows, :], dw_ref[...], db_ref[...], direction)
            cum = dot(mask, logdec, precision=highest)
            total = cum[edge:edge + 1, :]
            closing = (k_ref[rows, :].astype(f32) * jnp.exp(total - cum)).astype(bf16)
            term = dot(closing, v_ref[rows, :], ((0,), (0,)))
            state = term if state is None else jnp.exp(total).T * state + term
        state_ref[direction] = state


def local_kernel(q_ref, k_ref, v_ref, low_ref, extra_ref, dw_ref, db_ref, cos_ref, sin_ref,
                 out_ref, qc_ref, state_ref, total_ref):
    length, width = q_ref.shape
    size = 2 * BLOCK
    count = length // size
    rq, rk, within, scores = [], [], [], []
    for b in range(count):
        rows = slice(b * size, (b + 1) * size)
        cosine, sine = cos_ref[rows, :], sin_ref[rows, :]
        rq.append(rotate(q_ref[rows, :].astype(f32) * width ** -0.5, cosine, sine))
        rk.append(rotate(k_ref[rows, :].astype(f32), cosine, sine))
        scores.append(None)
    for direction in range(2):
        keep = triangle(size, direction == 1)
        mask = keep.astype(f32)
        edge = 0 if direction == 1 else size - 1
        middle = size // 2 if direction == 1 else size // 2 - 1
        state = None
        before = None
        for step in range(count):
            b = count - 1 - step if direction == 1 else step
            rows = slice(b * size, (b + 1) * size)
            logdec = decay_block(low_ref[rows, :], dw_ref[...], db_ref[...], direction)
            logdec = logdec + extra_ref[rows, direction:direction + 1]
            cum = dot(mask, logdec, precision=highest)
            total = cum[edge:edge + 1, :]
            center = cum[middle:middle + 1, :]
            q_mid = (rq[b] * jnp.exp(cum - center)).astype(bf16)
            k_mid = (rk[b] * jnp.exp(center - cum)).astype(bf16)
            score = jnp.where(keep, dot(q_mid, k_mid, ((1,), (1,))), 0.0)
            q_dec = rq[b] * jnp.exp(cum)
            if direction == 0:
                scores[b] = score
                out = None
            else:
                out = dot((scores[b] + score).astype(bf16), v_ref[rows, :])
            if state is not None:
                carried = dot(q_dec.astype(bf16), state.astype(bf16))
                out = carried if out is None else out + carried
            if direction == 0:
                out_ref[rows, :] = jnp.zeros((size, v_ref.shape[1]), f32) if out is None else out
            else:
                out_ref[rows, :] += out
            q_all = q_dec if before is None else q_dec * jnp.exp(before)
            qc_ref[rows, direction * width:(direction + 1) * width] = q_all.astype(bf16)
            closing = (rk[b] * jnp.exp(total - cum)).astype(bf16)
            term = dot(closing, v_ref[rows, :], ((0,), (0,)))
            state = term if state is None else jnp.exp(total).T * state + term
            before = total if before is None else before + total
        state_ref[direction * width:(direction + 1) * width, :] = state.astype(bf16)
        total_ref[direction:direction + 1, :] = before


def join_kernel(final, out_ref, qc_ref, states_ref, totals_ref, start_ref, gate_ref, gain_ref,
                place_ref, result_ref):
    count = states_ref.shape[0]
    width = qc_ref.shape[1] // 2
    place = place_ref[...]
    mixture = out_ref[...]
    for direction in range(2):
        state = start_ref[direction]
        for lap in range(count):
            j = count - 1 - lap if direction == 1 else lap
            decay = jnp.exp(totals_ref[j, direction:direction + 1, :]).T
            joined = decay * state + states_ref[
                j, direction * width:(direction + 1) * width, :].astype(f32)
            ahead = place < j if direction == 1 else place > j
            state = jnp.where(ahead, joined, state)
        mixture = mixture + dot(qc_ref[:, direction * width:(direction + 1) * width],
                                state.astype(bf16))
    if final:
        squares = jnp.mean(mixture * mixture, axis=1, keepdims=True)
        gate = gate_ref[...].astype(f32)
        normed = mixture * lax.rsqrt(squares + norm_eps) * gain_ref[...]
        result_ref[...] = (normed * (gate / (1.0 + jnp.exp(-gate)))).astype(bf16)
    else:
        result_ref[...] = mixture


def call(kernel, out_shape, *args):
    return pl.pallas_call(
        kernel,
        out_shape=out_shape,
        in_specs=[pl.BlockSpec(memory_space=pltpu.VMEM)] * len(args),
        out_specs=jax.tree.map(lambda _: pl.BlockSpec(memory_space=pltpu.VMEM), out_shape),
        compiler_params=pltpu.CompilerParams(vmem_limit_bytes=48 * 1024 * 1024),
        cost_estimate=pl.CostEstimate(flops=4_000_000_000, bytes_accessed=4_000_000,
                                      transcendentals=1_000_000),
    )(*args)


MESH = pl.DeviceIdType.MESH


def remote(src, dst, send_sem, recv_sem, axis, target):
    return pltpu.make_async_remote_copy(
        src_ref=src, dst_ref=dst, send_sem=send_sem, recv_sem=recv_sem,
        device_id={axis: target}, device_id_type=MESH)


class Line:
    def __init__(self, place, count, axis, target_of, view, chunks, send_sem, recv_sem):
        self.place, self.count, self.axis, self.target_of = place, count, axis, target_of
        self.view, self.chunks, self.send_sem, self.recv_sem = view, chunks, send_sem, recv_sem

    def copy(self, way, hop, chunk, block, target):
        ref = self.view(block, chunk)
        return remote(ref, ref, self.send_sem.at[way, hop, chunk],
                      self.recv_sem.at[way, hop, chunk], self.axis, self.target_of(target))

    def outgoing(self, way, hop):
        place, count = self.place, self.count
        if way == 0:
            return place - hop, place + 1, jnp.logical_and(place >= hop, place < count - 1)
        return place + hop, place - 1, jnp.logical_and(place + hop < count, place > 0)

    def each_send(self, way, hop, chunk, act):
        block, target, valid = self.outgoing(way, hop)

        @pl.when(valid)
        def _():
            act(self.copy(way, hop, chunk, block, target))

    def send(self, way, hop, chunk):
        self.each_send(way, hop, chunk, lambda c: c.start())

    def drain(self):
        for way in range(2):
            for hop in range(self.count - 1):
                for chunk in range(self.chunks):
                    self.each_send(way, hop, chunk, lambda c: c.wait_send())

    def arrive(self, way, hop, chunk, then=None):
        if way == 0:
            block, source, valid = self.place - 1 - hop, self.place - 1, self.place > hop
        else:
            block, source = self.place + 1 + hop, self.place + 1
            valid = self.place + 1 + hop < self.count

        @pl.when(valid)
        def _():
            self.copy(way, hop, chunk, block, source).wait_recv()
            if then is not None:
                then(block)

    def forward(self, hop, then=None):
        for chunk in range(self.chunks):
            for way in range(2):
                self.arrive(way, hop, chunk, None if then is None else functools.partial(then, way))
                if hop + 1 < self.count - 1:
                    self.send(way, hop + 1, chunk)


def open_kernel(partners):
    barrier = pltpu.get_barrier_semaphore()
    for axis, target in partners:
        pl.semaphore_signal(barrier, inc=1, device_id={axis: target}, device_id_type=MESH)
    return lambda: pl.semaphore_wait(barrier, len(partners))


def others(axis):
    count, place = lax.axis_size(axis), lax.axis_index(axis)
    return [lax.rem(place + k, count) for k in range(1, count)]


def sources(axis):
    count, place = lax.axis_size(axis), lax.axis_index(axis)
    return [lax.rem(place + count - k, count) for k in range(1, count)]


def spread(buffer, axis, send_sem, recv_sem):
    place = lax.axis_index(axis)
    for k, target in enumerate(others(axis)):
        remote(buffer.at[place], buffer.at[place], send_sem.at[k], recv_sem.at[k],
               axis, target).start()


def spread_arrive(buffer, axis, send_sem, recv_sem):
    for k, source in enumerate(sources(axis)):
        remote(buffer.at[source], buffer.at[source], send_sem.at[k], recv_sem.at[k],
               axis, source).wait_recv()


def spread_drain(buffer, axis, send_sem, recv_sem):
    place = lax.axis_index(axis)
    for k, target in enumerate(others(axis)):
        remote(buffer.at[place], buffer.at[place], send_sem.at[k], recv_sem.at[k],
               axis, target).wait_send()


def enter_kernel(chunks, latent_ref, context_ref, cond_ref, mw_ref, mb_ref, qw_ref, kw_ref,
                 ml_ref, mc_ref, gate_ref, qk_ref,
                 rows_ref, part_ref, sums_ref, zs, zr, xs, xr, cs, cr, ps, pr, ss, sr):
    sp, sp_count = lax.axis_index("sp"), lax.axis_size("sp")
    tp, tp_count = lax.axis_index("tp"), lax.axis_size("tp")
    own, model_width = latent_ref.shape
    depth = qw_ref.shape[0]
    head_keys = qk_ref.shape[1] // 2
    ready = open_kernel([("sp", t) for t in others("sp")] + [("tp", t) for t in others("tp")])
    v = cond_ref[...]
    activated = (v / (1.0 + jnp.exp(-v))).astype(bf16)
    part_ref[sp] = dot(activated, mw_ref[...])
    columns = pl.ds(pl.multiple_of((tp // (tp_count // ATTENTION_HEADS)) * head_keys, head_keys),
                    head_keys)
    qk_rows = pl.ds(pl.multiple_of(sp * depth, depth), depth)
    qk_ref[qk_rows, :head_keys] = qw_ref[:, columns]
    qk_ref[qk_rows, head_keys:] = kw_ref[:, columns]
    rows_ref[pl.ds(pl.multiple_of(tp * own, own), own), :] = latent_ref[...]

    step = depth // chunks
    z_line = Line(
        sp, sp_count, "sp", lambda p: p,
        lambda block, chunk: qk_ref.at[
            pl.ds(pl.multiple_of(block * depth + chunk * step, step), step), :],
        chunks, zs, zr)
    x_count = tp_count // 2
    x, core = tp // 2, tp % 2

    def rows_of(block, chunk):
        return rows_ref.at[pl.ds(pl.multiple_of((2 * block + core) * own, own), own), :]

    x_line = Line(x, x_count, "tp", lambda p: 2 * p + core, rows_of, 1, xs, xr)
    sibling = tp + 1 - 2 * core

    def cross(block, slot, other=False):
        side = 1 - core if other else core
        ref = rows_ref.at[pl.ds(pl.multiple_of((2 * block + side) * own, own), own), :]
        return remote(ref, ref, cs.at[slot], cr.at[slot], "tp", sibling)

    def slot_of(way, hop):
        return 1 + way * (x_count - 1) + hop

    ready()
    spread(part_ref, "sp", ps, pr)
    for way in range(2):
        x_line.send(way, 0, 0)
    cross(x, 0).start()
    for chunk in range(chunks):
        for way in range(2):
            z_line.send(way, 0, chunk)
    spread_arrive(part_ref, "sp", ps, pr)
    total = part_ref[0]
    for j in range(1, sp_count):
        total = total + part_ref[j]
    sums_ref[tp] = total
    spread(sums_ref, "tp", ss, sr)
    z_line.forward(0)
    for hop in range(x_count - 1):
        x_line.forward(hop, lambda way, block, hop=hop: cross(block, slot_of(way, hop)).start())
    if sp_count > 2:
        z_line.forward(1)
    spread_arrive(sums_ref, "tp", ss, sr)
    modulation = jnp.concatenate([sums_ref[j] for j in range(tp_count)], axis=1) + mb_ref[...]
    shifts = modulation[:, :model_width]
    scales = modulation[:, model_width:2 * model_width]
    gate_ref[...] = modulation[0:1, 2 * model_width:]
    mc_ref[...] = (context_ref[...].astype(f32) * (1.0 + scales[1:2]) + shifts[1:2]).astype(bf16)

    def each_cross(act_own, act_line):
        act_own()
        for way in range(2):
            for hop in range(x_count - 1):
                block = x - 1 - hop if way == 0 else x + 1 + hop
                valid = x > hop if way == 0 else x + 1 + hop < x_count

                @pl.when(valid)
                def _():
                    act_line(block, slot_of(way, hop))

    each_cross(lambda: cross(x, 0, True).wait_recv(),
               lambda block, slot: cross(block, slot, True).wait_recv())
    for j in range(tp_count):
        rows = slice(j * own, (j + 1) * own)
        ml_ref[rows, :] = (rows_ref[rows, :].astype(f32) * (1.0 + scales[0:1])
                           + shifts[0:1]).astype(bf16)
    for hop in range(2, sp_count - 1):
        z_line.forward(hop)
    each_cross(lambda: cross(x, 0).wait_send(),
               lambda block, slot: cross(block, slot).wait_send())
    spread_drain(part_ref, "sp", ps, pr)
    spread_drain(sums_ref, "tp", ss, sr)
    x_line.drain()
    z_line.drain()


def comm_call(kernel, out_shape, scratch, collective_id, *args):
    return pl.pallas_call(
        kernel,
        out_shape=out_shape,
        in_specs=[pl.BlockSpec(memory_space=pltpu.VMEM)] * len(args),
        out_specs=jax.tree.map(lambda _: pl.BlockSpec(memory_space=pltpu.VMEM), out_shape),
        scratch_shapes=scratch,
        compiler_params=pltpu.CompilerParams(
            vmem_limit_bytes=48 * 1024 * 1024, collective_id=collective_id,
            has_side_effects=True),
        cost_estimate=pl.CostEstimate(flops=20_000_000_000, bytes_accessed=60_000_000,
                                      transcendentals=1_000_000),
    )(*args)


def enter(latent, context, cond, mod_weight, mod_bias, query_weight, key_weight):
    sp_count, tp_count = lax.axis_size("sp"), lax.axis_size("tp")
    own, model_width = latent.shape
    depth = query_weight.shape[0]
    head_keys = query_weight.shape[1] // ATTENTION_HEADS
    chunks = 4
    sds = jax.ShapeDtypeStruct
    dma = pltpu.SemaphoreType.DMA
    x_hops = tp_count // 2 - 1
    return comm_call(
        functools.partial(enter_kernel, chunks),
        (
            sds((own * tp_count, model_width), bf16),
            sds(context.shape, bf16),
            sds((1, model_width), f32),
            sds((depth * sp_count, 2 * head_keys), bf16),
        ),
        [
            pltpu.VMEM((own * tp_count, model_width), bf16),
            pltpu.VMEM((sp_count, 2, mod_weight.shape[1]), f32),
            pltpu.VMEM((tp_count, 2, mod_weight.shape[1]), f32),
            dma((2, sp_count - 1, chunks)), dma((2, sp_count - 1, chunks)),
            dma((2, x_hops, 1)), dma((2, x_hops, 1)),
            dma((1 + 2 * x_hops,)), dma((1 + 2 * x_hops,)),
            dma((sp_count - 1,)), dma((sp_count - 1,)),
            dma((tp_count - 1,)), dma((tp_count - 1,)),
        ],
        1, latent, context, cond, mod_weight, mod_bias[None, :], query_weight, key_weight,
    )


def project(rows, weight):
    return jnp.dot(rows, weight, preferred_element_type=f32).astype(bf16)


def body(
    latent,
    context,
    condition,
    context_condition,
    mod_weight,
    mod_bias,
    query_weight,
    key_weight,
    value_weight,
    out_gate_weight,
    decay_in_weight,
    decay_weight,
    decay_bias,
    extra_decay,
    norm_gain,
    out_weight,
    final_gain,
    final_bias,
):
    head_keys = query_weight.shape[1] // ATTENTION_HEADS
    value_cols = value_weight.shape[1]
    tp_index = lax.axis_index("tp")
    sp_index = lax.axis_index("sp")
    head_share = lax.axis_size("tp") // ATTENTION_HEADS
    head_index = tp_index // head_share
    part_index = tp_index % head_share
    key_start = head_index * head_keys

    full_out = lax.all_gather(out_weight, "tp", axis=0, tiled=True)
    mod_latent, mod_context, branch_gate, qk_head = enter(
        latent, context, jnp.stack([condition, context_condition]), mod_weight, mod_bias,
        query_weight, key_weight,
    )
    context_local = jnp.concatenate(
        [
            project(mod_context, qk_head[:, head_keys:]),
            project(mod_context, value_weight),
            project(mod_context, decay_in_weight),
        ],
        axis=1,
    )
    gathered_context = lax.all_gather(context_local, "sp", axis=0, tiled=True)
    qk = project(mod_latent, qk_head)
    value_rows = project(mod_latent, value_weight)
    out_gate = project(mod_latent, out_gate_weight)
    low_rank = project(mod_latent, decay_in_weight)
    count = mod_latent.shape[0]
    token_places = sp_index * count + jnp.arange(count, dtype=jnp.int32)
    cosine, sine = rope_tables(token_places, head_keys)
    head_bias = lax.dynamic_slice_in_dim(decay_bias, key_start, head_keys, 1)
    head_gate = lax.dynamic_slice_in_dim(decay_weight, key_start, head_keys, 2)
    head_extra = lax.dynamic_index_in_dim(extra_decay, head_index, 1, keepdims=False).T

    sds = jax.ShapeDtypeStruct
    out_local, qc, states, totals = call(
        local_kernel,
        (
            sds((count, value_cols), f32),
            sds((count, 2 * head_keys), bf16),
            sds((2 * head_keys, value_cols), bf16),
            sds((2, head_keys), f32),
        ),
        qk[:, :head_keys], qk[:, head_keys:], value_rows, low_rank, head_extra, head_gate,
        head_bias, cosine, sine,
    )
    start = call(
        context_kernel,
        sds((2, head_keys, value_cols), f32),
        gathered_context[:, :head_keys],
        gathered_context[:, head_keys : head_keys + value_cols],
        gathered_context[:, head_keys + value_cols :],
        head_gate, head_bias,
    )
    states, totals, full_out = lax.optimization_barrier((states, totals, full_out))
    all_states = lax.all_gather(states, "sp")
    all_totals = lax.all_gather(totals, "sp")
    place = jnp.full((1, value_cols), sp_index, jnp.int32)
    gain_slice = lax.dynamic_slice_in_dim(norm_gain, part_index * value_cols, value_cols, 0)
    final = head_share == 1
    joined = call(
        functools.partial(join_kernel, final),
        sds((count, value_cols), bf16 if final else f32),
        out_local, qc, all_states, all_totals, start, out_gate, gain_slice[None, :], place,
    )
    if final:
        gated_rows = joined
    else:
        squares = jnp.sum(joined * joined, axis=1)
        onehot = (jnp.arange(ATTENTION_HEADS) == head_index).astype(f32)
        sums = lax.psum(onehot[:, None] * squares[None, :], "tp")
        head_sum = jnp.sum(sums * onehot[:, None], axis=0)
        normed = joined * lax.rsqrt(head_sum / DV + norm_eps)[:, None] * gain_slice
        gated_rows = (normed * jax.nn.silu(out_gate.astype(f32))).astype(bf16)
    regrouped = lax.all_to_all(gated_rows, "tp", split_axis=0, concat_axis=1, tiled=True)
    branch = jnp.dot(regrouped, full_out, preferred_element_type=f32)
    summed = residual_scale * latent.astype(f32) + branch_gate * branch
    row_mean = jnp.mean(summed, axis=1, keepdims=True)
    centered = summed - row_mean
    variance = jnp.mean(centered * centered, axis=1, keepdims=True)
    return (centered * lax.rsqrt(variance + norm_eps) * final_gain + final_bias).astype(bf16)


class Scratch(NamedTuple):
    cond: Any
    ctx_cond: Any
    mod_w: Any
    mod_b: Any
    wqk: Any
    rows: Any
    mod_latent: Any
    context: Any
    mod_context: Any
    low_w: Any
    value_w: Any
    gate_w: Any
    out_w: Any
    decay_w: Any
    decay_b: Any
    extra: Any
    norm_gain: Any
    final_gain: Any
    final_bias: Any
    part: Any
    sums: Any
    totals: Any
    ctx_totals: Any
    shifts: Any
    scales: Any
    branch_gate: Any
    cosine: Any
    sine: Any
    ctx_close: Any
    ctx_value: Any
    low: Any
    value: Any
    gate: Any
    key: Any
    cum: Any
    ahead: Any
    block_total: Any
    total: Any
    start: Any
    state: Any
    carry: Any
    own_decay: Any
    ahead_decay: Any
    chain_in: Any
    chain_out: Any
    q_all: Any
    mixture: Any
    joined: Any
    gated: Any
    gathered: Any
    branch: Any
    load_sem: Any
    zs: Any
    zr: Any
    ys: Any
    yr: Any
    xs: Any
    xr: Any
    cs: Any
    cr: Any
    ocs: Any
    ocr: Any
    ods: Any
    odr: Any
    oxs: Any
    oxr: Any
    oys: Any
    oyr: Any
    gs: Any
    gr: Any
    ps: Any
    pr: Any
    ts: Any
    tr: Any
    us: Any
    ur: Any
    ss: Any
    sr: Any
    hs: Any
    hr: Any


def spread_of(ref, axis, send_sem, recv_sem):
    return (lambda: spread(ref, axis, send_sem, recv_sem),
            lambda: spread_arrive(ref, axis, send_sem, recv_sem),
            lambda: spread_drain(ref, axis, send_sem, recv_sem))


class SharedLine(Line):
    def copy(self, way, hop, chunk, block, target):
        ref = self.view(block, chunk)
        return remote(ref, ref, self.send_sem.at[way, hop], self.recv_sem.at[way, hop, chunk],
                      self.axis, self.target_of(target))

    def drain_whole(self, whole):
        for way in range(2):
            for hop in range(self.count - 1):
                block, target, valid = self.outgoing(way, hop)

                @pl.when(valid)
                def _():
                    remote(whole, whole, self.send_sem.at[way, hop],
                           self.recv_sem.at[way, hop, 0], self.axis,
                           self.target_of(target)).wait_send()


PARTS = 4


def fused_kernel(latent, context, cond, ctx_cond, mod_w, mod_b, query_w, key_w, value_w, gate_w,
                 low_w, decay_w, decay_b, extra, norm_gain, out_w, final_gain, final_bias,
                 out_ref, s):
    grp = lax.axis_index("grp")
    sp, sp_count = lax.axis_index("sp"), lax.axis_size("sp")
    tp, tp_count = lax.axis_index("tp"), lax.axis_size("tp")
    own, width = latent.shape
    depth = query_w.shape[0]
    keys = query_w.shape[1] // ATTENTION_HEADS
    vals = value_w.shape[1]
    count = own * tp_count
    size = 2 * BLOCK
    blocks = count // size
    ctx = context.shape[0]
    x, core = tp // 2, tp % 2
    sibling, across = tp + 1 - 2 * core, 2 * (1 - x) + core
    far_sibling = 2 * (1 - x) + 1 - core

    def block_rows(j):
        return pl.ds(pl.multiple_of(j * own, own), own)

    ready = open_kernel([("sp", t) for t in others("sp")] + [("tp", t) for t in others("tp")]
                        + [("grp", 1 - grp)])
    head_cols = pl.ds(pl.multiple_of(tp * keys, keys), keys)
    own_depth = pl.ds(pl.multiple_of(sp * depth, depth), depth)
    loads = []
    for i, (source, target) in enumerate((
        (latent, s.rows.at[block_rows(tp), :]),
        (cond, s.cond), (ctx_cond, s.ctx_cond), (mod_w, s.mod_w),
        (key_w.at[:, head_cols], s.wqk.at[0, own_depth, :]),
        (query_w.at[:, head_cols], s.wqk.at[1, own_depth, :]),
        (mod_b, s.mod_b), (context, s.context),
        (low_w, s.low_w), (value_w, s.value_w),
        (decay_w.at[:, :, head_cols], s.decay_w),
        (decay_b.at[:, head_cols], s.decay_b), (extra, s.extra),
        (gate_w, s.gate_w), (norm_gain, s.norm_gain),
        (out_w, s.out_w.at[tp]), (final_gain, s.final_gain),
        (final_bias, s.final_bias),
    )):
        loads.append(pltpu.make_async_copy(source, target, s.load_sem.at[i]))
        loads[i].start()
    (load_latent, load_cond, load_ctx_cond, load_mod_w, load_key_w, load_query_w,
     load_mod_b, load_context, load_low_w, load_value_w, load_decay_w, load_decay_b,
     load_extra, load_gate_w, load_norm_gain, load_out_w, load_final_gain, load_final_bias) = loads

    half = depth // 2
    step = half // PARTS

    def weight_view(side):
        def view(block, chunk):
            start = block * depth + side * half + (chunk % PARTS) * step
            return s.wqk.at[chunk // PARTS, pl.ds(pl.multiple_of(start, step), step), :]
        return view

    line = SharedLine(sp, sp_count, "sp", lambda p: p, weight_view(grp), 2 * PARTS, s.zs, s.zr)

    def y_copy(ref, way, hop, matrix):
        return remote(ref, ref, s.ys.at[way, hop], s.yr.at[way, hop, matrix], "grp", 1 - grp)

    def z_arrive(hop, chunk, pass_on=True):
        for way in range(2):
            line.arrive(way, hop, chunk, (lambda block: y_copy(
                weight_view(grp)(block, chunk), way, hop, chunk // PARTS).start()) if pass_on else None)
            if hop + 1 < sp_count - 1:
                line.send(way, hop + 1, chunk)

    def y_each(hop, act):
        for way in range(2):
            block = sp - 1 - hop if way == 0 else sp + 1 + hop
            valid = sp > hop if way == 0 else sp + 1 + hop < sp_count

            @pl.when(valid)
            def _():
                act(block, way)

    def y_start(hop, chunk):
        y_each(hop, lambda block, way: y_copy(
            weight_view(grp)(block, chunk), way, hop, chunk // PARTS).start())

    def y_arrive(matrix):
        def wait(hop, block, way):
            start = pl.multiple_of(block * depth + (1 - grp) * half, half)
            y_copy(s.wqk.at[matrix, pl.ds(start, half), :], way, hop, matrix).wait_recv()

        for hop in range(sp_count - 1):
            y_each(hop, functools.partial(wait, hop))

    def y_drain():
        whole = s.wqk.at[0, pl.ds(0, depth), :]
        for hop in range(sp_count - 1):
            y_each(hop, lambda block, way: y_copy(whole, way, hop, 0).wait_send())

    key_chunks, query_chunks = range(PARTS), range(PARTS, 2 * PARTS)

    def send_own(chunks):
        for chunk in chunks:
            for way in range(2):
                line.send(way, 0, chunk)

    pieces, early = s.xr.shape[0], 3
    piece = own // pieces

    def rows_piece(j, p):
        return s.rows.at[pl.ds(pl.multiple_of(j * own + p * piece, piece), piece), :]

    def x_copy(j, p):
        return remote(rows_piece(j, p), rows_piece(j, p), s.xs.at[0], s.xr.at[p],
                      "tp", across)

    def cross(j, p, slot):
        return remote(rows_piece(j, p), rows_piece(j, p), s.cs.at[slot], s.cr.at[slot],
                      "tp", sibling)

    def cross_whole(j, slot):
        ref = s.rows.at[block_rows(j), :]
        return remote(ref, ref, s.cs.at[slot], s.cr.at[slot], "tp", sibling)

    out_rows = s.out_w.shape[1]
    out_half = out_rows // 2
    out_pieces = s.oyr.shape[0]
    out_step = out_half // out_pieces

    direct = out_pieces // 4
    shared = out_pieces - direct

    def out_piece(j, side, p):
        start = pl.multiple_of(side * out_half + p * out_step, out_step)
        return s.out_w.at[j, pl.ds(start, out_step), :]

    def out_bytes(count):
        return s.out_w.at[tp, pl.ds(0, count * out_step), :]

    def out_own_copy(j=tp):
        return remote(s.out_w.at[j], s.out_w.at[j], s.ocs.at[0], s.ocr.at[0], "tp", sibling)

    def out_x(j, k):
        side, p = (grp, k) if k < out_pieces else (1 - grp, shared + k - out_pieces)
        ref = out_piece(j, side, p)
        return remote(ref, ref, s.oxs.at[0], s.oxr.at[k], "tp", across)

    def out_y(side, p):
        ref = out_piece(across, side, p)
        return remote(ref, ref, s.oys.at[0], s.oyr.at[p], "grp", 1 - grp)

    def out_pass(ref, way):
        return remote(ref, ref, s.ods.at[way], s.odr.at[way], "tp", sibling)

    def relay_x(k):
        copy = out_x(across, k)
        copy.wait_recv()
        if k < shared:
            out_y(grp, k).start()
        side, p = (grp, k) if k < out_pieces else (1 - grp, shared + k - out_pieces)
        out_pass(out_piece(across, side, p), 0).start()

    def relay_y(p):
        out_y(1 - grp, p).wait_recv()
        out_pass(out_piece(across, 1 - grp, p), 1).start()

    part_go, part_arrive, part_drain = spread_of(s.part, "sp", s.ps, s.pr)
    sums_go, sums_arrive, sums_drain = spread_of(s.sums, "tp", s.ss, s.sr)
    tot_go, tot_arrive, tot_drain = spread_of(s.totals, "sp", s.ts, s.tr)
    ctx_go, ctx_arrive, ctx_drain = spread_of(s.ctx_totals, "sp", s.us, s.ur)

    load_latent.wait()
    ready()
    for p in range(pieces):
        if p < early:
            x_copy(tp, p).start()
        cross(tp, p, 0).start()
    for load in (load_cond, load_ctx_cond, load_mod_w):
        load.wait()
    v = jnp.concatenate([s.cond[...], s.ctx_cond[...]], axis=0)
    activated = (v / (1.0 + jnp.exp(-v))).astype(bf16)
    s.part[sp] = dot(activated, s.mod_w[...])
    part_go()
    load_key_w.wait()
    load_query_w.wait()
    send_own(key_chunks)
    send_own(query_chunks[:PARTS // 2])

    quarter = keys // 4

    def rope(b, carry):
        rows = pl.ds(pl.multiple_of(b * size, size), size)
        lane = lax.broadcasted_iota(jnp.int32, (1, keys), 1)
        index = jnp.bitwise_and(lane, quarter - 1).astype(f32)
        frequency = jnp.exp(index * (-jnp.log(rope_base) / quarter))
        by_row = lane < keys // 2
        first = jnp.bitwise_and(lane, 2 * quarter - 1) < quarter
        place = lax.broadcasted_iota(jnp.int32, (size, 1), 0) + (sp * count + b * size)
        place = place.astype(f32)
        row = jnp.floor((place + 0.5) * (1.0 / GRID_W))
        col = place - row * GRID_W
        angle = jnp.where(by_row, row, col) * frequency
        s.cosine[rows, :] = jnp.cos(angle)
        sine = jnp.sin(angle)
        s.sine[rows, :] = jnp.where(first, -sine, sine)
        return carry

    lax.fori_loop(0, blocks, rope, 0)

    @pl.when(sp == 0)
    def _():
        s.chain_in[0] = jnp.zeros(s.chain_in.shape[1:], bf16)

    @pl.when(sp == sp_count - 1)
    def _():
        s.chain_in[1] = jnp.zeros(s.chain_in.shape[1:], bf16)

    part_arrive()
    total = s.part[0]
    for j in range(1, sp_count):
        total = total + s.part[j]
    s.sums[tp] = total
    sums_go()
    for p in range(early, pieces):
        x_copy(tp, p).start()
    load_out_w.wait()
    out_own_copy().start()
    for k in range(out_pieces + direct):
        out_x(tp, k).start()
    for chunk in key_chunks:
        z_arrive(0, chunk)
    send_own(query_chunks[PARTS // 2:])
    sums_arrive()
    for load in (load_mod_b, load_context, load_low_w, load_value_w, load_decay_w, load_decay_b, load_extra):
        load.wait()
    modulation = (jnp.concatenate([s.sums[j] for j in range(tp_count)], axis=1)
                  + s.mod_b[...])
    s.shifts[...] = modulation[:, :width]
    s.scales[...] = 1.0 + modulation[:, width:2 * width]
    s.branch_gate[...] = modulation[0:1, 2 * width:]
    s.mod_context[...] = (s.context[...].astype(f32) * s.scales[1:2, :]
                             + s.shifts[1:2, :]).astype(bf16)

    def decay_of(low, direction):
        rank = s.decay_w.shape[1]
        logits = dot(low[:, direction * rank:(direction + 1) * rank], s.decay_w[direction])
        return log_sigmoid(logits + s.decay_b[direction:direction + 1, :]) / gate_scale

    own_head = lax.broadcasted_iota(jnp.int32, (ATTENTION_HEADS, size), 0) == tp

    def project_chip(chip):
        rows = pl.ds(pl.multiple_of(chip * 2 * own, 2 * own), 2 * own)
        mod = (s.rows[rows, :].astype(f32) * s.scales[0:1, :]
               + s.shifts[0:1, :]).astype(bf16)
        s.mod_latent[rows, :] = mod
        s.low[rows, :] = dot(mod, s.low_w[...], ((1,), (1,))).astype(bf16)
        s.value[rows, :] = dot(mod, s.value_w[...]).astype(bf16)

    def gate_chip(chip):
        rows = pl.ds(pl.multiple_of(chip * 2 * own, 2 * own), 2 * own)
        s.gate[rows, :] = dot(s.mod_latent[rows, :], s.gate_w[...]).astype(bf16)

    def decay_chip(chip):
        for i in range(2 * own // size):
            b = chip * (2 * own // size) + i
            rows = pl.ds(pl.multiple_of(b * size, size), size)
            low = s.low[rows, :]
            for direction in range(2):
                mask = triangle(size, direction == 1).astype(f32)
                edge = 0 if direction == 1 else size - 1
                head_extra = jnp.sum(jnp.where(own_head, s.extra[direction, :, rows], 0.0),
                                     axis=0, keepdims=True)
                added = jnp.sum(mask * head_extra, axis=1, keepdims=True)
                cum = dot(mask, decay_of(low, direction), precision=highest) + added
                s.cum[direction, rows, :] = cum
                s.block_total[direction, b] = cum[edge:edge + 1, :]

    ctx_low = dot(s.mod_context[...], s.low_w[...], ((1,), (1,))).astype(bf16)
    ctx_totals = []
    for direction in range(2):
        mask = triangle(ctx, direction == 1).astype(f32)
        edge = 0 if direction == 1 else ctx - 1
        cum = dot(mask, decay_of(ctx_low, direction), precision=highest)
        ctx_totals.append(cum[edge:edge + 1, :])
        s.ctx_close[direction] = jnp.exp(ctx_totals[direction] - cum)
    s.ctx_totals[sp] = jnp.concatenate(ctx_totals, axis=0)
    ctx_go()
    s.ctx_value[...] = dot(s.mod_context[...], s.value_w[...]).astype(bf16)
    for chunk in key_chunks:
        if sp_count > 2:
            z_arrive(1, chunk)
    cross_whole(sibling, 0).wait_recv()
    project_chip(x)
    decay_chip(x)
    for chunk in query_chunks:
        z_arrive(0, chunk, False)
    for hop in range(2, sp_count - 1):
        for chunk in key_chunks:
            z_arrive(hop, chunk)
    for chunk in query_chunks:
        y_start(0, chunk)
    for p in range(pieces):
        x_copy(across, p).wait_recv()
        cross(across, p, 1).start()
    load_gate_w.wait()
    gate_chip(x)
    cross_whole(far_sibling, 1).wait_recv()
    project_chip(1 - x)
    if sp_count > 2:
        for chunk in query_chunks:
            z_arrive(1, chunk)
    decay_chip(1 - x)
    for direction in range(2):
        before = None
        for turn in range(blocks):
            b = blocks - 1 - turn if direction == 1 else turn
            if before is not None:
                s.ahead[direction, b:b + 1, :] = before
            block_total = s.block_total[direction, b]
            before = block_total if before is None else before + block_total
        s.total[direction:direction + 1, :] = before
    s.totals[sp] = s.total[...]
    tot_go()
    y_arrive(0)
    chunk_width = s.chain_in.shape[4]
    part_keys = s.chain_in.shape[3]
    chunk_count = vals // chunk_width
    turns_each = s.chain_in.shape[2]
    steps = 2 * turns_each

    def column(row):
        return jnp.broadcast_to(jnp.exp(row).T, (keys, chunk_width))

    def column_chunks():
        return [slice(c * chunk_width, (c + 1) * chunk_width) for c in range(chunk_count)]

    def sum_of(ref, direction, later):
        total = jnp.zeros((1, keys), f32)
        for j in range(sp_count):
            chosen = (j > sp) if later else (j < sp)
            total = total + jnp.where(chosen, ref[j, direction:direction + 1, :], 0.0)
        return total

    ctx_key = dot(s.mod_context[...], s.wqk[0]).astype(bf16).astype(f32)
    ctx_arrive()
    for direction in range(2):
        closing = (ctx_key * s.ctx_close[direction]).astype(bf16)
        after = column(sum_of(s.ctx_totals, direction, direction == 0))
        carry = dot(closing, s.ctx_value[...], ((0,), (0,)))
        for cols in column_chunks():
            s.carry[direction, :, cols] = after * carry[:, cols]
    first_way = jnp.where(sp < sp_count // 2, 0, 1)

    def ends(way):
        return (jnp.where(way == 0, sp > 0, sp < sp_count - 1),
                jnp.where(way == 0, sp < sp_count - 1, sp > 0))

    def chain_copy(way, kind, c, target):
        return remote(s.chain_out.at[way, kind, c], s.chain_in.at[way, kind, c],
                      s.hs.at[way], s.hr.at[way, kind, c], "sp", target)

    def chain_part(c):
        part, col = c % (keys // part_keys), c // (keys // part_keys)
        return (slice(part * part_keys, (part + 1) * part_keys),
                slice(col * chunk_width, (col + 1) * chunk_width))

    def chain_send(way, kind, c):
        rows, cols = chain_part(c)
        held = s.chain_in[way, kind, c].astype(f32)
        if kind == 0:
            added = held + s.carry[1 - way, rows, cols]
        else:
            added = s.own_decay[way, rows, :] * held + s.state[way, rows, cols]
        s.chain_out[way, kind, c] = added.astype(bf16)
        chain_copy(way, kind, c, sp + 1 - 2 * way).start()

    def chain_open(way, kind):
        has_before, has_next = ends(way)

        @pl.when(jnp.logical_and(has_next, jnp.logical_not(has_before)))
        def _():
            if kind == 1:
                for cols in column_chunks():
                    s.state[way, :, cols] += s.own_decay[way] * s.carry[way, :, cols]
            for c in range(turns_each):
                chain_send(way, kind, c)

    def chain(way, i):
        kind, c = i // turns_each, i % turns_each
        has_before, has_next = ends(way)

        @pl.when(has_before)
        def _():
            chain_copy(way, kind, c, sp - 1 + 2 * way).wait_recv()

            @pl.when(has_next)
            def _():
                chain_send(way, kind, c)

    chain_open(first_way, 0)
    for b in range(blocks):
        rows = slice(b * size, (b + 1) * size)
        key = dot(s.mod_latent[rows, :], s.wqk[0]).astype(bf16)
        s.key[rows, :] = rotate(key.astype(f32), s.cosine[rows, :], s.sine[rows, :])
    for direction in range(2):
        edge = 0 if direction == 1 else size - 1
        state = None
        for turn in range(blocks):
            b = blocks - 1 - turn if direction == 1 else turn
            rows = slice(b * size, (b + 1) * size)
            cum = s.cum[direction, rows, :]
            block_total = cum[edge:edge + 1, :]
            closing = (s.key[rows, :] * jnp.exp(block_total - cum)).astype(bf16)
            term = dot(closing, s.value[rows, :], ((0,), (0,)))
            if state is None:
                state = term
            else:
                s.start[direction, b] = state.astype(bf16)
                state = jnp.exp(block_total).T * state + term
        s.state[direction] = state
    for direction in range(2):
        s.own_decay[direction] = column(s.total[direction:direction + 1, :])
    chain_open(first_way, 1)
    relay_x(0)
    tot_arrive()
    for direction in range(2):
        s.ahead_decay[direction] = column(sum_of(s.totals, direction, direction == 1))

        @pl.when(ends(direction)[0])
        def _():
            both = s.own_decay[direction] * s.ahead_decay[direction]
            for cols in column_chunks():
                s.state[direction, :, cols] += both * s.carry[direction, :, cols]

    def attend(b):
        rows = slice(b * size, (b + 1) * size)
        query = dot(s.mod_latent[rows, :], s.wqk[1]).astype(bf16)
        rq = rotate(query.astype(f32) * keys ** -0.5, s.cosine[rows, :], s.sine[rows, :])
        rk = s.key[rows, :]
        scores, out = None, None
        for direction in range(2):
            keep = triangle(size, direction == 1)
            middle = size // 2 if direction == 1 else size // 2 - 1
            cum = s.cum[direction, rows, :]
            center = cum[middle:middle + 1, :]
            q_mid = (rq * jnp.exp(cum - center)).astype(bf16)
            k_mid = (rk * jnp.exp(center - cum)).astype(bf16)
            score = jnp.where(keep, dot(q_mid, k_mid, ((1,), (1,))), 0.0)
            scores = score if scores is None else scores + score
            q_dec = rq * jnp.exp(cum)
            q_all = q_dec
            if b != (blocks - 1 if direction == 1 else 0):
                carried = dot(q_dec.astype(bf16), s.start[direction, b])
                out = carried if out is None else out + carried
                q_all = q_dec * jnp.exp(s.ahead[direction, b:b + 1, :])
            s.q_all[rows, direction * keys:(direction + 1) * keys] = q_all.astype(bf16)
        inner = dot(scores.astype(bf16), s.value[rows, :])
        s.mixture[rows, :] = inner if out is None else out + inner

    lag, early_turns = 4, 8

    def chain_turn(turn):
        if turn < steps:
            chain(first_way, turn)
        if lag <= turn < steps + lag:
            chain(1 - first_way, turn - lag)

    for turn in range(lag):
        chain_turn(turn)
    for hop in range(2, sp_count - 1):
        for chunk in query_chunks:
            z_arrive(hop, chunk)
    for k in range(1, 3):
        relay_x(k)
    gate_chip(1 - x)
    for turn in range(lag, early_turns):
        chain_turn(turn)
    y_arrive(1)
    for turn in range(max(2 * blocks, steps + lag - early_turns)):
        if turn % 2 == 0 and turn < 2 * blocks:
            attend(turn // 2)
        chain_turn(early_turns + turn)
        if turn % 2 == 0 and 3 + turn // 2 < shared:
            relay_x(3 + turn // 2)
    for c in range(turns_each):
        rows, cols = chain_part(c)
        for direction in range(2):
            joined = (s.chain_in[direction, 1, c].astype(f32)
                      + s.ahead_decay[direction, rows, :]
                      * (s.carry[direction, rows, cols]
                         + s.chain_in[1 - direction, 0, c].astype(f32)))
            start = direction * keys + rows.start
            s.joined[start:start + part_keys, cols] = joined.astype(bf16)
    for load in (load_norm_gain, load_final_gain, load_final_bias):
        load.wait()

    def gate_rows(j):
        rows = block_rows(j)
        mixture = s.mixture[rows, :] + dot(s.q_all[rows, :], s.joined[...])
        squares = jnp.mean(mixture * mixture, axis=1, keepdims=True)
        gate = s.gate[rows, :].astype(f32)
        normed = mixture * lax.rsqrt(squares + norm_eps) * s.norm_gain[...]
        s.gated[rows, :] = (normed * (gate / (1.0 + jnp.exp(-gate)))).astype(bf16)

    def gated_copy(k, j):
        return remote(s.gated.at[block_rows(j), :], s.gathered.at[tp], s.gs.at[k], s.gr.at[k],
                      "tp", j)

    def gated_arrive(k, j):
        remote(s.gathered.at[j], s.gathered.at[j], s.gs.at[k], s.gr.at[k], "tp", j).wait_recv()

    out_chunks = 4
    out_width = width // out_chunks
    out_cols = [slice(n * out_width, (n + 1) * out_width) for n in range(out_chunks)]

    for k, j in ((1, across), (2, far_sibling), (0, sibling)):
        gate_rows(j)
        gated_copy(k, j).start()
    gate_rows(tp)
    for k in range(max(3, shared), out_pieces + direct):
        relay_x(k)
    for p in range(shared):
        relay_y(p)
    out_own_copy(sibling).wait_recv()
    for cols in out_cols:
        s.branch[:, cols] = dot(s.gated[block_rows(tp), :], s.out_w[tp, :, cols])
    gated_arrive(0, sibling)
    for cols in out_cols:
        s.branch[:, cols] += dot(s.gathered[sibling], s.out_w[sibling, :, cols])
    out_pass(out_bytes(out_pieces + direct), 0).wait_recv()
    out_pass(out_bytes(shared), 1).wait_recv()
    gated_arrive(1, across)
    for cols in out_cols:
        s.branch[:, cols] += dot(s.gathered[across], s.out_w[across, :, cols])
    gated_arrive(2, far_sibling)
    for cols in out_cols:
        branch = s.branch[:, cols] + dot(s.gathered[far_sibling], s.out_w[far_sibling, :, cols])
        s.branch[:, cols] = (residual_scale * s.rows[block_rows(tp), cols].astype(f32)
                             + s.branch_gate[:, cols] * branch)
    summed = s.branch[...]
    centered = summed - jnp.mean(summed, axis=1, keepdims=True)
    variance = jnp.mean(centered * centered, axis=1, keepdims=True)
    out_ref[...] = (centered * lax.rsqrt(variance + norm_eps) * s.final_gain[...]
                    + s.final_bias[...]).astype(bf16)

    part_drain()
    sums_drain()
    tot_drain()
    ctx_drain()
    line.drain_whole(s.wqk.at[0, pl.ds(0, depth), :])
    y_drain()
    own_rows = s.rows.at[block_rows(tp), :]
    remote(own_rows, own_rows, s.xs.at[0], s.xr.at[0], "tp", across).wait_send()
    for slot in range(2):
        cross_whole(tp, slot).wait_send()
    for way in range(2):
        has_next = sp < sp_count - 1 if way == 0 else sp > 0

        @pl.when(has_next)
        def _():
            remote(s.chain_out.at[way], s.chain_in.at[way], s.hs.at[way], s.hr.at[way, 0, 0],
                   "sp", sp + 1 - 2 * way).wait_send()
    out_own_copy().wait_send()
    ref = out_bytes(out_pieces + direct)
    remote(ref, ref, s.oxs.at[0], s.oxr.at[0], "tp", across).wait_send()
    out_pass(ref, 0).wait_send()
    ref = out_bytes(shared)
    remote(ref, ref, s.oys.at[0], s.oyr.at[0], "grp", 1 - grp).wait_send()
    out_pass(ref, 1).wait_send()
    for k, j in enumerate((sibling, across, far_sibling)):
        gated_copy(k, j).wait_send()


def fused(latent, context, condition, context_condition, mod_weight, mod_bias, query_weight,
          key_weight, value_weight, out_gate_weight, decay_in_weight, decay_weight, decay_bias,
          extra_decay, norm_gain, out_weight, final_gain, final_bias):
    sp_count, tp_count = lax.axis_size("sp"), lax.axis_size("tp")
    own, width = latent.shape
    depth = query_weight.shape[0]
    keys = query_weight.shape[1] // ATTENTION_HEADS
    vals = value_weight.shape[1]
    ctx = context.shape[0]
    count = own * tp_count
    blocks = count // (2 * BLOCK)
    mod_cols = mod_weight.shape[1]
    chains, outs, pieces = 4, 8, 8
    args = (latent, context, condition[None, :], context_condition[None, :], mod_weight,
            mod_bias[None, :], query_weight, key_weight, value_weight, out_gate_weight,
            decay_in_weight.T, decay_weight, decay_bias, extra_decay, norm_gain[None, :],
            out_weight, final_gain[None, :], final_bias[None, :])
    dma, vmem = pltpu.SemaphoreType.DMA, pltpu.VMEM
    hops = sp_count - 1
    scratch = Scratch(
        cond=vmem((1, condition.shape[0]), f32),
        ctx_cond=vmem((1, condition.shape[0]), f32),
        mod_w=vmem(mod_weight.shape, bf16),
        mod_b=vmem((1, mod_bias.shape[0]), f32),
        wqk=vmem((2, depth * sp_count, keys), bf16),
        rows=vmem((count, width), bf16),
        mod_latent=vmem((count, width), bf16),
        context=vmem(context.shape, bf16),
        mod_context=vmem(context.shape, bf16),
        low_w=vmem(decay_in_weight.shape[::-1], bf16),
        value_w=vmem(value_weight.shape, bf16),
        gate_w=vmem(out_gate_weight.shape, bf16),
        out_w=vmem((tp_count,) + out_weight.shape, bf16),
        decay_w=vmem(decay_weight.shape[:2] + (keys,), bf16),
        decay_b=vmem((2, keys), f32),
        extra=vmem(extra_decay.shape, f32),
        norm_gain=vmem((1, vals), f32),
        final_gain=vmem((1, width), f32),
        final_bias=vmem((1, width), f32),
        part=vmem((sp_count, 2, mod_cols), f32),
        sums=vmem((tp_count, 2, mod_cols), f32),
        totals=vmem((sp_count, 2, keys), f32),
        ctx_totals=vmem((sp_count, 2, keys), f32),
        shifts=vmem((2, width), f32),
        scales=vmem((2, width), f32),
        branch_gate=vmem((1, width), f32),
        cosine=vmem((count, keys), f32),
        sine=vmem((count, keys), f32),
        ctx_close=vmem((2, ctx, keys), f32),
        ctx_value=vmem((ctx, vals), bf16),
        low=vmem((count, decay_in_weight.shape[1]), bf16),
        value=vmem((count, vals), bf16),
        gate=vmem((count, vals), bf16),
        key=vmem((count, keys), f32),
        cum=vmem((2, count, keys), f32),
        ahead=vmem((2, blocks, keys), f32),
        block_total=vmem((2, blocks, 1, keys), f32),
        total=vmem((2, keys), f32),
        start=vmem((2, blocks, keys, vals), bf16),
        state=vmem((2, keys, vals), f32),
        carry=vmem((2, keys, vals), f32),
        own_decay=vmem((2, keys, vals // chains), f32),
        ahead_decay=vmem((2, keys, vals // chains), f32),
        chain_in=vmem((2, 2, 2 * chains, keys // 2, vals // chains), bf16),
        chain_out=vmem((2, 2, 2 * chains, keys // 2, vals // chains), bf16),
        q_all=vmem((count, 2 * keys), bf16),
        mixture=vmem((count, vals), f32),
        joined=vmem((2 * keys, vals), bf16),
        gated=vmem((count, vals), bf16),
        gathered=vmem((tp_count, own, vals), bf16),
        branch=vmem((own, width), f32),
        load_sem=dma((len(args),)),
        zs=dma((2, hops)), zr=dma((2, hops, 2 * PARTS)),
        ys=dma((2, hops)), yr=dma((2, hops, 2)),
        xs=dma((1,)), xr=dma((pieces,)), cs=dma((2,)), cr=dma((2,)),
        ocs=dma((1,)), ocr=dma((1,)), ods=dma((2,)), odr=dma((2,)),
        oxs=dma((1,)), oxr=dma((outs + outs // 4,)), oys=dma((1,)), oyr=dma((outs,)),
        gs=dma((tp_count - 1,)), gr=dma((tp_count - 1,)),
        ps=dma((hops,)), pr=dma((hops,)), ts=dma((hops,)), tr=dma((hops,)),
        us=dma((hops,)), ur=dma((hops,)),
        ss=dma((tp_count - 1,)), sr=dma((tp_count - 1,)),
        hs=dma((2,)), hr=dma((2, 2, 2 * chains)),
    )
    return pl.pallas_call(
        fused_kernel,
        out_shape=jax.ShapeDtypeStruct((own, width), bf16),
        in_specs=[pl.BlockSpec(memory_space=pltpu.HBM)] * len(args),
        out_specs=pl.BlockSpec(memory_space=pltpu.VMEM),
        scratch_shapes=[scratch],
        compiler_params=pltpu.CompilerParams(
            vmem_limit_bytes=60 * 1024 * 1024, collective_id=2, has_side_effects=True),
        cost_estimate=pl.CostEstimate(flops=6_000_000_000, bytes_accessed=12_000_000,
                                      transcendentals=2_000_000),
    )(*args)


def whole_heads(mesh):
    return mesh.shape["tp"] == ATTENTION_HEADS and mesh.shape["grp"] == 2


def solution(mesh):
    placed = (
        P(("grp", "sp", "tp"), None),
        P(("grp", "sp"), None),
        P(("grp", "sp")),
        P("sp"),
        P("sp", "tp"),
        P(),
        P("sp", None),
        P("sp", None),
        P(None, "tp"),
        P(None, "tp"),
        P(),
        P(),
        P(),
        P(None, None, "sp"),
        P(),
        P("tp", None),
        P(),
        P(),
    )
    return jax.shard_map(
        fused if whole_heads(mesh) else body, mesh=mesh, in_specs=placed, out_specs=P(("grp", "sp", "tp"), None), check_vma=False
    )
```

```python
import functools
from typing import Any, NamedTuple

import jax
import jax.numpy as jnp
from jax import lax
from jax.experimental import pallas as pl
from jax.experimental.pallas import tpu as pltpu
from jax.sharding import PartitionSpec as P

ATTENTION_HEADS = 4
DV = 512
BLOCK = 64
GRID_W = 64


norm_eps = 1e-05
gate_scale = 16.0
rope_base = 10000.0
residual_scale = 2.0**0.5
highest = lax.Precision.HIGHEST
f32 = jnp.float32
bf16 = jnp.bfloat16


def rope_tables(token_places, width):
    quarter = width // 4
    frequency = rope_base ** (-jnp.arange(quarter, dtype=f32) / quarter)
    row_angle = (token_places // GRID_W).astype(f32)[:, None] * frequency
    col_angle = (token_places % GRID_W).astype(f32)[:, None] * frequency
    cosine = jnp.concatenate([jnp.cos(row_angle)] * 2 + [jnp.cos(col_angle)] * 2, axis=1)
    row_sine, col_sine = jnp.sin(row_angle), jnp.sin(col_angle)
    sine = jnp.concatenate([-row_sine, row_sine, -col_sine, col_sine], axis=1)
    return cosine, sine


def dot(a, b, contract=((1,), (0,)), precision=None):
    return lax.dot_general(a, b, (contract, ((), ())), precision=precision,
                           preferred_element_type=f32)


def log_sigmoid(x):
    return jnp.minimum(x, 0.0) - jnp.log1p(jnp.exp(-jnp.abs(x)))


def rotate(x, cosine, sine):
    half = x.shape[1] // 2
    parts = [pltpu.roll(x[:, i * half:(i + 1) * half], half // 2, 1) for i in range(2)]
    return x * cosine + jnp.concatenate(parts, axis=1) * sine


def triangle(size, reverse):
    row = lax.broadcasted_iota(jnp.int32, (size, size), 0)
    col = lax.broadcasted_iota(jnp.int32, (size, size), 1)
    return row <= col if reverse else row >= col


def decay_block(low, decay_weight, decay_bias, direction):
    rank = decay_weight.shape[1]
    logits = dot(low[:, direction * rank:(direction + 1) * rank], decay_weight[direction])
    return log_sigmoid(logits + decay_bias[direction:direction + 1, :]) / gate_scale


def context_kernel(k_ref, v_ref, low_ref, dw_ref, db_ref, state_ref):
    length, width = k_ref.shape
    size = min(2 * BLOCK, length)
    count = length // size
    for direction in range(2):
        mask = triangle(size, direction == 1).astype(f32)
        edge = 0 if direction == 1 else size - 1
        state = None
        for step in range(count):
            b = count - 1 - step if direction == 1 else step
            rows = slice(b * size, (b + 1) * size)
            logdec = decay_block(low_ref[rows, :], dw_ref[...], db_ref[...], direction)
            cum = dot(mask, logdec, precision=highest)
            total = cum[edge:edge + 1, :]
            closing = (k_ref[rows, :].astype(f32) * jnp.exp(total - cum)).astype(bf16)
            term = dot(closing, v_ref[rows, :], ((0,), (0,)))
            state = term if state is None else jnp.exp(total).T * state + term
        state_ref[direction] = state


def local_kernel(q_ref, k_ref, v_ref, low_ref, extra_ref, dw_ref, db_ref, cos_ref, sin_ref,
                 out_ref, qc_ref, state_ref, total_ref):
    length, width = q_ref.shape
    size = 2 * BLOCK
    count = length // size
    rq, rk, within, scores = [], [], [], []
    for b in range(count):
        rows = slice(b * size, (b + 1) * size)
        cosine, sine = cos_ref[rows, :], sin_ref[rows, :]
        rq.append(rotate(q_ref[rows, :].astype(f32) * width ** -0.5, cosine, sine))
        rk.append(rotate(k_ref[rows, :].astype(f32), cosine, sine))
        scores.append(None)
    for direction in range(2):
        keep = triangle(size, direction == 1)
        mask = keep.astype(f32)
        edge = 0 if direction == 1 else size - 1
        middle = size // 2 if direction == 1 else size // 2 - 1
        state = None
        before = None
        for step in range(count):
            b = count - 1 - step if direction == 1 else step
            rows = slice(b * size, (b + 1) * size)
            logdec = decay_block(low_ref[rows, :], dw_ref[...], db_ref[...], direction)
            logdec = logdec + extra_ref[rows, direction:direction + 1]
            cum = dot(mask, logdec, precision=highest)
            total = cum[edge:edge + 1, :]
            center = cum[middle:middle + 1, :]
            q_mid = (rq[b] * jnp.exp(cum - center)).astype(bf16)
            k_mid = (rk[b] * jnp.exp(center - cum)).astype(bf16)
            score = jnp.where(keep, dot(q_mid, k_mid, ((1,), (1,))), 0.0)
            q_dec = rq[b] * jnp.exp(cum)
            if direction == 0:
                scores[b] = score
                out = None
            else:
                out = dot((scores[b] + score).astype(bf16), v_ref[rows, :])
            if state is not None:
                carried = dot(q_dec.astype(bf16), state.astype(bf16))
                out = carried if out is None else out + carried
            if direction == 0:
                out_ref[rows, :] = jnp.zeros((size, v_ref.shape[1]), f32) if out is None else out
            else:
                out_ref[rows, :] += out
            q_all = q_dec if before is None else q_dec * jnp.exp(before)
            qc_ref[rows, direction * width:(direction + 1) * width] = q_all.astype(bf16)
            closing = (rk[b] * jnp.exp(total - cum)).astype(bf16)
            term = dot(closing, v_ref[rows, :], ((0,), (0,)))
            state = term if state is None else jnp.exp(total).T * state + term
            before = total if before is None else before + total
        state_ref[direction * width:(direction + 1) * width, :] = state.astype(bf16)
        total_ref[direction:direction + 1, :] = before


def join_kernel(final, out_ref, qc_ref, states_ref, totals_ref, start_ref, gate_ref, gain_ref,
                place_ref, result_ref):
    count = states_ref.shape[0]
    width = qc_ref.shape[1] // 2
    place = place_ref[...]
    mixture = out_ref[...]
    for direction in range(2):
        state = start_ref[direction]
        for lap in range(count):
            j = count - 1 - lap if direction == 1 else lap
            decay = jnp.exp(totals_ref[j, direction:direction + 1, :]).T
            joined = decay * state + states_ref[
                j, direction * width:(direction + 1) * width, :].astype(f32)
            ahead = place < j if direction == 1 else place > j
            state = jnp.where(ahead, joined, state)
        mixture = mixture + dot(qc_ref[:, direction * width:(direction + 1) * width],
                                state.astype(bf16))
    if final:
        squares = jnp.mean(mixture * mixture, axis=1, keepdims=True)
        gate = gate_ref[...].astype(f32)
        normed = mixture * lax.rsqrt(squares + norm_eps) * gain_ref[...]
        result_ref[...] = (normed * (gate / (1.0 + jnp.exp(-gate)))).astype(bf16)
    else:
        result_ref[...] = mixture


def call(kernel, out_shape, *args):
    return pl.pallas_call(
        kernel,
        out_shape=out_shape,
        in_specs=[pl.BlockSpec(memory_space=pltpu.VMEM)] * len(args),
        out_specs=jax.tree.map(lambda _: pl.BlockSpec(memory_space=pltpu.VMEM), out_shape),
        compiler_params=pltpu.CompilerParams(vmem_limit_bytes=48 * 1024 * 1024),
        cost_estimate=pl.CostEstimate(flops=4_000_000_000, bytes_accessed=4_000_000,
                                      transcendentals=1_000_000),
    )(*args)


MESH = pl.DeviceIdType.MESH


def remote(src, dst, send_sem, recv_sem, axis, target):
    return pltpu.make_async_remote_copy(
        src_ref=src, dst_ref=dst, send_sem=send_sem, recv_sem=recv_sem,
        device_id={axis: target}, device_id_type=MESH)


class Line:
    def __init__(self, place, count, axis, target_of, view, chunks, send_sem, recv_sem):
        self.place, self.count, self.axis, self.target_of = place, count, axis, target_of
        self.view, self.chunks, self.send_sem, self.recv_sem = view, chunks, send_sem, recv_sem

    def copy(self, way, hop, chunk, block, target):
        ref = self.view(block, chunk)
        return remote(ref, ref, self.send_sem.at[way, hop, chunk],
                      self.recv_sem.at[way, hop, chunk], self.axis, self.target_of(target))

    def outgoing(self, way, hop):
        place, count = self.place, self.count
        if way == 0:
            return place - hop, place + 1, jnp.logical_and(place >= hop, place < count - 1)
        return place + hop, place - 1, jnp.logical_and(place + hop < count, place > 0)

    def each_send(self, way, hop, chunk, act):
        block, target, valid = self.outgoing(way, hop)

        @pl.when(valid)
        def _():
            act(self.copy(way, hop, chunk, block, target))

    def send(self, way, hop, chunk):
        self.each_send(way, hop, chunk, lambda c: c.start())

    def drain(self):
        for way in range(2):
            for hop in range(self.count - 1):
                for chunk in range(self.chunks):
                    self.each_send(way, hop, chunk, lambda c: c.wait_send())

    def arrive(self, way, hop, chunk, then=None):
        if way == 0:
            block, source, valid = self.place - 1 - hop, self.place - 1, self.place > hop
        else:
            block, source = self.place + 1 + hop, self.place + 1
            valid = self.place + 1 + hop < self.count

        @pl.when(valid)
        def _():
            self.copy(way, hop, chunk, block, source).wait_recv()
            if then is not None:
                then(block)

    def forward(self, hop, then=None):
        for chunk in range(self.chunks):
            for way in range(2):
                self.arrive(way, hop, chunk, None if then is None else functools.partial(then, way))
                if hop + 1 < self.count - 1:
                    self.send(way, hop + 1, chunk)


def open_kernel(partners):
    barrier = pltpu.get_barrier_semaphore()
    for axis, target in partners:
        pl.semaphore_signal(barrier, inc=1, device_id={axis: target}, device_id_type=MESH)
    return lambda: pl.semaphore_wait(barrier, len(partners))


def others(axis):
    count, place = lax.axis_size(axis), lax.axis_index(axis)
    return [lax.rem(place + k, count) for k in range(1, count)]


def sources(axis):
    count, place = lax.axis_size(axis), lax.axis_index(axis)
    return [lax.rem(place + count - k, count) for k in range(1, count)]


def spread(buffer, axis, send_sem, recv_sem):
    place = lax.axis_index(axis)
    for k, target in enumerate(others(axis)):
        remote(buffer.at[place], buffer.at[place], send_sem.at[k], recv_sem.at[k],
               axis, target).start()


def spread_arrive(buffer, axis, send_sem, recv_sem):
    for k, source in enumerate(sources(axis)):
        remote(buffer.at[source], buffer.at[source], send_sem.at[k], recv_sem.at[k],
               axis, source).wait_recv()


def spread_drain(buffer, axis, send_sem, recv_sem):
    place = lax.axis_index(axis)
    for k, target in enumerate(others(axis)):
        remote(buffer.at[place], buffer.at[place], send_sem.at[k], recv_sem.at[k],
               axis, target).wait_send()


def enter_kernel(chunks, latent_ref, context_ref, cond_ref, mw_ref, mb_ref, qw_ref, kw_ref,
                 ml_ref, mc_ref, gate_ref, qk_ref,
                 rows_ref, part_ref, sums_ref, zs, zr, xs, xr, cs, cr, ps, pr, ss, sr):
    sp, sp_count = lax.axis_index("sp"), lax.axis_size("sp")
    tp, tp_count = lax.axis_index("tp"), lax.axis_size("tp")
    own, model_width = latent_ref.shape
    depth = qw_ref.shape[0]
    head_keys = qk_ref.shape[1] // 2
    ready = open_kernel([("sp", t) for t in others("sp")] + [("tp", t) for t in others("tp")])
    v = cond_ref[...]
    activated = (v / (1.0 + jnp.exp(-v))).astype(bf16)
    part_ref[sp] = dot(activated, mw_ref[...])
    columns = pl.ds(pl.multiple_of((tp // (tp_count // ATTENTION_HEADS)) * head_keys, head_keys),
                    head_keys)
    qk_rows = pl.ds(pl.multiple_of(sp * depth, depth), depth)
    qk_ref[qk_rows, :head_keys] = qw_ref[:, columns]
    qk_ref[qk_rows, head_keys:] = kw_ref[:, columns]
    rows_ref[pl.ds(pl.multiple_of(tp * own, own), own), :] = latent_ref[...]

    step = depth // chunks
    z_line = Line(
        sp, sp_count, "sp", lambda p: p,
        lambda block, chunk: qk_ref.at[
            pl.ds(pl.multiple_of(block * depth + chunk * step, step), step), :],
        chunks, zs, zr)
    x_count = tp_count // 2
    x, core = tp // 2, tp % 2

    def rows_of(block, chunk):
        return rows_ref.at[pl.ds(pl.multiple_of((2 * block + core) * own, own), own), :]

    x_line = Line(x, x_count, "tp", lambda p: 2 * p + core, rows_of, 1, xs, xr)
    sibling = tp + 1 - 2 * core

    def cross(block, slot, other=False):
        side = 1 - core if other else core
        ref = rows_ref.at[pl.ds(pl.multiple_of((2 * block + side) * own, own), own), :]
        return remote(ref, ref, cs.at[slot], cr.at[slot], "tp", sibling)

    def slot_of(way, hop):
        return 1 + way * (x_count - 1) + hop

    ready()
    spread(part_ref, "sp", ps, pr)
    for way in range(2):
        x_line.send(way, 0, 0)
    cross(x, 0).start()
    for chunk in range(chunks):
        for way in range(2):
            z_line.send(way, 0, chunk)
    spread_arrive(part_ref, "sp", ps, pr)
    total = part_ref[0]
    for j in range(1, sp_count):
        total = total + part_ref[j]
    sums_ref[tp] = total
    spread(sums_ref, "tp", ss, sr)
    z_line.forward(0)
    for hop in range(x_count - 1):
        x_line.forward(hop, lambda way, block, hop=hop: cross(block, slot_of(way, hop)).start())
    if sp_count > 2:
        z_line.forward(1)
    spread_arrive(sums_ref, "tp", ss, sr)
    modulation = jnp.concatenate([sums_ref[j] for j in range(tp_count)], axis=1) + mb_ref[...]
    shifts = modulation[:, :model_width]
    scales = modulation[:, model_width:2 * model_width]
    gate_ref[...] = modulation[0:1, 2 * model_width:]
    mc_ref[...] = (context_ref[...].astype(f32) * (1.0 + scales[1:2]) + shifts[1:2]).astype(bf16)

    def each_cross(act_own, act_line):
        act_own()
        for way in range(2):
            for hop in range(x_count - 1):
                block = x - 1 - hop if way == 0 else x + 1 + hop
                valid = x > hop if way == 0 else x + 1 + hop < x_count

                @pl.when(valid)
                def _():
                    act_line(block, slot_of(way, hop))

    each_cross(lambda: cross(x, 0, True).wait_recv(),
               lambda block, slot: cross(block, slot, True).wait_recv())
    for j in range(tp_count):
        rows = slice(j * own, (j + 1) * own)
        ml_ref[rows, :] = (rows_ref[rows, :].astype(f32) * (1.0 + scales[0:1])
                           + shifts[0:1]).astype(bf16)
    for hop in range(2, sp_count - 1):
        z_line.forward(hop)
    each_cross(lambda: cross(x, 0).wait_send(),
               lambda block, slot: cross(block, slot).wait_send())
    spread_drain(part_ref, "sp", ps, pr)
    spread_drain(sums_ref, "tp", ss, sr)
    x_line.drain()
    z_line.drain()


def comm_call(kernel, out_shape, scratch, collective_id, *args):
    return pl.pallas_call(
        kernel,
        out_shape=out_shape,
        in_specs=[pl.BlockSpec(memory_space=pltpu.VMEM)] * len(args),
        out_specs=jax.tree.map(lambda _: pl.BlockSpec(memory_space=pltpu.VMEM), out_shape),
        scratch_shapes=scratch,
        compiler_params=pltpu.CompilerParams(
            vmem_limit_bytes=48 * 1024 * 1024, collective_id=collective_id,
            has_side_effects=True),
        cost_estimate=pl.CostEstimate(flops=20_000_000_000, bytes_accessed=60_000_000,
                                      transcendentals=1_000_000),
    )(*args)


def enter(latent, context, cond, mod_weight, mod_bias, query_weight, key_weight):
    sp_count, tp_count = lax.axis_size("sp"), lax.axis_size("tp")
    own, model_width = latent.shape
    depth = query_weight.shape[0]
    head_keys = query_weight.shape[1] // ATTENTION_HEADS
    chunks = 4
    sds = jax.ShapeDtypeStruct
    dma = pltpu.SemaphoreType.DMA
    x_hops = tp_count // 2 - 1
    return comm_call(
        functools.partial(enter_kernel, chunks),
        (
            sds((own * tp_count, model_width), bf16),
            sds(context.shape, bf16),
            sds((1, model_width), f32),
            sds((depth * sp_count, 2 * head_keys), bf16),
        ),
        [
            pltpu.VMEM((own * tp_count, model_width), bf16),
            pltpu.VMEM((sp_count, 2, mod_weight.shape[1]), f32),
            pltpu.VMEM((tp_count, 2, mod_weight.shape[1]), f32),
            dma((2, sp_count - 1, chunks)), dma((2, sp_count - 1, chunks)),
            dma((2, x_hops, 1)), dma((2, x_hops, 1)),
            dma((1 + 2 * x_hops,)), dma((1 + 2 * x_hops,)),
            dma((sp_count - 1,)), dma((sp_count - 1,)),
            dma((tp_count - 1,)), dma((tp_count - 1,)),
        ],
        1, latent, context, cond, mod_weight, mod_bias[None, :], query_weight, key_weight,
    )


def project(rows, weight):
    return jnp.dot(rows, weight, preferred_element_type=f32).astype(bf16)


def body(
    latent,
    context,
    condition,
    context_condition,
    mod_weight,
    mod_bias,
    query_weight,
    key_weight,
    value_weight,
    out_gate_weight,
    decay_in_weight,
    decay_weight,
    decay_bias,
    extra_decay,
    norm_gain,
    out_weight,
    final_gain,
    final_bias,
):
    head_keys = query_weight.shape[1] // ATTENTION_HEADS
    value_cols = value_weight.shape[1]
    tp_index = lax.axis_index("tp")
    sp_index = lax.axis_index("sp")
    head_share = lax.axis_size("tp") // ATTENTION_HEADS
    head_index = tp_index // head_share
    part_index = tp_index % head_share
    key_start = head_index * head_keys

    full_out = lax.all_gather(out_weight, "tp", axis=0, tiled=True)
    mod_latent, mod_context, branch_gate, qk_head = enter(
        latent, context, jnp.stack([condition, context_condition]), mod_weight, mod_bias,
        query_weight, key_weight,
    )
    context_local = jnp.concatenate(
        [
            project(mod_context, qk_head[:, head_keys:]),
            project(mod_context, value_weight),
            project(mod_context, decay_in_weight),
        ],
        axis=1,
    )
    gathered_context = lax.all_gather(context_local, "sp", axis=0, tiled=True)
    qk = project(mod_latent, qk_head)
    value_rows = project(mod_latent, value_weight)
    out_gate = project(mod_latent, out_gate_weight)
    low_rank = project(mod_latent, decay_in_weight)
    count = mod_latent.shape[0]
    token_places = sp_index * count + jnp.arange(count, dtype=jnp.int32)
    cosine, sine = rope_tables(token_places, head_keys)
    head_bias = lax.dynamic_slice_in_dim(decay_bias, key_start, head_keys, 1)
    head_gate = lax.dynamic_slice_in_dim(decay_weight, key_start, head_keys, 2)
    head_extra = lax.dynamic_index_in_dim(extra_decay, head_index, 1, keepdims=False).T

    sds = jax.ShapeDtypeStruct
    out_local, qc, states, totals = call(
        local_kernel,
        (
            sds((count, value_cols), f32),
            sds((count, 2 * head_keys), bf16),
            sds((2 * head_keys, value_cols), bf16),
            sds((2, head_keys), f32),
        ),
        qk[:, :head_keys], qk[:, head_keys:], value_rows, low_rank, head_extra, head_gate,
        head_bias, cosine, sine,
    )
    start = call(
        context_kernel,
        sds((2, head_keys, value_cols), f32),
        gathered_context[:, :head_keys],
        gathered_context[:, head_keys : head_keys + value_cols],
        gathered_context[:, head_keys + value_cols :],
        head_gate, head_bias,
    )
    states, totals, full_out = lax.optimization_barrier((states, totals, full_out))
    all_states = lax.all_gather(states, "sp")
    all_totals = lax.all_gather(totals, "sp")
    place = jnp.full((1, value_cols), sp_index, jnp.int32)
    gain_slice = lax.dynamic_slice_in_dim(norm_gain, part_index * value_cols, value_cols, 0)
    final = head_share == 1
    joined = call(
        functools.partial(join_kernel, final),
        sds((count, value_cols), bf16 if final else f32),
        out_local, qc, all_states, all_totals, start, out_gate, gain_slice[None, :], place,
    )
    if final:
        gated_rows = joined
    else:
        squares = jnp.sum(joined * joined, axis=1)
        onehot = (jnp.arange(ATTENTION_HEADS) == head_index).astype(f32)
        sums = lax.psum(onehot[:, None] * squares[None, :], "tp")
        head_sum = jnp.sum(sums * onehot[:, None], axis=0)
        normed = joined * lax.rsqrt(head_sum / DV + norm_eps)[:, None] * gain_slice
        gated_rows = (normed * jax.nn.silu(out_gate.astype(f32))).astype(bf16)
    regrouped = lax.all_to_all(gated_rows, "tp", split_axis=0, concat_axis=1, tiled=True)
    branch = jnp.dot(regrouped, full_out, preferred_element_type=f32)
    summed = residual_scale * latent.astype(f32) + branch_gate * branch
    row_mean = jnp.mean(summed, axis=1, keepdims=True)
    centered = summed - row_mean
    variance = jnp.mean(centered * centered, axis=1, keepdims=True)
    return (centered * lax.rsqrt(variance + norm_eps) * final_gain + final_bias).astype(bf16)


class Scratch(NamedTuple):
    cond: Any
    ctx_cond: Any
    mod_w: Any
    mod_b: Any
    wqk: Any
    rows: Any
    mod_latent: Any
    context: Any
    mod_context: Any
    low_w: Any
    value_w: Any
    gate_w: Any
    out_w: Any
    decay_w: Any
    decay_b: Any
    extra: Any
    norm_gain: Any
    part: Any
    sums: Any
    totals: Any
    ctx_totals: Any
    shifts: Any
    scales: Any
    branch_gate: Any
    cosine: Any
    sine: Any
    ctx_close: Any
    ctx_value: Any
    low: Any
    value: Any
    gate: Any
    key: Any
    cum: Any
    ahead: Any
    block_total: Any
    total: Any
    start: Any
    state: Any
    carry: Any
    own_decay: Any
    ahead_decay: Any
    chain_in: Any
    chain_out: Any
    q_all: Any
    mixture: Any
    joined: Any
    gated: Any
    gathered: Any
    branch: Any
    load_sem: Any
    zs: Any
    zr: Any
    ys: Any
    yr: Any
    xs: Any
    xr: Any
    cs: Any
    cr: Any
    ocs: Any
    ocr: Any
    ods: Any
    odr: Any
    oxs: Any
    oxr: Any
    oys: Any
    oyr: Any
    gs: Any
    gr: Any
    ps: Any
    pr: Any
    ts: Any
    tr: Any
    us: Any
    ur: Any
    ss: Any
    sr: Any
    hs: Any
    hr: Any


def spread_of(ref, axis, send_sem, recv_sem):
    return (lambda: spread(ref, axis, send_sem, recv_sem),
            lambda: spread_arrive(ref, axis, send_sem, recv_sem),
            lambda: spread_drain(ref, axis, send_sem, recv_sem))


class SharedLine(Line):
    def copy(self, way, hop, chunk, block, target):
        ref = self.view(block, chunk)
        return remote(ref, ref, self.send_sem.at[way, hop], self.recv_sem.at[way, hop, chunk],
                      self.axis, self.target_of(target))

    def drain_whole(self, whole):
        for way in range(2):
            for hop in range(self.count - 1):
                block, target, valid = self.outgoing(way, hop)

                @pl.when(valid)
                def _():
                    remote(whole, whole, self.send_sem.at[way, hop],
                           self.recv_sem.at[way, hop, 0], self.axis,
                           self.target_of(target)).wait_send()


PARTS = 4


def fused_kernel(latent, context, cond, ctx_cond, mod_w, mod_b, query_w, key_w, value_w, gate_w,
                 low_w, decay_w, decay_b, extra, norm_gain, out_w, summed_ref, s):
    grp = lax.axis_index("grp")
    sp, sp_count = lax.axis_index("sp"), lax.axis_size("sp")
    tp, tp_count = lax.axis_index("tp"), lax.axis_size("tp")
    own, width = latent.shape
    depth = query_w.shape[0]
    keys = query_w.shape[1] // ATTENTION_HEADS
    vals = value_w.shape[1]
    count = own * tp_count
    size = 2 * BLOCK
    blocks = count // size
    ctx = context.shape[0]
    x, core = tp // 2, tp % 2
    sibling, across = tp + 1 - 2 * core, 2 * (1 - x) + core
    far_sibling = 2 * (1 - x) + 1 - core

    def block_rows(j):
        return pl.ds(pl.multiple_of(j * own, own), own)

    ready = open_kernel([("sp", t) for t in others("sp")] + [("tp", t) for t in others("tp")]
                        + [("grp", 1 - grp)])
    head_cols = pl.ds(pl.multiple_of(tp * keys, keys), keys)
    own_depth = pl.ds(pl.multiple_of(sp * depth, depth), depth)
    loads = []
    for i, (source, target) in enumerate((
        (latent, s.rows.at[block_rows(tp), :]),
        (cond, s.cond), (ctx_cond, s.ctx_cond), (mod_w, s.mod_w),
        (key_w.at[:, head_cols], s.wqk.at[0, own_depth, :]),
        (query_w.at[:, head_cols], s.wqk.at[1, own_depth, :]),
        (mod_b, s.mod_b), (context, s.context),
        (low_w, s.low_w), (value_w, s.value_w),
        (decay_w.at[:, :, head_cols], s.decay_w),
        (decay_b.at[:, head_cols], s.decay_b), (extra, s.extra),
        (gate_w, s.gate_w), (norm_gain, s.norm_gain),
        (out_w, s.out_w.at[tp]),
    )):
        loads.append(pltpu.make_async_copy(source, target, s.load_sem.at[i]))
        loads[i].start()
    (load_latent, load_cond, load_ctx_cond, load_mod_w, load_key_w, load_query_w,
     load_mod_b, load_context, load_low_w, load_value_w, load_decay_w, load_decay_b,
     load_extra, load_gate_w, load_norm_gain, load_out_w) = loads

    half = depth // 2
    step = half // PARTS

    def weight_view(side):
        def view(block, chunk):
            start = block * depth + side * half + (chunk % PARTS) * step
            return s.wqk.at[chunk // PARTS, pl.ds(pl.multiple_of(start, step), step), :]
        return view

    line = SharedLine(sp, sp_count, "sp", lambda p: p, weight_view(grp), 2 * PARTS, s.zs, s.zr)

    def y_copy(ref, way, hop, matrix):
        return remote(ref, ref, s.ys.at[way, hop], s.yr.at[way, hop, matrix], "grp", 1 - grp)

    def z_arrive(hop, chunk, pass_on=True):
        for way in range(2):
            line.arrive(way, hop, chunk, (lambda block: y_copy(
                weight_view(grp)(block, chunk), way, hop, chunk // PARTS).start()) if pass_on else None)
            if hop + 1 < sp_count - 1:
                line.send(way, hop + 1, chunk)

    def y_each(hop, act):
        for way in range(2):
            block = sp - 1 - hop if way == 0 else sp + 1 + hop
            valid = sp > hop if way == 0 else sp + 1 + hop < sp_count

            @pl.when(valid)
            def _():
                act(block, way)

    def y_start(hop, chunk):
        y_each(hop, lambda block, way: y_copy(
            weight_view(grp)(block, chunk), way, hop, chunk // PARTS).start())

    def y_arrive(matrix):
        def wait(hop, block, way):
            start = pl.multiple_of(block * depth + (1 - grp) * half, half)
            y_copy(s.wqk.at[matrix, pl.ds(start, half), :], way, hop, matrix).wait_recv()

        for hop in range(sp_count - 1):
            y_each(hop, functools.partial(wait, hop))

    def y_drain():
        whole = s.wqk.at[0, pl.ds(0, depth), :]
        for hop in range(sp_count - 1):
            y_each(hop, lambda block, way: y_copy(whole, way, hop, 0).wait_send())

    key_chunks, query_chunks = range(PARTS), range(PARTS, 2 * PARTS)

    def send_own(chunks):
        for chunk in chunks:
            for way in range(2):
                line.send(way, 0, chunk)

    pieces, early = s.xr.shape[0], 3
    piece = own // pieces

    def rows_piece(j, p):
        return s.rows.at[pl.ds(pl.multiple_of(j * own + p * piece, piece), piece), :]

    def x_copy(j, p):
        return remote(rows_piece(j, p), rows_piece(j, p), s.xs.at[0], s.xr.at[p],
                      "tp", across)

    def cross(j, p, slot):
        return remote(rows_piece(j, p), rows_piece(j, p), s.cs.at[slot], s.cr.at[slot],
                      "tp", sibling)

    def cross_whole(j, slot):
        ref = s.rows.at[block_rows(j), :]
        return remote(ref, ref, s.cs.at[slot], s.cr.at[slot], "tp", sibling)

    out_rows = s.out_w.shape[1]
    out_half = out_rows // 2
    out_pieces = s.oyr.shape[0]
    out_step = out_half // out_pieces

    direct = out_pieces // 4
    shared = out_pieces - direct

    def out_piece(j, side, p):
        start = pl.multiple_of(side * out_half + p * out_step, out_step)
        return s.out_w.at[j, pl.ds(start, out_step), :]

    def out_bytes(count):
        return s.out_w.at[tp, pl.ds(0, count * out_step), :]

    def out_own_copy(j=tp):
        return remote(s.out_w.at[j], s.out_w.at[j], s.ocs.at[0], s.ocr.at[0], "tp", sibling)

    def out_x(j, k):
        side, p = (grp, k) if k < out_pieces else (1 - grp, shared + k - out_pieces)
        ref = out_piece(j, side, p)
        return remote(ref, ref, s.oxs.at[0], s.oxr.at[k], "tp", across)

    def out_y(side, p):
        ref = out_piece(across, side, p)
        return remote(ref, ref, s.oys.at[0], s.oyr.at[p], "grp", 1 - grp)

    def out_pass(ref, way):
        return remote(ref, ref, s.ods.at[way], s.odr.at[way], "tp", sibling)

    def relay_x(k):
        copy = out_x(across, k)
        copy.wait_recv()
        if k < shared:
            out_y(grp, k).start()
        side, p = (grp, k) if k < out_pieces else (1 - grp, shared + k - out_pieces)
        out_pass(out_piece(across, side, p), 0).start()

    def relay_y(p):
        out_y(1 - grp, p).wait_recv()
        out_pass(out_piece(across, 1 - grp, p), 1).start()

    part_go, part_arrive, part_drain = spread_of(s.part, "sp", s.ps, s.pr)
    sums_go, sums_arrive, sums_drain = spread_of(s.sums, "tp", s.ss, s.sr)
    tot_go, tot_arrive, tot_drain = spread_of(s.totals, "sp", s.ts, s.tr)
    ctx_go, ctx_arrive, ctx_drain = spread_of(s.ctx_totals, "sp", s.us, s.ur)

    load_latent.wait()
    ready()
    for p in range(pieces):
        if p < early:
            x_copy(tp, p).start()
        cross(tp, p, 0).start()
    for load in (load_cond, load_ctx_cond, load_mod_w):
        load.wait()
    v = jnp.concatenate([s.cond[...], s.ctx_cond[...]], axis=0)
    activated = (v / (1.0 + jnp.exp(-v))).astype(bf16)
    s.part[sp] = dot(activated, s.mod_w[...])
    part_go()
    load_key_w.wait()
    load_query_w.wait()
    send_own(key_chunks)
    send_own(query_chunks[:PARTS // 2])

    quarter = keys // 4

    def rope(b, carry):
        rows = pl.ds(pl.multiple_of(b * size, size), size)
        lane = lax.broadcasted_iota(jnp.int32, (1, keys), 1)
        index = jnp.bitwise_and(lane, quarter - 1).astype(f32)
        frequency = jnp.exp(index * (-jnp.log(rope_base) / quarter))
        by_row = lane < keys // 2
        first = jnp.bitwise_and(lane, 2 * quarter - 1) < quarter
        place = lax.broadcasted_iota(jnp.int32, (size, 1), 0) + (sp * count + b * size)
        place = place.astype(f32)
        row = jnp.floor((place + 0.5) * (1.0 / GRID_W))
        col = place - row * GRID_W
        angle = jnp.where(by_row, row, col) * frequency
        s.cosine[rows, :] = jnp.cos(angle)
        sine = jnp.sin(angle)
        s.sine[rows, :] = jnp.where(first, -sine, sine)
        return carry

    lax.fori_loop(0, blocks, rope, 0)

    @pl.when(sp == 0)
    def _():
        s.chain_in[0] = jnp.zeros(s.chain_in.shape[1:], bf16)

    @pl.when(sp == sp_count - 1)
    def _():
        s.chain_in[1] = jnp.zeros(s.chain_in.shape[1:], bf16)

    part_arrive()
    total = s.part[0]
    for j in range(1, sp_count):
        total = total + s.part[j]
    s.sums[tp] = total
    sums_go()
    for p in range(early, pieces):
        x_copy(tp, p).start()
    load_out_w.wait()
    out_own_copy().start()
    for k in range(out_pieces + direct):
        out_x(tp, k).start()
    for chunk in key_chunks:
        z_arrive(0, chunk)
    send_own(query_chunks[PARTS // 2:])
    sums_arrive()
    for load in (load_mod_b, load_context, load_low_w, load_value_w, load_decay_w, load_decay_b, load_extra):
        load.wait()
    modulation = (jnp.concatenate([s.sums[j] for j in range(tp_count)], axis=1)
                  + s.mod_b[...])
    s.shifts[...] = modulation[:, :width]
    s.scales[...] = 1.0 + modulation[:, width:2 * width]
    s.branch_gate[...] = modulation[0:1, 2 * width:]
    s.mod_context[...] = (s.context[...].astype(f32) * s.scales[1:2, :]
                             + s.shifts[1:2, :]).astype(bf16)

    def decay_of(low, direction):
        rank = s.decay_w.shape[1]
        logits = dot(low[:, direction * rank:(direction + 1) * rank], s.decay_w[direction])
        return log_sigmoid(logits + s.decay_b[direction:direction + 1, :]) / gate_scale

    own_head = lax.broadcasted_iota(jnp.int32, (ATTENTION_HEADS, size), 0) == tp

    def project_chip(chip):
        rows = pl.ds(pl.multiple_of(chip * 2 * own, 2 * own), 2 * own)
        mod = (s.rows[rows, :].astype(f32) * s.scales[0:1, :]
               + s.shifts[0:1, :]).astype(bf16)
        s.mod_latent[rows, :] = mod
        s.low[rows, :] = dot(mod, s.low_w[...], ((1,), (1,))).astype(bf16)
        s.value[rows, :] = dot(mod, s.value_w[...]).astype(bf16)

    def gate_chip(chip):
        rows = pl.ds(pl.multiple_of(chip * 2 * own, 2 * own), 2 * own)
        s.gate[rows, :] = dot(s.mod_latent[rows, :], s.gate_w[...]).astype(bf16)

    def decay_chip(chip):
        for i in range(2 * own // size):
            b = chip * (2 * own // size) + i
            rows = pl.ds(pl.multiple_of(b * size, size), size)
            low = s.low[rows, :]
            for direction in range(2):
                mask = triangle(size, direction == 1).astype(f32)
                edge = 0 if direction == 1 else size - 1
                head_extra = jnp.sum(jnp.where(own_head, s.extra[direction, :, rows], 0.0),
                                     axis=0, keepdims=True)
                added = jnp.sum(mask * head_extra, axis=1, keepdims=True)
                cum = dot(mask, decay_of(low, direction), precision=highest) + added
                s.cum[direction, rows, :] = cum
                s.block_total[direction, b] = cum[edge:edge + 1, :]

    ctx_low = dot(s.mod_context[...], s.low_w[...], ((1,), (1,))).astype(bf16)
    ctx_totals = []
    for direction in range(2):
        mask = triangle(ctx, direction == 1).astype(f32)
        edge = 0 if direction == 1 else ctx - 1
        cum = dot(mask, decay_of(ctx_low, direction), precision=highest)
        ctx_totals.append(cum[edge:edge + 1, :])
        s.ctx_close[direction] = jnp.exp(ctx_totals[direction] - cum)
    s.ctx_totals[sp] = jnp.concatenate(ctx_totals, axis=0)
    ctx_go()
    s.ctx_value[...] = dot(s.mod_context[...], s.value_w[...]).astype(bf16)
    for chunk in key_chunks:
        if sp_count > 2:
            z_arrive(1, chunk)
    cross_whole(sibling, 0).wait_recv()
    project_chip(x)
    decay_chip(x)
    for chunk in query_chunks:
        z_arrive(0, chunk, False)
    for hop in range(2, sp_count - 1):
        for chunk in key_chunks:
            z_arrive(hop, chunk)
    for chunk in query_chunks:
        y_start(0, chunk)
    for p in range(pieces):
        x_copy(across, p).wait_recv()
        cross(across, p, 1).start()
    load_gate_w.wait()
    gate_chip(x)
    cross_whole(far_sibling, 1).wait_recv()
    project_chip(1 - x)
    if sp_count > 2:
        for chunk in query_chunks:
            z_arrive(1, chunk)
    decay_chip(1 - x)
    for direction in range(2):
        before = None
        for turn in range(blocks):
            b = blocks - 1 - turn if direction == 1 else turn
            if before is not None:
                s.ahead[direction, b:b + 1, :] = before
            block_total = s.block_total[direction, b]
            before = block_total if before is None else before + block_total
        s.total[direction:direction + 1, :] = before
    s.totals[sp] = s.total[...]
    tot_go()
    y_arrive(0)
    chunk_width = s.chain_in.shape[4]
    part_keys = s.chain_in.shape[3]
    chunk_count = vals // chunk_width
    turns_each = s.chain_in.shape[2]
    steps = 2 * turns_each

    def column(row):
        return jnp.broadcast_to(jnp.exp(row).T, (keys, chunk_width))

    def column_chunks():
        return [slice(c * chunk_width, (c + 1) * chunk_width) for c in range(chunk_count)]

    def sum_of(ref, direction, later):
        total = jnp.zeros((1, keys), f32)
        for j in range(sp_count):
            chosen = (j > sp) if later else (j < sp)
            total = total + jnp.where(chosen, ref[j, direction:direction + 1, :], 0.0)
        return total

    ctx_key = dot(s.mod_context[...], s.wqk[0]).astype(bf16).astype(f32)
    ctx_arrive()
    for direction in range(2):
        closing = (ctx_key * s.ctx_close[direction]).astype(bf16)
        after = column(sum_of(s.ctx_totals, direction, direction == 0))
        carry = dot(closing, s.ctx_value[...], ((0,), (0,)))
        for cols in column_chunks():
            s.carry[direction, :, cols] = after * carry[:, cols]
    first_way = jnp.where(sp < sp_count // 2, 0, 1)

    def ends(way):
        return (jnp.where(way == 0, sp > 0, sp < sp_count - 1),
                jnp.where(way == 0, sp < sp_count - 1, sp > 0))

    def chain_copy(way, kind, c, target):
        return remote(s.chain_out.at[way, kind, c], s.chain_in.at[way, kind, c],
                      s.hs.at[way], s.hr.at[way, kind, c], "sp", target)

    def chain_part(c):
        part, col = c % (keys // part_keys), c // (keys // part_keys)
        return (slice(part * part_keys, (part + 1) * part_keys),
                slice(col * chunk_width, (col + 1) * chunk_width))

    def chain_send(way, kind, c):
        rows, cols = chain_part(c)
        held = s.chain_in[way, kind, c].astype(f32)
        if kind == 0:
            added = held + s.carry[1 - way, rows, cols]
        else:
            added = s.own_decay[way, rows, :] * held + s.state[way, rows, cols]
        s.chain_out[way, kind, c] = added.astype(bf16)
        chain_copy(way, kind, c, sp + 1 - 2 * way).start()

    def chain_open(way, kind):
        has_before, has_next = ends(way)

        @pl.when(jnp.logical_and(has_next, jnp.logical_not(has_before)))
        def _():
            if kind == 1:
                for cols in column_chunks():
                    s.state[way, :, cols] += s.own_decay[way] * s.carry[way, :, cols]
            for c in range(turns_each):
                chain_send(way, kind, c)

    def chain(way, i):
        kind, c = i // turns_each, i % turns_each
        has_before, has_next = ends(way)

        @pl.when(has_before)
        def _():
            chain_copy(way, kind, c, sp - 1 + 2 * way).wait_recv()

            @pl.when(has_next)
            def _():
                chain_send(way, kind, c)

    chain_open(first_way, 0)
    for b in range(blocks):
        rows = slice(b * size, (b + 1) * size)
        key = dot(s.mod_latent[rows, :], s.wqk[0]).astype(bf16)
        s.key[rows, :] = rotate(key.astype(f32), s.cosine[rows, :], s.sine[rows, :])
    for direction in range(2):
        edge = 0 if direction == 1 else size - 1
        state = None
        for turn in range(blocks):
            b = blocks - 1 - turn if direction == 1 else turn
            rows = slice(b * size, (b + 1) * size)
            cum = s.cum[direction, rows, :]
            block_total = cum[edge:edge + 1, :]
            closing = (s.key[rows, :] * jnp.exp(block_total - cum)).astype(bf16)
            term = dot(closing, s.value[rows, :], ((0,), (0,)))
            if state is None:
                state = term
            else:
                s.start[direction, b] = state.astype(bf16)
                state = jnp.exp(block_total).T * state + term
        s.state[direction] = state
    for direction in range(2):
        s.own_decay[direction] = column(s.total[direction:direction + 1, :])
    chain_open(first_way, 1)
    relay_x(0)
    tot_arrive()
    for direction in range(2):
        s.ahead_decay[direction] = column(sum_of(s.totals, direction, direction == 1))

        @pl.when(ends(direction)[0])
        def _():
            both = s.own_decay[direction] * s.ahead_decay[direction]
            for cols in column_chunks():
                s.state[direction, :, cols] += both * s.carry[direction, :, cols]

    def attend(b):
        rows = slice(b * size, (b + 1) * size)
        query = dot(s.mod_latent[rows, :], s.wqk[1]).astype(bf16)
        rq = rotate(query.astype(f32) * keys ** -0.5, s.cosine[rows, :], s.sine[rows, :])
        rk = s.key[rows, :]
        scores, out = None, None
        for direction in range(2):
            keep = triangle(size, direction == 1)
            middle = size // 2 if direction == 1 else size // 2 - 1
            cum = s.cum[direction, rows, :]
            center = cum[middle:middle + 1, :]
            q_mid = (rq * jnp.exp(cum - center)).astype(bf16)
            k_mid = (rk * jnp.exp(center - cum)).astype(bf16)
            score = jnp.where(keep, dot(q_mid, k_mid, ((1,), (1,))), 0.0)
            scores = score if scores is None else scores + score
            q_dec = rq * jnp.exp(cum)
            q_all = q_dec
            if b != (blocks - 1 if direction == 1 else 0):
                carried = dot(q_dec.astype(bf16), s.start[direction, b])
                out = carried if out is None else out + carried
                q_all = q_dec * jnp.exp(s.ahead[direction, b:b + 1, :])
            s.q_all[rows, direction * keys:(direction + 1) * keys] = q_all.astype(bf16)
        inner = dot(scores.astype(bf16), s.value[rows, :])
        s.mixture[rows, :] = inner if out is None else out + inner

    lag, early_turns = 4, 8

    def chain_turn(turn):
        if turn < steps:
            chain(first_way, turn)
        if lag <= turn < steps + lag:
            chain(1 - first_way, turn - lag)

    for turn in range(lag):
        chain_turn(turn)
    for hop in range(2, sp_count - 1):
        for chunk in query_chunks:
            z_arrive(hop, chunk)
    for k in range(1, 3):
        relay_x(k)
    gate_chip(1 - x)
    for turn in range(lag, early_turns):
        chain_turn(turn)
    y_arrive(1)
    for turn in range(max(2 * blocks, steps + lag - early_turns)):
        if turn % 2 == 0 and turn < 2 * blocks:
            attend(turn // 2)
        chain_turn(early_turns + turn)
        if turn % 2 == 0 and 3 + turn // 2 < shared:
            relay_x(3 + turn // 2)
    for c in range(turns_each):
        rows, cols = chain_part(c)
        for direction in range(2):
            joined = (s.chain_in[direction, 1, c].astype(f32)
                      + s.ahead_decay[direction, rows, :]
                      * (s.carry[direction, rows, cols]
                         + s.chain_in[1 - direction, 0, c].astype(f32)))
            start = direction * keys + rows.start
            s.joined[start:start + part_keys, cols] = joined.astype(bf16)
    load_norm_gain.wait()

    def gate_rows(j):
        rows = block_rows(j)
        mixture = s.mixture[rows, :] + dot(s.q_all[rows, :], s.joined[...])
        squares = jnp.mean(mixture * mixture, axis=1, keepdims=True)
        gate = s.gate[rows, :].astype(f32)
        normed = mixture * lax.rsqrt(squares + norm_eps) * s.norm_gain[...]
        s.gated[rows, :] = (normed * (gate / (1.0 + jnp.exp(-gate)))).astype(bf16)

    def gated_copy(k, j):
        return remote(s.gated.at[block_rows(j), :], s.gathered.at[tp], s.gs.at[k], s.gr.at[k],
                      "tp", j)

    def gated_arrive(k, j):
        remote(s.gathered.at[j], s.gathered.at[j], s.gs.at[k], s.gr.at[k], "tp", j).wait_recv()

    out_chunks = 4
    out_width = width // out_chunks
    out_cols = [slice(n * out_width, (n + 1) * out_width) for n in range(out_chunks)]

    for k, j in ((1, across), (2, far_sibling), (0, sibling)):
        gate_rows(j)
        gated_copy(k, j).start()
    gate_rows(tp)
    for k in range(max(3, shared), out_pieces + direct):
        relay_x(k)
    out_own_copy(sibling).wait_recv()
    for cols in out_cols:
        s.branch[:, cols] = dot(s.gated[block_rows(tp), :], s.out_w[tp, :, cols])
    gated_arrive(0, sibling)
    for cols in out_cols:
        s.branch[:, cols] += dot(s.gathered[sibling], s.out_w[sibling, :, cols])
    for p in range(shared):
        relay_y(p)
    out_pass(out_bytes(out_pieces + direct), 0).wait_recv()
    out_pass(out_bytes(shared), 1).wait_recv()
    gated_arrive(1, across)
    for cols in out_cols:
        s.branch[:, cols] += dot(s.gathered[across], s.out_w[across, :, cols])
    gated_arrive(2, far_sibling)
    for cols in out_cols:
        branch = s.branch[:, cols] + dot(s.gathered[far_sibling], s.out_w[far_sibling, :, cols])
        summed_ref[:, cols] = (residual_scale * s.rows[block_rows(tp), cols].astype(f32)
                             + s.branch_gate[:, cols] * branch)
    part_drain()
    sums_drain()
    tot_drain()
    ctx_drain()
    line.drain_whole(s.wqk.at[0, pl.ds(0, depth), :])
    y_drain()
    own_rows = s.rows.at[block_rows(tp), :]
    remote(own_rows, own_rows, s.xs.at[0], s.xr.at[0], "tp", across).wait_send()
    for slot in range(2):
        cross_whole(tp, slot).wait_send()
    for way in range(2):
        has_next = sp < sp_count - 1 if way == 0 else sp > 0

        @pl.when(has_next)
        def _():
            remote(s.chain_out.at[way], s.chain_in.at[way], s.hs.at[way], s.hr.at[way, 0, 0],
                   "sp", sp + 1 - 2 * way).wait_send()
    out_own_copy().wait_send()
    ref = out_bytes(out_pieces + direct)
    remote(ref, ref, s.oxs.at[0], s.oxr.at[0], "tp", across).wait_send()
    out_pass(ref, 0).wait_send()
    ref = out_bytes(shared)
    remote(ref, ref, s.oys.at[0], s.oyr.at[0], "grp", 1 - grp).wait_send()
    out_pass(ref, 1).wait_send()
    for k, j in enumerate((sibling, across, far_sibling)):
        gated_copy(k, j).wait_send()


def norm_kernel(summed_ref, gain_ref, bias_ref, out_ref):
    summed = summed_ref[...]
    centered = summed - jnp.mean(summed, axis=1, keepdims=True)
    variance = jnp.mean(centered * centered, axis=1, keepdims=True)
    out_ref[...] = (centered * lax.rsqrt(variance + norm_eps) * gain_ref[...]
                    + bias_ref[...]).astype(bf16)


def fused(latent, context, condition, context_condition, mod_weight, mod_bias, query_weight,
          key_weight, value_weight, out_gate_weight, decay_in_weight, decay_weight, decay_bias,
          extra_decay, norm_gain, out_weight, final_gain, final_bias):
    sp_count, tp_count = lax.axis_size("sp"), lax.axis_size("tp")
    own, width = latent.shape
    depth = query_weight.shape[0]
    keys = query_weight.shape[1] // ATTENTION_HEADS
    vals = value_weight.shape[1]
    ctx = context.shape[0]
    count = own * tp_count
    blocks = count // (2 * BLOCK)
    mod_cols = mod_weight.shape[1]
    chains, outs, pieces = 4, 8, 8
    args = (latent, context, condition[None, :], context_condition[None, :], mod_weight,
            mod_bias[None, :], query_weight, key_weight, value_weight, out_gate_weight,
            decay_in_weight.T, decay_weight, decay_bias, extra_decay, norm_gain[None, :],
            out_weight)
    dma, vmem = pltpu.SemaphoreType.DMA, pltpu.VMEM
    hops = sp_count - 1
    scratch = Scratch(
        cond=vmem((1, condition.shape[0]), f32),
        ctx_cond=vmem((1, condition.shape[0]), f32),
        mod_w=vmem(mod_weight.shape, bf16),
        mod_b=vmem((1, mod_bias.shape[0]), f32),
        wqk=vmem((2, depth * sp_count, keys), bf16),
        rows=vmem((count, width), bf16),
        mod_latent=vmem((count, width), bf16),
        context=vmem(context.shape, bf16),
        mod_context=vmem(context.shape, bf16),
        low_w=vmem(decay_in_weight.shape[::-1], bf16),
        value_w=vmem(value_weight.shape, bf16),
        gate_w=vmem(out_gate_weight.shape, bf16),
        out_w=vmem((tp_count,) + out_weight.shape, bf16),
        decay_w=vmem(decay_weight.shape[:2] + (keys,), bf16),
        decay_b=vmem((2, keys), f32),
        extra=vmem(extra_decay.shape, f32),
        norm_gain=vmem((1, vals), f32),
        part=vmem((sp_count, 2, mod_cols), f32),
        sums=vmem((tp_count, 2, mod_cols), f32),
        totals=vmem((sp_count, 2, keys), f32),
        ctx_totals=vmem((sp_count, 2, keys), f32),
        shifts=vmem((2, width), f32),
        scales=vmem((2, width), f32),
        branch_gate=vmem((1, width), f32),
        cosine=vmem((count, keys), f32),
        sine=vmem((count, keys), f32),
        ctx_close=vmem((2, ctx, keys), f32),
        ctx_value=vmem((ctx, vals), bf16),
        low=vmem((count, decay_in_weight.shape[1]), bf16),
        value=vmem((count, vals), bf16),
        gate=vmem((count, vals), bf16),
        key=vmem((count, keys), f32),
        cum=vmem((2, count, keys), f32),
        ahead=vmem((2, blocks, keys), f32),
        block_total=vmem((2, blocks, 1, keys), f32),
        total=vmem((2, keys), f32),
        start=vmem((2, blocks, keys, vals), bf16),
        state=vmem((2, keys, vals), f32),
        carry=vmem((2, keys, vals), f32),
        own_decay=vmem((2, keys, vals // chains), f32),
        ahead_decay=vmem((2, keys, vals // chains), f32),
        chain_in=vmem((2, 2, 2 * chains, keys // 2, vals // chains), bf16),
        chain_out=vmem((2, 2, 2 * chains, keys // 2, vals // chains), bf16),
        q_all=vmem((count, 2 * keys), bf16),
        mixture=vmem((count, vals), f32),
        joined=vmem((2 * keys, vals), bf16),
        gated=vmem((count, vals), bf16),
        gathered=vmem((tp_count, own, vals), bf16),
        branch=vmem((own, width), f32),
        load_sem=dma((len(args),)),
        zs=dma((2, hops)), zr=dma((2, hops, 2 * PARTS)),
        ys=dma((2, hops)), yr=dma((2, hops, 2)),
        xs=dma((1,)), xr=dma((pieces,)), cs=dma((2,)), cr=dma((2,)),
        ocs=dma((1,)), ocr=dma((1,)), ods=dma((2,)), odr=dma((2,)),
        oxs=dma((1,)), oxr=dma((outs + outs // 4,)), oys=dma((1,)), oyr=dma((outs,)),
        gs=dma((tp_count - 1,)), gr=dma((tp_count - 1,)),
        ps=dma((hops,)), pr=dma((hops,)), ts=dma((hops,)), tr=dma((hops,)),
        us=dma((hops,)), ur=dma((hops,)),
        ss=dma((tp_count - 1,)), sr=dma((tp_count - 1,)),
        hs=dma((2,)), hr=dma((2, 2, 2 * chains)),
    )
    summed = pl.pallas_call(
        fused_kernel,
        out_shape=pltpu.VMEM((own, width), f32),
        in_specs=[pl.BlockSpec(memory_space=pltpu.HBM)] * len(args),
        out_specs=pl.BlockSpec(memory_space=pltpu.VMEM),
        scratch_shapes=[scratch],
        compiler_params=pltpu.CompilerParams(
            vmem_limit_bytes=60 * 1024 * 1024, collective_id=2, has_side_effects=True),
        cost_estimate=pl.CostEstimate(flops=6_000_000_000, bytes_accessed=12_000_000,
                                      transcendentals=2_000_000),
    )(*args)
    return pl.pallas_call(
        norm_kernel,
        out_shape=jax.ShapeDtypeStruct((own, width), bf16),
        in_specs=[pl.BlockSpec(memory_space=pltpu.VMEM)] * 3,
        out_specs=pl.BlockSpec(memory_space=pltpu.VMEM),
        compiler_params=pltpu.CompilerParams(vmem_limit_bytes=8 * 1024 * 1024),
        cost_estimate=pl.CostEstimate(flops=2_000_000, bytes_accessed=2_000_000,
                                      transcendentals=1_000),
    )(summed, final_gain[None, :], final_bias[None, :])


def whole_heads(mesh):
    return mesh.shape["tp"] == ATTENTION_HEADS and mesh.shape["grp"] == 2


def solution(mesh):
    placed = (
        P(("grp", "sp", "tp"), None),
        P(("grp", "sp"), None),
        P(("grp", "sp")),
        P("sp"),
        P("sp", "tp"),
        P(),
        P("sp", None),
        P("sp", None),
        P(None, "tp"),
        P(None, "tp"),
        P(),
        P(),
        P(),
        P(None, None, "sp"),
        P(),
        P("tp", None),
        P(),
        P(),
    )
    return jax.shard_map(
        fused if whole_heads(mesh) else body, mesh=mesh, in_specs=placed, out_specs=P(("grp", "sp", "tp"), None), check_vma=False
    )
```

```python
import functools
from typing import Any, NamedTuple

import jax
import jax.numpy as jnp
from jax import lax
from jax.experimental import pallas as pl
from jax.experimental.pallas import tpu as pltpu
from jax.sharding import PartitionSpec as P

ATTENTION_HEADS = 4
DV = 512
BLOCK = 64
GRID_W = 64


norm_eps = 1e-05
gate_scale = 16.0
rope_base = 10000.0
residual_scale = 2.0**0.5
highest = lax.Precision.HIGHEST
f32 = jnp.float32
bf16 = jnp.bfloat16


def rope_tables(token_places, width):
    quarter = width // 4
    frequency = rope_base ** (-jnp.arange(quarter, dtype=f32) / quarter)
    row_angle = (token_places // GRID_W).astype(f32)[:, None] * frequency
    col_angle = (token_places % GRID_W).astype(f32)[:, None] * frequency
    cosine = jnp.concatenate([jnp.cos(row_angle)] * 2 + [jnp.cos(col_angle)] * 2, axis=1)
    row_sine, col_sine = jnp.sin(row_angle), jnp.sin(col_angle)
    sine = jnp.concatenate([-row_sine, row_sine, -col_sine, col_sine], axis=1)
    return cosine, sine


def dot(a, b, contract=((1,), (0,)), precision=None):
    return lax.dot_general(a, b, (contract, ((), ())), precision=precision,
                           preferred_element_type=f32)


def log_sigmoid(x):
    return jnp.minimum(x, 0.0) - jnp.log1p(jnp.exp(-jnp.abs(x)))


def rotate(x, cosine, sine):
    half = x.shape[1] // 2
    parts = [pltpu.roll(x[:, i * half:(i + 1) * half], half // 2, 1) for i in range(2)]
    return x * cosine + jnp.concatenate(parts, axis=1) * sine


def triangle(size, reverse):
    row = lax.broadcasted_iota(jnp.int32, (size, size), 0)
    col = lax.broadcasted_iota(jnp.int32, (size, size), 1)
    return row <= col if reverse else row >= col


def decay_block(low, decay_weight, decay_bias, direction):
    rank = decay_weight.shape[1]
    logits = dot(low[:, direction * rank:(direction + 1) * rank], decay_weight[direction])
    return log_sigmoid(logits + decay_bias[direction:direction + 1, :]) / gate_scale


def context_kernel(k_ref, v_ref, low_ref, dw_ref, db_ref, state_ref):
    length, width = k_ref.shape
    size = min(2 * BLOCK, length)
    count = length // size
    for direction in range(2):
        mask = triangle(size, direction == 1).astype(f32)
        edge = 0 if direction == 1 else size - 1
        state = None
        for step in range(count):
            b = count - 1 - step if direction == 1 else step
            rows = slice(b * size, (b + 1) * size)
            logdec = decay_block(low_ref[rows, :], dw_ref[...], db_ref[...], direction)
            cum = dot(mask, logdec, precision=highest)
            total = cum[edge:edge + 1, :]
            closing = (k_ref[rows, :].astype(f32) * jnp.exp(total - cum)).astype(bf16)
            term = dot(closing, v_ref[rows, :], ((0,), (0,)))
            state = term if state is None else jnp.exp(total).T * state + term
        state_ref[direction] = state


def local_kernel(q_ref, k_ref, v_ref, low_ref, extra_ref, dw_ref, db_ref, cos_ref, sin_ref,
                 out_ref, qc_ref, state_ref, total_ref):
    length, width = q_ref.shape
    size = 2 * BLOCK
    count = length // size
    rq, rk, within, scores = [], [], [], []
    for b in range(count):
        rows = slice(b * size, (b + 1) * size)
        cosine, sine = cos_ref[rows, :], sin_ref[rows, :]
        rq.append(rotate(q_ref[rows, :].astype(f32) * width ** -0.5, cosine, sine))
        rk.append(rotate(k_ref[rows, :].astype(f32), cosine, sine))
        scores.append(None)
    for direction in range(2):
        keep = triangle(size, direction == 1)
        mask = keep.astype(f32)
        edge = 0 if direction == 1 else size - 1
        middle = size // 2 if direction == 1 else size // 2 - 1
        state = None
        before = None
        for step in range(count):
            b = count - 1 - step if direction == 1 else step
            rows = slice(b * size, (b + 1) * size)
            logdec = decay_block(low_ref[rows, :], dw_ref[...], db_ref[...], direction)
            logdec = logdec + extra_ref[rows, direction:direction + 1]
            cum = dot(mask, logdec, precision=highest)
            total = cum[edge:edge + 1, :]
            center = cum[middle:middle + 1, :]
            q_mid = (rq[b] * jnp.exp(cum - center)).astype(bf16)
            k_mid = (rk[b] * jnp.exp(center - cum)).astype(bf16)
            score = jnp.where(keep, dot(q_mid, k_mid, ((1,), (1,))), 0.0)
            q_dec = rq[b] * jnp.exp(cum)
            if direction == 0:
                scores[b] = score
                out = None
            else:
                out = dot((scores[b] + score).astype(bf16), v_ref[rows, :])
            if state is not None:
                carried = dot(q_dec.astype(bf16), state.astype(bf16))
                out = carried if out is None else out + carried
            if direction == 0:
                out_ref[rows, :] = jnp.zeros((size, v_ref.shape[1]), f32) if out is None else out
            else:
                out_ref[rows, :] += out
            q_all = q_dec if before is None else q_dec * jnp.exp(before)
            qc_ref[rows, direction * width:(direction + 1) * width] = q_all.astype(bf16)
            closing = (rk[b] * jnp.exp(total - cum)).astype(bf16)
            term = dot(closing, v_ref[rows, :], ((0,), (0,)))
            state = term if state is None else jnp.exp(total).T * state + term
            before = total if before is None else before + total
        state_ref[direction * width:(direction + 1) * width, :] = state.astype(bf16)
        total_ref[direction:direction + 1, :] = before


def join_kernel(final, out_ref, qc_ref, states_ref, totals_ref, start_ref, gate_ref, gain_ref,
                place_ref, result_ref):
    count = states_ref.shape[0]
    width = qc_ref.shape[1] // 2
    place = place_ref[...]
    mixture = out_ref[...]
    for direction in range(2):
        state = start_ref[direction]
        for lap in range(count):
            j = count - 1 - lap if direction == 1 else lap
            decay = jnp.exp(totals_ref[j, direction:direction + 1, :]).T
            joined = decay * state + states_ref[
                j, direction * width:(direction + 1) * width, :].astype(f32)
            ahead = place < j if direction == 1 else place > j
            state = jnp.where(ahead, joined, state)
        mixture = mixture + dot(qc_ref[:, direction * width:(direction + 1) * width],
                                state.astype(bf16))
    if final:
        squares = jnp.mean(mixture * mixture, axis=1, keepdims=True)
        gate = gate_ref[...].astype(f32)
        normed = mixture * lax.rsqrt(squares + norm_eps) * gain_ref[...]
        result_ref[...] = (normed * (gate / (1.0 + jnp.exp(-gate)))).astype(bf16)
    else:
        result_ref[...] = mixture


def call(kernel, out_shape, *args):
    return pl.pallas_call(
        kernel,
        out_shape=out_shape,
        in_specs=[pl.BlockSpec(memory_space=pltpu.VMEM)] * len(args),
        out_specs=jax.tree.map(lambda _: pl.BlockSpec(memory_space=pltpu.VMEM), out_shape),
        compiler_params=pltpu.CompilerParams(vmem_limit_bytes=48 * 1024 * 1024),
        cost_estimate=pl.CostEstimate(flops=4_000_000_000, bytes_accessed=4_000_000,
                                      transcendentals=1_000_000),
    )(*args)


MESH = pl.DeviceIdType.MESH


def remote(src, dst, send_sem, recv_sem, axis, target):
    return pltpu.make_async_remote_copy(
        src_ref=src, dst_ref=dst, send_sem=send_sem, recv_sem=recv_sem,
        device_id={axis: target}, device_id_type=MESH)


class Line:
    def __init__(self, place, count, axis, target_of, view, chunks, send_sem, recv_sem):
        self.place, self.count, self.axis, self.target_of = place, count, axis, target_of
        self.view, self.chunks, self.send_sem, self.recv_sem = view, chunks, send_sem, recv_sem

    def copy(self, way, hop, chunk, block, target):
        ref = self.view(block, chunk)
        return remote(ref, ref, self.send_sem.at[way, hop, chunk],
                      self.recv_sem.at[way, hop, chunk], self.axis, self.target_of(target))

    def outgoing(self, way, hop):
        place, count = self.place, self.count
        if way == 0:
            return place - hop, place + 1, jnp.logical_and(place >= hop, place < count - 1)
        return place + hop, place - 1, jnp.logical_and(place + hop < count, place > 0)

    def each_send(self, way, hop, chunk, act):
        block, target, valid = self.outgoing(way, hop)

        @pl.when(valid)
        def _():
            act(self.copy(way, hop, chunk, block, target))

    def send(self, way, hop, chunk):
        self.each_send(way, hop, chunk, lambda c: c.start())

    def drain(self):
        for way in range(2):
            for hop in range(self.count - 1):
                for chunk in range(self.chunks):
                    self.each_send(way, hop, chunk, lambda c: c.wait_send())

    def arrive(self, way, hop, chunk, then=None):
        if way == 0:
            block, source, valid = self.place - 1 - hop, self.place - 1, self.place > hop
        else:
            block, source = self.place + 1 + hop, self.place + 1
            valid = self.place + 1 + hop < self.count

        @pl.when(valid)
        def _():
            self.copy(way, hop, chunk, block, source).wait_recv()
            if then is not None:
                then(block)

    def forward(self, hop, then=None):
        for chunk in range(self.chunks):
            for way in range(2):
                self.arrive(way, hop, chunk, None if then is None else functools.partial(then, way))
                if hop + 1 < self.count - 1:
                    self.send(way, hop + 1, chunk)


def open_kernel(partners):
    barrier = pltpu.get_barrier_semaphore()
    for axis, target in partners:
        pl.semaphore_signal(barrier, inc=1, device_id={axis: target}, device_id_type=MESH)
    return lambda: pl.semaphore_wait(barrier, len(partners))


def others(axis):
    count, place = lax.axis_size(axis), lax.axis_index(axis)
    return [lax.rem(place + k, count) for k in range(1, count)]


def sources(axis):
    count, place = lax.axis_size(axis), lax.axis_index(axis)
    return [lax.rem(place + count - k, count) for k in range(1, count)]


def spread(buffer, axis, send_sem, recv_sem):
    place = lax.axis_index(axis)
    for k, target in enumerate(others(axis)):
        remote(buffer.at[place], buffer.at[place], send_sem.at[k], recv_sem.at[k],
               axis, target).start()


def spread_arrive(buffer, axis, send_sem, recv_sem):
    for k, source in enumerate(sources(axis)):
        remote(buffer.at[source], buffer.at[source], send_sem.at[k], recv_sem.at[k],
               axis, source).wait_recv()


def spread_drain(buffer, axis, send_sem, recv_sem):
    place = lax.axis_index(axis)
    for k, target in enumerate(others(axis)):
        remote(buffer.at[place], buffer.at[place], send_sem.at[k], recv_sem.at[k],
               axis, target).wait_send()


def enter_kernel(chunks, latent_ref, context_ref, cond_ref, mw_ref, mb_ref, qw_ref, kw_ref,
                 ml_ref, mc_ref, gate_ref, qk_ref,
                 rows_ref, part_ref, sums_ref, zs, zr, xs, xr, cs, cr, ps, pr, ss, sr):
    sp, sp_count = lax.axis_index("sp"), lax.axis_size("sp")
    tp, tp_count = lax.axis_index("tp"), lax.axis_size("tp")
    own, model_width = latent_ref.shape
    depth = qw_ref.shape[0]
    head_keys = qk_ref.shape[1] // 2
    ready = open_kernel([("sp", t) for t in others("sp")] + [("tp", t) for t in others("tp")])
    v = cond_ref[...]
    activated = (v / (1.0 + jnp.exp(-v))).astype(bf16)
    part_ref[sp] = dot(activated, mw_ref[...])
    columns = pl.ds(pl.multiple_of((tp // (tp_count // ATTENTION_HEADS)) * head_keys, head_keys),
                    head_keys)
    qk_rows = pl.ds(pl.multiple_of(sp * depth, depth), depth)
    qk_ref[qk_rows, :head_keys] = qw_ref[:, columns]
    qk_ref[qk_rows, head_keys:] = kw_ref[:, columns]
    rows_ref[pl.ds(pl.multiple_of(tp * own, own), own), :] = latent_ref[...]

    step = depth // chunks
    z_line = Line(
        sp, sp_count, "sp", lambda p: p,
        lambda block, chunk: qk_ref.at[
            pl.ds(pl.multiple_of(block * depth + chunk * step, step), step), :],
        chunks, zs, zr)
    x_count = tp_count // 2
    x, core = tp // 2, tp % 2

    def rows_of(block, chunk):
        return rows_ref.at[pl.ds(pl.multiple_of((2 * block + core) * own, own), own), :]

    x_line = Line(x, x_count, "tp", lambda p: 2 * p + core, rows_of, 1, xs, xr)
    sibling = tp + 1 - 2 * core

    def cross(block, slot, other=False):
        side = 1 - core if other else core
        ref = rows_ref.at[pl.ds(pl.multiple_of((2 * block + side) * own, own), own), :]
        return remote(ref, ref, cs.at[slot], cr.at[slot], "tp", sibling)

    def slot_of(way, hop):
        return 1 + way * (x_count - 1) + hop

    ready()
    spread(part_ref, "sp", ps, pr)
    for way in range(2):
        x_line.send(way, 0, 0)
    cross(x, 0).start()
    for chunk in range(chunks):
        for way in range(2):
            z_line.send(way, 0, chunk)
    spread_arrive(part_ref, "sp", ps, pr)
    total = part_ref[0]
    for j in range(1, sp_count):
        total = total + part_ref[j]
    sums_ref[tp] = total
    spread(sums_ref, "tp", ss, sr)
    z_line.forward(0)
    for hop in range(x_count - 1):
        x_line.forward(hop, lambda way, block, hop=hop: cross(block, slot_of(way, hop)).start())
    if sp_count > 2:
        z_line.forward(1)
    spread_arrive(sums_ref, "tp", ss, sr)
    modulation = jnp.concatenate([sums_ref[j] for j in range(tp_count)], axis=1) + mb_ref[...]
    shifts = modulation[:, :model_width]
    scales = modulation[:, model_width:2 * model_width]
    gate_ref[...] = modulation[0:1, 2 * model_width:]
    mc_ref[...] = (context_ref[...].astype(f32) * (1.0 + scales[1:2]) + shifts[1:2]).astype(bf16)

    def each_cross(act_own, act_line):
        act_own()
        for way in range(2):
            for hop in range(x_count - 1):
                block = x - 1 - hop if way == 0 else x + 1 + hop
                valid = x > hop if way == 0 else x + 1 + hop < x_count

                @pl.when(valid)
                def _():
                    act_line(block, slot_of(way, hop))

    each_cross(lambda: cross(x, 0, True).wait_recv(),
               lambda block, slot: cross(block, slot, True).wait_recv())
    for j in range(tp_count):
        rows = slice(j * own, (j + 1) * own)
        ml_ref[rows, :] = (rows_ref[rows, :].astype(f32) * (1.0 + scales[0:1])
                           + shifts[0:1]).astype(bf16)
    for hop in range(2, sp_count - 1):
        z_line.forward(hop)
    each_cross(lambda: cross(x, 0).wait_send(),
               lambda block, slot: cross(block, slot).wait_send())
    spread_drain(part_ref, "sp", ps, pr)
    spread_drain(sums_ref, "tp", ss, sr)
    x_line.drain()
    z_line.drain()


def comm_call(kernel, out_shape, scratch, collective_id, *args):
    return pl.pallas_call(
        kernel,
        out_shape=out_shape,
        in_specs=[pl.BlockSpec(memory_space=pltpu.VMEM)] * len(args),
        out_specs=jax.tree.map(lambda _: pl.BlockSpec(memory_space=pltpu.VMEM), out_shape),
        scratch_shapes=scratch,
        compiler_params=pltpu.CompilerParams(
            vmem_limit_bytes=48 * 1024 * 1024, collective_id=collective_id,
            has_side_effects=True),
        cost_estimate=pl.CostEstimate(flops=20_000_000_000, bytes_accessed=60_000_000,
                                      transcendentals=1_000_000),
    )(*args)


def enter(latent, context, cond, mod_weight, mod_bias, query_weight, key_weight):
    sp_count, tp_count = lax.axis_size("sp"), lax.axis_size("tp")
    own, model_width = latent.shape
    depth = query_weight.shape[0]
    head_keys = query_weight.shape[1] // ATTENTION_HEADS
    chunks = 4
    sds = jax.ShapeDtypeStruct
    dma = pltpu.SemaphoreType.DMA
    x_hops = tp_count // 2 - 1
    return comm_call(
        functools.partial(enter_kernel, chunks),
        (
            sds((own * tp_count, model_width), bf16),
            sds(context.shape, bf16),
            sds((1, model_width), f32),
            sds((depth * sp_count, 2 * head_keys), bf16),
        ),
        [
            pltpu.VMEM((own * tp_count, model_width), bf16),
            pltpu.VMEM((sp_count, 2, mod_weight.shape[1]), f32),
            pltpu.VMEM((tp_count, 2, mod_weight.shape[1]), f32),
            dma((2, sp_count - 1, chunks)), dma((2, sp_count - 1, chunks)),
            dma((2, x_hops, 1)), dma((2, x_hops, 1)),
            dma((1 + 2 * x_hops,)), dma((1 + 2 * x_hops,)),
            dma((sp_count - 1,)), dma((sp_count - 1,)),
            dma((tp_count - 1,)), dma((tp_count - 1,)),
        ],
        1, latent, context, cond, mod_weight, mod_bias[None, :], query_weight, key_weight,
    )


def project(rows, weight):
    return jnp.dot(rows, weight, preferred_element_type=f32).astype(bf16)


def body(
    latent,
    context,
    condition,
    context_condition,
    mod_weight,
    mod_bias,
    query_weight,
    key_weight,
    value_weight,
    out_gate_weight,
    decay_in_weight,
    decay_weight,
    decay_bias,
    extra_decay,
    norm_gain,
    out_weight,
    final_gain,
    final_bias,
):
    head_keys = query_weight.shape[1] // ATTENTION_HEADS
    value_cols = value_weight.shape[1]
    tp_index = lax.axis_index("tp")
    sp_index = lax.axis_index("sp")
    head_share = lax.axis_size("tp") // ATTENTION_HEADS
    head_index = tp_index // head_share
    part_index = tp_index % head_share
    key_start = head_index * head_keys

    full_out = lax.all_gather(out_weight, "tp", axis=0, tiled=True)
    mod_latent, mod_context, branch_gate, qk_head = enter(
        latent, context, jnp.stack([condition, context_condition]), mod_weight, mod_bias,
        query_weight, key_weight,
    )
    context_local = jnp.concatenate(
        [
            project(mod_context, qk_head[:, head_keys:]),
            project(mod_context, value_weight),
            project(mod_context, decay_in_weight),
        ],
        axis=1,
    )
    gathered_context = lax.all_gather(context_local, "sp", axis=0, tiled=True)
    qk = project(mod_latent, qk_head)
    value_rows = project(mod_latent, value_weight)
    out_gate = project(mod_latent, out_gate_weight)
    low_rank = project(mod_latent, decay_in_weight)
    count = mod_latent.shape[0]
    token_places = sp_index * count + jnp.arange(count, dtype=jnp.int32)
    cosine, sine = rope_tables(token_places, head_keys)
    head_bias = lax.dynamic_slice_in_dim(decay_bias, key_start, head_keys, 1)
    head_gate = lax.dynamic_slice_in_dim(decay_weight, key_start, head_keys, 2)
    head_extra = lax.dynamic_index_in_dim(extra_decay, head_index, 1, keepdims=False).T

    sds = jax.ShapeDtypeStruct
    out_local, qc, states, totals = call(
        local_kernel,
        (
            sds((count, value_cols), f32),
            sds((count, 2 * head_keys), bf16),
            sds((2 * head_keys, value_cols), bf16),
            sds((2, head_keys), f32),
        ),
        qk[:, :head_keys], qk[:, head_keys:], value_rows, low_rank, head_extra, head_gate,
        head_bias, cosine, sine,
    )
    start = call(
        context_kernel,
        sds((2, head_keys, value_cols), f32),
        gathered_context[:, :head_keys],
        gathered_context[:, head_keys : head_keys + value_cols],
        gathered_context[:, head_keys + value_cols :],
        head_gate, head_bias,
    )
    states, totals, full_out = lax.optimization_barrier((states, totals, full_out))
    all_states = lax.all_gather(states, "sp")
    all_totals = lax.all_gather(totals, "sp")
    place = jnp.full((1, value_cols), sp_index, jnp.int32)
    gain_slice = lax.dynamic_slice_in_dim(norm_gain, part_index * value_cols, value_cols, 0)
    final = head_share == 1
    joined = call(
        functools.partial(join_kernel, final),
        sds((count, value_cols), bf16 if final else f32),
        out_local, qc, all_states, all_totals, start, out_gate, gain_slice[None, :], place,
    )
    if final:
        gated_rows = joined
    else:
        squares = jnp.sum(joined * joined, axis=1)
        onehot = (jnp.arange(ATTENTION_HEADS) == head_index).astype(f32)
        sums = lax.psum(onehot[:, None] * squares[None, :], "tp")
        head_sum = jnp.sum(sums * onehot[:, None], axis=0)
        normed = joined * lax.rsqrt(head_sum / DV + norm_eps)[:, None] * gain_slice
        gated_rows = (normed * jax.nn.silu(out_gate.astype(f32))).astype(bf16)
    regrouped = lax.all_to_all(gated_rows, "tp", split_axis=0, concat_axis=1, tiled=True)
    branch = jnp.dot(regrouped, full_out, preferred_element_type=f32)
    summed = residual_scale * latent.astype(f32) + branch_gate * branch
    row_mean = jnp.mean(summed, axis=1, keepdims=True)
    centered = summed - row_mean
    variance = jnp.mean(centered * centered, axis=1, keepdims=True)
    return (centered * lax.rsqrt(variance + norm_eps) * final_gain + final_bias).astype(bf16)


class Scratch(NamedTuple):
    cond: Any
    ctx_cond: Any
    mod_w: Any
    mod_b: Any
    wqk: Any
    rows: Any
    mod_latent: Any
    context: Any
    mod_context: Any
    low_w: Any
    value_w: Any
    gate_w: Any
    out_w: Any
    decay_w: Any
    decay_b: Any
    extra: Any
    norm_gain: Any
    part: Any
    sums: Any
    totals: Any
    ctx_totals: Any
    shifts: Any
    scales: Any
    branch_gate: Any
    cosine: Any
    sine: Any
    ctx_close: Any
    ctx_value: Any
    low: Any
    value: Any
    gate: Any
    key: Any
    cum: Any
    ahead: Any
    block_total: Any
    total: Any
    start: Any
    state: Any
    carry: Any
    own_decay: Any
    ahead_decay: Any
    chain_in: Any
    chain_out: Any
    q_all: Any
    mixture: Any
    joined: Any
    gated: Any
    gathered: Any
    branch: Any
    load_sem: Any
    zs: Any
    zr: Any
    ys: Any
    yr: Any
    xs: Any
    xr: Any
    cs: Any
    cr: Any
    ocs: Any
    ocr: Any
    ods: Any
    odr: Any
    oxs: Any
    oxr: Any
    oys: Any
    oyr: Any
    gs: Any
    gr: Any
    ps: Any
    pr: Any
    ts: Any
    tr: Any
    us: Any
    ur: Any
    ss: Any
    sr: Any
    hs: Any
    hr: Any


def spread_of(ref, axis, send_sem, recv_sem):
    return (lambda: spread(ref, axis, send_sem, recv_sem),
            lambda: spread_arrive(ref, axis, send_sem, recv_sem),
            lambda: spread_drain(ref, axis, send_sem, recv_sem))


class SharedLine(Line):
    def copy(self, way, hop, chunk, block, target):
        ref = self.view(block, chunk)
        return remote(ref, ref, self.send_sem.at[way, hop], self.recv_sem.at[way, hop, chunk],
                      self.axis, self.target_of(target))

    def drain_whole(self, whole):
        for way in range(2):
            for hop in range(self.count - 1):
                block, target, valid = self.outgoing(way, hop)

                @pl.when(valid)
                def _():
                    remote(whole, whole, self.send_sem.at[way, hop],
                           self.recv_sem.at[way, hop, 0], self.axis,
                           self.target_of(target)).wait_send()


PARTS = 4


def fused_kernel(latent, context, cond, ctx_cond, mod_w, mod_b, query_w, key_w, value_w, gate_w,
                 low_w, decay_w, decay_b, extra, norm_gain, out_w, summed_ref, s):
    grp = lax.axis_index("grp")
    sp, sp_count = lax.axis_index("sp"), lax.axis_size("sp")
    tp, tp_count = lax.axis_index("tp"), lax.axis_size("tp")
    own, width = latent.shape
    depth = query_w.shape[0]
    keys = query_w.shape[1] // ATTENTION_HEADS
    vals = value_w.shape[1]
    count = own * tp_count
    size = 2 * BLOCK
    blocks = count // size
    ctx = context.shape[0]
    x, core = tp // 2, tp % 2
    sibling, across = tp + 1 - 2 * core, 2 * (1 - x) + core
    far_sibling = 2 * (1 - x) + 1 - core

    def block_rows(j):
        return pl.ds(pl.multiple_of(j * own, own), own)

    ready = open_kernel([("sp", t) for t in others("sp")] + [("tp", t) for t in others("tp")]
                        + [("grp", 1 - grp)])
    head_cols = pl.ds(pl.multiple_of(tp * keys, keys), keys)
    own_depth = pl.ds(pl.multiple_of(sp * depth, depth), depth)
    loads = []
    for i, (source, target) in enumerate((
        (latent, s.rows.at[block_rows(tp), :]),
        (cond, s.cond), (ctx_cond, s.ctx_cond), (mod_w, s.mod_w),
        (key_w.at[:, head_cols], s.wqk.at[0, own_depth, :]),
        (query_w.at[:, head_cols], s.wqk.at[1, own_depth, :]),
        (mod_b, s.mod_b), (context, s.context),
        (low_w, s.low_w), (value_w, s.value_w),
        (decay_w.at[:, :, head_cols], s.decay_w),
        (decay_b.at[:, head_cols], s.decay_b), (extra, s.extra),
        (gate_w, s.gate_w), (norm_gain, s.norm_gain),
        (out_w, s.out_w.at[tp]),
    )):
        loads.append(pltpu.make_async_copy(source, target, s.load_sem.at[i]))
        loads[i].start()
    (load_latent, load_cond, load_ctx_cond, load_mod_w, load_key_w, load_query_w,
     load_mod_b, load_context, load_low_w, load_value_w, load_decay_w, load_decay_b,
     load_extra, load_gate_w, load_norm_gain, load_out_w) = loads

    half = depth // 2
    step = half // PARTS

    def weight_view(side):
        def view(block, chunk):
            start = block * depth + side * half + (chunk % PARTS) * step
            return s.wqk.at[chunk // PARTS, pl.ds(pl.multiple_of(start, step), step), :]
        return view

    line = SharedLine(sp, sp_count, "sp", lambda p: p, weight_view(grp), 2 * PARTS, s.zs, s.zr)

    def y_copy(ref, way, hop, matrix):
        return remote(ref, ref, s.ys.at[way, hop], s.yr.at[way, hop, matrix], "grp", 1 - grp)

    def z_arrive(hop, chunk, pass_on=True):
        for way in range(2):
            line.arrive(way, hop, chunk, (lambda block: y_copy(
                weight_view(grp)(block, chunk), way, hop, chunk // PARTS).start()) if pass_on else None)
            if hop + 1 < sp_count - 1:
                line.send(way, hop + 1, chunk)

    def y_each(hop, act):
        for way in range(2):
            block = sp - 1 - hop if way == 0 else sp + 1 + hop
            valid = sp > hop if way == 0 else sp + 1 + hop < sp_count

            @pl.when(valid)
            def _():
                act(block, way)

    def y_start(hop, chunk):
        y_each(hop, lambda block, way: y_copy(
            weight_view(grp)(block, chunk), way, hop, chunk // PARTS).start())

    def y_arrive(matrix):
        def wait(hop, block, way):
            start = pl.multiple_of(block * depth + (1 - grp) * half, half)
            y_copy(s.wqk.at[matrix, pl.ds(start, half), :], way, hop, matrix).wait_recv()

        for hop in range(sp_count - 1):
            y_each(hop, functools.partial(wait, hop))

    def y_drain():
        whole = s.wqk.at[0, pl.ds(0, depth), :]
        for hop in range(sp_count - 1):
            y_each(hop, lambda block, way: y_copy(whole, way, hop, 0).wait_send())

    key_chunks, query_chunks = range(PARTS), range(PARTS, 2 * PARTS)

    def send_own(chunks):
        for chunk in chunks:
            for way in range(2):
                line.send(way, 0, chunk)

    pieces, early = s.xr.shape[0], 3
    piece = own // pieces

    def rows_piece(j, p):
        return s.rows.at[pl.ds(pl.multiple_of(j * own + p * piece, piece), piece), :]

    def x_copy(j, p):
        return remote(rows_piece(j, p), rows_piece(j, p), s.xs.at[0], s.xr.at[p],
                      "tp", across)

    def cross(j, p, slot):
        return remote(rows_piece(j, p), rows_piece(j, p), s.cs.at[slot], s.cr.at[slot],
                      "tp", sibling)

    def cross_whole(j, slot):
        ref = s.rows.at[block_rows(j), :]
        return remote(ref, ref, s.cs.at[slot], s.cr.at[slot], "tp", sibling)

    out_rows = s.out_w.shape[1]
    out_half = out_rows // 2
    out_pieces = s.oyr.shape[0]
    out_step = out_half // out_pieces

    direct = out_pieces // 4
    shared = out_pieces - direct

    def out_piece(j, side, p):
        start = pl.multiple_of(side * out_half + p * out_step, out_step)
        return s.out_w.at[j, pl.ds(start, out_step), :]

    def out_bytes(count):
        return s.out_w.at[tp, pl.ds(0, count * out_step), :]

    def out_own_copy(j=tp):
        return remote(s.out_w.at[j], s.out_w.at[j], s.ocs.at[0], s.ocr.at[0], "tp", sibling)

    def out_x(j, k):
        side, p = (grp, k) if k < out_pieces else (1 - grp, shared + k - out_pieces)
        ref = out_piece(j, side, p)
        return remote(ref, ref, s.oxs.at[0], s.oxr.at[k], "tp", across)

    def out_y(side, p):
        ref = out_piece(across, side, p)
        return remote(ref, ref, s.oys.at[0], s.oyr.at[p], "grp", 1 - grp)

    def out_pass(ref, way):
        return remote(ref, ref, s.ods.at[way], s.odr.at[way], "tp", sibling)

    def relay_x(k):
        copy = out_x(across, k)
        copy.wait_recv()
        if k < shared:
            out_y(grp, k).start()
        side, p = (grp, k) if k < out_pieces else (1 - grp, shared + k - out_pieces)
        out_pass(out_piece(across, side, p), 0).start()

    def relay_y(p):
        out_y(1 - grp, p).wait_recv()
        out_pass(out_piece(across, 1 - grp, p), 1).start()

    part_go, part_arrive, part_drain = spread_of(s.part, "sp", s.ps, s.pr)
    sums_go, sums_arrive, sums_drain = spread_of(s.sums, "tp", s.ss, s.sr)
    tot_go, tot_arrive, tot_drain = spread_of(s.totals, "sp", s.ts, s.tr)
    ctx_go, ctx_arrive, ctx_drain = spread_of(s.ctx_totals, "sp", s.us, s.ur)

    load_latent.wait()
    ready()
    for p in range(pieces):
        if p < early:
            x_copy(tp, p).start()
        cross(tp, p, 0).start()
    for load in (load_cond, load_ctx_cond, load_mod_w):
        load.wait()
    v = jnp.concatenate([s.cond[...], s.ctx_cond[...]], axis=0)
    activated = (v / (1.0 + jnp.exp(-v))).astype(bf16)
    s.part[sp] = dot(activated, s.mod_w[...])
    part_go()
    load_key_w.wait()
    load_query_w.wait()
    send_own(key_chunks)
    send_own(query_chunks[:PARTS // 2])

    quarter = keys // 4

    def rope(b, carry):
        rows = pl.ds(pl.multiple_of(b * size, size), size)
        lane = lax.broadcasted_iota(jnp.int32, (1, keys), 1)
        index = jnp.bitwise_and(lane, quarter - 1).astype(f32)
        frequency = jnp.exp(index * (-jnp.log(rope_base) / quarter))
        by_row = lane < keys // 2
        first = jnp.bitwise_and(lane, 2 * quarter - 1) < quarter
        place = lax.broadcasted_iota(jnp.int32, (size, 1), 0) + (sp * count + b * size)
        place = place.astype(f32)
        row = jnp.floor((place + 0.5) * (1.0 / GRID_W))
        col = place - row * GRID_W
        angle = jnp.where(by_row, row, col) * frequency
        s.cosine[rows, :] = jnp.cos(angle)
        sine = jnp.sin(angle)
        s.sine[rows, :] = jnp.where(first, -sine, sine)
        return carry

    lax.fori_loop(0, blocks, rope, 0)

    @pl.when(sp == 0)
    def _():
        s.chain_in[0] = jnp.zeros(s.chain_in.shape[1:], bf16)

    @pl.when(sp == sp_count - 1)
    def _():
        s.chain_in[1] = jnp.zeros(s.chain_in.shape[1:], bf16)

    part_arrive()
    total = s.part[0]
    for j in range(1, sp_count):
        total = total + s.part[j]
    s.sums[tp] = total
    sums_go()
    for p in range(early, pieces):
        x_copy(tp, p).start()
    load_out_w.wait()
    out_own_copy().start()
    for k in range(out_pieces + direct):
        out_x(tp, k).start()
    for chunk in key_chunks:
        z_arrive(0, chunk)
    send_own(query_chunks[PARTS // 2:])
    sums_arrive()
    for load in (load_mod_b, load_context, load_low_w, load_value_w, load_decay_w, load_decay_b, load_extra):
        load.wait()
    modulation = (jnp.concatenate([s.sums[j] for j in range(tp_count)], axis=1)
                  + s.mod_b[...])
    s.shifts[...] = modulation[:, :width]
    s.scales[...] = 1.0 + modulation[:, width:2 * width]
    s.branch_gate[...] = modulation[0:1, 2 * width:]
    s.mod_context[...] = (s.context[...].astype(f32) * s.scales[1:2, :]
                             + s.shifts[1:2, :]).astype(bf16)

    def decay_of(low, direction):
        rank = s.decay_w.shape[1]
        logits = dot(low[:, direction * rank:(direction + 1) * rank], s.decay_w[direction])
        return log_sigmoid(logits + s.decay_b[direction:direction + 1, :]) / gate_scale

    own_head = lax.broadcasted_iota(jnp.int32, (ATTENTION_HEADS, size), 0) == tp

    def project_chip(chip):
        rows = pl.ds(pl.multiple_of(chip * 2 * own, 2 * own), 2 * own)
        mod = (s.rows[rows, :].astype(f32) * s.scales[0:1, :]
               + s.shifts[0:1, :]).astype(bf16)
        s.mod_latent[rows, :] = mod
        s.low[rows, :] = dot(mod, s.low_w[...], ((1,), (1,))).astype(bf16)
        s.value[rows, :] = dot(mod, s.value_w[...]).astype(bf16)

    def gate_chip(chip):
        rows = pl.ds(pl.multiple_of(chip * 2 * own, 2 * own), 2 * own)
        s.gate[rows, :] = dot(s.mod_latent[rows, :], s.gate_w[...]).astype(bf16)

    def decay_chip(chip):
        for i in range(2 * own // size):
            b = chip * (2 * own // size) + i
            rows = pl.ds(pl.multiple_of(b * size, size), size)
            low = s.low[rows, :]
            for direction in range(2):
                mask = triangle(size, direction == 1).astype(f32)
                edge = 0 if direction == 1 else size - 1
                head_extra = jnp.sum(jnp.where(own_head, s.extra[direction, :, rows], 0.0),
                                     axis=0, keepdims=True)
                added = jnp.sum(mask * head_extra, axis=1, keepdims=True)
                cum = dot(mask, decay_of(low, direction), precision=highest) + added
                s.cum[direction, rows, :] = cum
                s.block_total[direction, b] = cum[edge:edge + 1, :]

    ctx_low = dot(s.mod_context[...], s.low_w[...], ((1,), (1,))).astype(bf16)
    ctx_totals = []
    for direction in range(2):
        mask = triangle(ctx, direction == 1).astype(f32)
        edge = 0 if direction == 1 else ctx - 1
        cum = dot(mask, decay_of(ctx_low, direction), precision=highest)
        ctx_totals.append(cum[edge:edge + 1, :])
        s.ctx_close[direction] = jnp.exp(ctx_totals[direction] - cum)
    s.ctx_totals[sp] = jnp.concatenate(ctx_totals, axis=0)
    ctx_go()
    s.ctx_value[...] = dot(s.mod_context[...], s.value_w[...]).astype(bf16)
    for chunk in key_chunks:
        if sp_count > 2:
            z_arrive(1, chunk)
    cross_whole(sibling, 0).wait_recv()
    project_chip(x)
    decay_chip(x)
    for chunk in query_chunks:
        z_arrive(0, chunk, False)
    for hop in range(2, sp_count - 1):
        for chunk in key_chunks:
            z_arrive(hop, chunk)
    for chunk in query_chunks:
        y_start(0, chunk)
    for p in range(pieces):
        x_copy(across, p).wait_recv()
        cross(across, p, 1).start()
    load_gate_w.wait()
    gate_chip(x)
    cross_whole(far_sibling, 1).wait_recv()
    project_chip(1 - x)
    if sp_count > 2:
        for chunk in query_chunks:
            z_arrive(1, chunk)
    decay_chip(1 - x)
    for direction in range(2):
        before = None
        for turn in range(blocks):
            b = blocks - 1 - turn if direction == 1 else turn
            if before is not None:
                s.ahead[direction, b:b + 1, :] = before
            block_total = s.block_total[direction, b]
            before = block_total if before is None else before + block_total
        s.total[direction:direction + 1, :] = before
    s.totals[sp] = s.total[...]
    tot_go()
    y_arrive(0)
    chunk_width = s.chain_in.shape[4]
    part_keys = s.chain_in.shape[3]
    chunk_count = vals // chunk_width
    turns_each = s.chain_in.shape[2]
    steps = 2 * turns_each

    def column(row):
        return jnp.broadcast_to(jnp.exp(row).T, (keys, chunk_width))

    def column_chunks():
        return [slice(c * chunk_width, (c + 1) * chunk_width) for c in range(chunk_count)]

    def sum_of(ref, direction, later):
        total = jnp.zeros((1, keys), f32)
        for j in range(sp_count):
            chosen = (j > sp) if later else (j < sp)
            total = total + jnp.where(chosen, ref[j, direction:direction + 1, :], 0.0)
        return total

    ctx_key = dot(s.mod_context[...], s.wqk[0]).astype(bf16).astype(f32)
    ctx_arrive()
    for direction in range(2):
        closing = (ctx_key * s.ctx_close[direction]).astype(bf16)
        after = column(sum_of(s.ctx_totals, direction, direction == 0))
        carry = dot(closing, s.ctx_value[...], ((0,), (0,)))
        for cols in column_chunks():
            s.carry[direction, :, cols] = after * carry[:, cols]
    first_way = jnp.where(sp < sp_count // 2, 0, 1)

    def ends(way):
        return (jnp.where(way == 0, sp > 0, sp < sp_count - 1),
                jnp.where(way == 0, sp < sp_count - 1, sp > 0))

    def chain_copy(way, kind, c, target):
        return remote(s.chain_out.at[way, kind, c], s.chain_in.at[way, kind, c],
                      s.hs.at[way], s.hr.at[way, kind, c], "sp", target)

    def chain_part(c):
        part, col = c % (keys // part_keys), c // (keys // part_keys)
        return (slice(part * part_keys, (part + 1) * part_keys),
                slice(col * chunk_width, (col + 1) * chunk_width))

    def chain_send(way, kind, c):
        rows, cols = chain_part(c)
        held = s.chain_in[way, kind, c].astype(f32)
        if kind == 0:
            added = held + s.carry[1 - way, rows, cols]
        else:
            added = s.own_decay[way, rows, :] * held + s.state[way, rows, cols]
        s.chain_out[way, kind, c] = added.astype(bf16)
        chain_copy(way, kind, c, sp + 1 - 2 * way).start()

    def chain_open(way, kind):
        has_before, has_next = ends(way)

        @pl.when(jnp.logical_and(has_next, jnp.logical_not(has_before)))
        def _():
            if kind == 1:
                for cols in column_chunks():
                    s.state[way, :, cols] += s.own_decay[way] * s.carry[way, :, cols]
            for c in range(turns_each):
                chain_send(way, kind, c)

    def chain(way, i):
        kind, c = i // turns_each, i % turns_each
        has_before, has_next = ends(way)

        @pl.when(has_before)
        def _():
            chain_copy(way, kind, c, sp - 1 + 2 * way).wait_recv()

            @pl.when(has_next)
            def _():
                chain_send(way, kind, c)

    chain_open(first_way, 0)
    for b in range(blocks):
        rows = slice(b * size, (b + 1) * size)
        key = dot(s.mod_latent[rows, :], s.wqk[0]).astype(bf16)
        s.key[rows, :] = rotate(key.astype(f32), s.cosine[rows, :], s.sine[rows, :])
    for direction in range(2):
        edge = 0 if direction == 1 else size - 1
        state = None
        for turn in range(blocks):
            b = blocks - 1 - turn if direction == 1 else turn
            rows = slice(b * size, (b + 1) * size)
            cum = s.cum[direction, rows, :]
            block_total = cum[edge:edge + 1, :]
            closing = (s.key[rows, :] * jnp.exp(block_total - cum)).astype(bf16)
            term = dot(closing, s.value[rows, :], ((0,), (0,)))
            if state is None:
                state = term
            else:
                s.start[direction, b] = state.astype(bf16)
                state = jnp.exp(block_total).T * state + term
        s.state[direction] = state
    for direction in range(2):
        s.own_decay[direction] = column(s.total[direction:direction + 1, :])
    chain_open(first_way, 1)
    relay_x(0)
    tot_arrive()
    for direction in range(2):
        s.ahead_decay[direction] = column(sum_of(s.totals, direction, direction == 1))

        @pl.when(ends(direction)[0])
        def _():
            both = s.own_decay[direction] * s.ahead_decay[direction]
            for cols in column_chunks():
                s.state[direction, :, cols] += both * s.carry[direction, :, cols]

    def attend(b):
        rows = slice(b * size, (b + 1) * size)
        query = dot(s.mod_latent[rows, :], s.wqk[1]).astype(bf16)
        rq = rotate(query.astype(f32) * keys ** -0.5, s.cosine[rows, :], s.sine[rows, :])
        rk = s.key[rows, :]
        scores, out = None, None
        for direction in range(2):
            keep = triangle(size, direction == 1)
            middle = size // 2 if direction == 1 else size // 2 - 1
            cum = s.cum[direction, rows, :]
            center = cum[middle:middle + 1, :]
            q_mid = (rq * jnp.exp(cum - center)).astype(bf16)
            k_mid = (rk * jnp.exp(center - cum)).astype(bf16)
            score = jnp.where(keep, dot(q_mid, k_mid, ((1,), (1,))), 0.0)
            scores = score if scores is None else scores + score
            q_dec = rq * jnp.exp(cum)
            q_all = q_dec
            if b != (blocks - 1 if direction == 1 else 0):
                carried = dot(q_dec.astype(bf16), s.start[direction, b])
                out = carried if out is None else out + carried
                q_all = q_dec * jnp.exp(s.ahead[direction, b:b + 1, :])
            s.q_all[rows, direction * keys:(direction + 1) * keys] = q_all.astype(bf16)
        inner = dot(scores.astype(bf16), s.value[rows, :])
        s.mixture[rows, :] = inner if out is None else out + inner

    lag, early_turns = 4, 8

    def chain_turn(turn):
        if turn < steps:
            chain(first_way, turn)
        if lag <= turn < steps + lag:
            chain(1 - first_way, turn - lag)

    gate_chip(1 - x)
    for turn in range(lag):
        chain_turn(turn)
    for hop in range(2, sp_count - 1):
        for chunk in query_chunks:
            z_arrive(hop, chunk)
    for k in range(1, 3):
        relay_x(k)
    for turn in range(lag, early_turns):
        chain_turn(turn)
    y_arrive(1)
    for turn in range(max(2 * blocks, steps + lag - early_turns)):
        if turn % 2 == 0 and turn < 2 * blocks:
            attend(turn // 2)
        chain_turn(early_turns + turn)
        if turn % 2 == 0 and 3 + turn // 2 < shared:
            relay_x(3 + turn // 2)
    for c in range(turns_each):
        rows, cols = chain_part(c)
        for direction in range(2):
            joined = (s.chain_in[direction, 1, c].astype(f32)
                      + s.ahead_decay[direction, rows, :]
                      * (s.carry[direction, rows, cols]
                         + s.chain_in[1 - direction, 0, c].astype(f32)))
            start = direction * keys + rows.start
            s.joined[start:start + part_keys, cols] = joined.astype(bf16)
    load_norm_gain.wait()

    def gate_rows(j):
        rows = block_rows(j)
        mixture = s.mixture[rows, :] + dot(s.q_all[rows, :], s.joined[...])
        squares = jnp.mean(mixture * mixture, axis=1, keepdims=True)
        gate = s.gate[rows, :].astype(f32)
        normed = mixture * lax.rsqrt(squares + norm_eps) * s.norm_gain[...]
        s.gated[rows, :] = (normed * (gate / (1.0 + jnp.exp(-gate)))).astype(bf16)

    def gated_copy(k, j):
        return remote(s.gated.at[block_rows(j), :], s.gathered.at[tp], s.gs.at[k], s.gr.at[k],
                      "tp", j)

    def gated_arrive(k, j):
        remote(s.gathered.at[j], s.gathered.at[j], s.gs.at[k], s.gr.at[k], "tp", j).wait_recv()

    out_chunks = 4
    out_width = width // out_chunks
    out_cols = [slice(n * out_width, (n + 1) * out_width) for n in range(out_chunks)]

    for k, j in ((1, across), (2, far_sibling), (0, sibling)):
        gate_rows(j)
        gated_copy(k, j).start()
    gate_rows(tp)
    for k in range(max(3, shared), out_pieces + direct):
        relay_x(k)
    out_own_copy(sibling).wait_recv()
    for cols in out_cols:
        s.branch[:, cols] = dot(s.gated[block_rows(tp), :], s.out_w[tp, :, cols])
    gated_arrive(0, sibling)
    for cols in out_cols:
        s.branch[:, cols] += dot(s.gathered[sibling], s.out_w[sibling, :, cols])
    for p in range(shared):
        relay_y(p)
    out_pass(out_bytes(out_pieces + direct), 0).wait_recv()
    out_pass(out_bytes(shared), 1).wait_recv()
    gated_arrive(1, across)
    for cols in out_cols:
        s.branch[:, cols] += dot(s.gathered[across], s.out_w[across, :, cols])
    gated_arrive(2, far_sibling)
    for cols in out_cols:
        branch = s.branch[:, cols] + dot(s.gathered[far_sibling], s.out_w[far_sibling, :, cols])
        summed_ref[:, cols] = (residual_scale * s.rows[block_rows(tp), cols].astype(f32)
                             + s.branch_gate[:, cols] * branch)
    part_drain()
    sums_drain()
    tot_drain()
    ctx_drain()
    line.drain_whole(s.wqk.at[0, pl.ds(0, depth), :])
    y_drain()
    own_rows = s.rows.at[block_rows(tp), :]
    remote(own_rows, own_rows, s.xs.at[0], s.xr.at[0], "tp", across).wait_send()
    for slot in range(2):
        cross_whole(tp, slot).wait_send()
    for way in range(2):
        has_next = sp < sp_count - 1 if way == 0 else sp > 0

        @pl.when(has_next)
        def _():
            remote(s.chain_out.at[way], s.chain_in.at[way], s.hs.at[way], s.hr.at[way, 0, 0],
                   "sp", sp + 1 - 2 * way).wait_send()
    out_own_copy().wait_send()
    ref = out_bytes(out_pieces + direct)
    remote(ref, ref, s.oxs.at[0], s.oxr.at[0], "tp", across).wait_send()
    out_pass(ref, 0).wait_send()
    ref = out_bytes(shared)
    remote(ref, ref, s.oys.at[0], s.oyr.at[0], "grp", 1 - grp).wait_send()
    out_pass(ref, 1).wait_send()
    for k, j in enumerate((sibling, across, far_sibling)):
        gated_copy(k, j).wait_send()


def norm_kernel(summed_ref, gain_ref, bias_ref, out_ref):
    summed = summed_ref[...]
    centered = summed - jnp.mean(summed, axis=1, keepdims=True)
    variance = jnp.mean(centered * centered, axis=1, keepdims=True)
    out_ref[...] = (centered * lax.rsqrt(variance + norm_eps) * gain_ref[...]
                    + bias_ref[...]).astype(bf16)


def fused(latent, context, condition, context_condition, mod_weight, mod_bias, query_weight,
          key_weight, value_weight, out_gate_weight, decay_in_weight, decay_weight, decay_bias,
          extra_decay, norm_gain, out_weight, final_gain, final_bias):
    sp_count, tp_count = lax.axis_size("sp"), lax.axis_size("tp")
    own, width = latent.shape
    depth = query_weight.shape[0]
    keys = query_weight.shape[1] // ATTENTION_HEADS
    vals = value_weight.shape[1]
    ctx = context.shape[0]
    count = own * tp_count
    blocks = count // (2 * BLOCK)
    mod_cols = mod_weight.shape[1]
    chains, outs, pieces = 4, 8, 8
    args = (latent, context, condition[None, :], context_condition[None, :], mod_weight,
            mod_bias[None, :], query_weight, key_weight, value_weight, out_gate_weight,
            decay_in_weight.T, decay_weight, decay_bias, extra_decay, norm_gain[None, :],
            out_weight)
    dma, vmem = pltpu.SemaphoreType.DMA, pltpu.VMEM
    hops = sp_count - 1
    scratch = Scratch(
        cond=vmem((1, condition.shape[0]), f32),
        ctx_cond=vmem((1, condition.shape[0]), f32),
        mod_w=vmem(mod_weight.shape, bf16),
        mod_b=vmem((1, mod_bias.shape[0]), f32),
        wqk=vmem((2, depth * sp_count, keys), bf16),
        rows=vmem((count, width), bf16),
        mod_latent=vmem((count, width), bf16),
        context=vmem(context.shape, bf16),
        mod_context=vmem(context.shape, bf16),
        low_w=vmem(decay_in_weight.shape[::-1], bf16),
        value_w=vmem(value_weight.shape, bf16),
        gate_w=vmem(out_gate_weight.shape, bf16),
        out_w=vmem((tp_count,) + out_weight.shape, bf16),
        decay_w=vmem(decay_weight.shape[:2] + (keys,), bf16),
        decay_b=vmem((2, keys), f32),
        extra=vmem(extra_decay.shape, f32),
        norm_gain=vmem((1, vals), f32),
        part=vmem((sp_count, 2, mod_cols), f32),
        sums=vmem((tp_count, 2, mod_cols), f32),
        totals=vmem((sp_count, 2, keys), f32),
        ctx_totals=vmem((sp_count, 2, keys), f32),
        shifts=vmem((2, width), f32),
        scales=vmem((2, width), f32),
        branch_gate=vmem((1, width), f32),
        cosine=vmem((count, keys), f32),
        sine=vmem((count, keys), f32),
        ctx_close=vmem((2, ctx, keys), f32),
        ctx_value=vmem((ctx, vals), bf16),
        low=vmem((count, decay_in_weight.shape[1]), bf16),
        value=vmem((count, vals), bf16),
        gate=vmem((count, vals), bf16),
        key=vmem((count, keys), f32),
        cum=vmem((2, count, keys), f32),
        ahead=vmem((2, blocks, keys), f32),
        block_total=vmem((2, blocks, 1, keys), f32),
        total=vmem((2, keys), f32),
        start=vmem((2, blocks, keys, vals), bf16),
        state=vmem((2, keys, vals), f32),
        carry=vmem((2, keys, vals), f32),
        own_decay=vmem((2, keys, vals // chains), f32),
        ahead_decay=vmem((2, keys, vals // chains), f32),
        chain_in=vmem((2, 2, 2 * chains, keys // 2, vals // chains), bf16),
        chain_out=vmem((2, 2, 2 * chains, keys // 2, vals // chains), bf16),
        q_all=vmem((count, 2 * keys), bf16),
        mixture=vmem((count, vals), f32),
        joined=vmem((2 * keys, vals), bf16),
        gated=vmem((count, vals), bf16),
        gathered=vmem((tp_count, own, vals), bf16),
        branch=vmem((own, width), f32),
        load_sem=dma((len(args),)),
        zs=dma((2, hops)), zr=dma((2, hops, 2 * PARTS)),
        ys=dma((2, hops)), yr=dma((2, hops, 2)),
        xs=dma((1,)), xr=dma((pieces,)), cs=dma((2,)), cr=dma((2,)),
        ocs=dma((1,)), ocr=dma((1,)), ods=dma((2,)), odr=dma((2,)),
        oxs=dma((1,)), oxr=dma((outs + outs // 4,)), oys=dma((1,)), oyr=dma((outs,)),
        gs=dma((tp_count - 1,)), gr=dma((tp_count - 1,)),
        ps=dma((hops,)), pr=dma((hops,)), ts=dma((hops,)), tr=dma((hops,)),
        us=dma((hops,)), ur=dma((hops,)),
        ss=dma((tp_count - 1,)), sr=dma((tp_count - 1,)),
        hs=dma((2,)), hr=dma((2, 2, 2 * chains)),
    )
    summed = pl.pallas_call(
        fused_kernel,
        out_shape=pltpu.VMEM((own, width), f32),
        in_specs=[pl.BlockSpec(memory_space=pltpu.HBM)] * len(args),
        out_specs=pl.BlockSpec(memory_space=pltpu.VMEM),
        scratch_shapes=[scratch],
        compiler_params=pltpu.CompilerParams(
            vmem_limit_bytes=60 * 1024 * 1024, collective_id=2, has_side_effects=True),
        cost_estimate=pl.CostEstimate(flops=6_000_000_000, bytes_accessed=12_000_000,
                                      transcendentals=2_000_000),
    )(*args)
    return pl.pallas_call(
        norm_kernel,
        out_shape=jax.ShapeDtypeStruct((own, width), bf16),
        in_specs=[pl.BlockSpec(memory_space=pltpu.VMEM)] * 3,
        out_specs=pl.BlockSpec(memory_space=pltpu.VMEM),
        compiler_params=pltpu.CompilerParams(vmem_limit_bytes=8 * 1024 * 1024),
        cost_estimate=pl.CostEstimate(flops=2_000_000, bytes_accessed=2_000_000,
                                      transcendentals=1_000),
    )(summed, final_gain[None, :], final_bias[None, :])


def whole_heads(mesh):
    return mesh.shape["tp"] == ATTENTION_HEADS and mesh.shape["grp"] == 2


def solution(mesh):
    placed = (
        P(("grp", "sp", "tp"), None),
        P(("grp", "sp"), None),
        P(("grp", "sp")),
        P("sp"),
        P("sp", "tp"),
        P(),
        P("sp", None),
        P("sp", None),
        P(None, "tp"),
        P(None, "tp"),
        P(),
        P(),
        P(),
        P(None, None, "sp"),
        P(),
        P("tp", None),
        P(),
        P(),
    )
    return jax.shard_map(
        fused if whole_heads(mesh) else body, mesh=mesh, in_specs=placed, out_specs=P(("grp", "sp", "tp"), None), check_vma=False
    )
```
